32 devices in a mesh: sp: 8 (over z, y), dp: 4 (over x, core).
Axes of the slice: x: 2, y: 2, z: 4, core: 2. Of those that a mesh axis runs over, the one named last changes fastest.
Arguments:
- out_cotangent: bfloat16 [4, 2048, 2048], P('dp', 'sp'), may hold values from -6 to 6
- value_pre: bfloat16 [4, 2048, 2048], P('dp', 'sp'), may hold values from -8 to 8
- gate_pre: bfloat16 [4, 2048, 2048], P('dp', 'sp'), may hold values from -8 to 8
- out_weight: bfloat16 [2048, 2048], P('dp'), may hold values from -0.125 to 0.125
- conv_kernel: bfloat16 [31, 2048], P(None, 'sp'), may hold values from -6 to 6
- norm_gain: bfloat16 [2048], P('sp'), may hold values from 0.099609375 to 1.8984375
Outputs:
- grad_value: bfloat16 [4, 2048, 2048], P('dp', 'sp')
- grad_gate: bfloat16 [4, 2048, 2048], P('dp', 'sp')
- grad_out_weight: float32 [2048, 2048], P(('sp', 'dp'))
- grad_kernel: float32 [31, 2048], P(None, 'sp')
- grad_gain: float32 [2048], P('sp')
The draws below stay inside these ranges and needn't reach their ends.
All inputs are finite; a program needn't handle non-finite values.
Results may differ from the reference program's by a relative error of at most 0.011.
Values may be sent and summed in bfloat16 or wider, within the bound.
A program may use at most 128 MiB of HBM per device.

```python
import math
import jax
import jax.numpy as jnp
from jax import lax

D = 2048
CONV_W = 31
SEQS = 4
LENGTH = 2048
TOKENS = 8192


def draw_value_pre(key, part):
    keys = jax.random.split(jax.random.fold_in(key, 11), 2)
    shape = (SEQS, LENGTH, D)
    row_scale = jnp.exp(jax.random.uniform(keys[1], (SEQS, LENGTH, 1), jnp.float32, math.log(0.4), math.log(2.5)))
    values_out = jax.random.normal(keys[0], shape, jnp.float32) * row_scale
    return jnp.clip(values_out, -8.0, 8.0).astype(jnp.bfloat16)


def draw_conv_kernel(key, part):
    keys = jax.random.split(jax.random.fold_in(key, 23), 2)
    position = jnp.arange(D, dtype=jnp.float32) / float(D)
    rough = jnp.exp(jax.random.uniform(keys[1], (1, D), jnp.float32, math.log(0.5), math.log(2.0)))
    column_scale = jnp.exp(math.log(6.0) * position)[None, :] * rough
    taps = jax.random.normal(keys[0], (CONV_W, D), jnp.float32)
    taps = taps * column_scale * float(CONV_W) ** (-0.5)
    return jnp.clip(taps, -6.0, 6.0).astype(jnp.bfloat16)


def shard_levels(rng, shape, pieces, low, high):
    def one(axis_at, blocks):
        steps = jax.random.uniform(jax.random.fold_in(jax.random.fold_in(rng, 6), axis_at), (blocks,), jnp.float32, low / len(pieces), high / len(pieces))
        return jnp.repeat(jnp.exp(steps), shape[axis_at] // blocks).reshape((-1,) + (1,) * (len(shape) - axis_at - 1))

    gain = one(*pieces[0])
    for cut in pieces[1:]:
        gain = gain * one(*cut)
    return gain


def normal_values(rng, shape, spread, limit, cuts=(), kind=jnp.bfloat16):
    values = jax.random.normal(rng, shape, jnp.float32) * spread
    if len(cuts) > 0:
        values = shard_levels(rng, shape, cuts, -0.22, 0.18) * values
    return jnp.clip(values, min=-limit, max=limit).astype(kind)


def setup_inputs(seed: int = 0) -> dict:
    key_list = jax.random.split(jax.random.key(seed), 7)
    out_cotangent = normal_values(key_list[0], (SEQS, LENGTH, D), 1.0, 6.0, ((0, 4), (1, 8)))
    value_pre = draw_value_pre(jax.random.fold_in(key_list[6], 71), 0)
    gate_pre = normal_values(key_list[2], (SEQS, LENGTH, D), 1.5, 8.0, ((0, 4), (1, 8)))
    out_weight = normal_values(key_list[3], (D, D), D ** -0.5, 0.125, ((0, 4),))
    conv_kernel = draw_conv_kernel(jax.random.fold_in(key_list[6], 71), 0)
    norm_gain = jnp.clip(1.0 + 0.18 * jax.random.normal(key_list[5], (D,), jnp.float32), 0.099609375, 1.8984375).astype(jnp.bfloat16)
    return {"out_cotangent": out_cotangent, "value_pre": value_pre, "gate_pre": gate_pre, "out_weight": out_weight, "conv_kernel": conv_kernel, "norm_gain": norm_gain}


epsilon = 1e-05

def shift_down(array, offset):
    return jnp.pad(array, ((offset, 0), (0, 0)))[:array.shape[0]]

def shift_up(array, offset):
    return jnp.pad(array, ((0, offset), (0, 0)))[offset:]

def reference(out_cotangent, value_pre, gate_pre, out_weight, conv_kernel, norm_gain):
    taps_float = conv_kernel.astype(jnp.float32)
    gain_float = norm_gain.astype(jnp.float32)
    weight_sum = jnp.zeros((D, D), jnp.float32)
    kernel_sum = jnp.zeros((CONV_W, D), jnp.float32)
    gain_sum = jnp.zeros((D,), jnp.float32)
    value_grads = []
    gate_grads = []
    for sequence in range(SEQS):
        cotangent = out_cotangent[sequence]
        values_in = value_pre[sequence].astype(jnp.float32)
        sigmoid_gate = jax.nn.sigmoid(gate_pre[sequence].astype(jnp.float32))
        gated = (values_in * sigmoid_gate).astype(jnp.bfloat16)
        gated_float = gated.astype(jnp.float32)
        conv = jnp.zeros(gated_float.shape, jnp.float32)
        for offset in range(CONV_W):
            conv = conv + taps_float[offset] * shift_down(gated_float, offset)
        centre = lax.optimization_barrier(jnp.mean(conv, axis=1, keepdims=True))
        deviation = conv - centre
        variance = lax.optimization_barrier(jnp.mean(deviation * deviation, axis=1, keepdims=True))
        inv_scale = lax.rsqrt(variance + epsilon)
        centred = deviation * inv_scale
        normed = centred * gain_float
        activation = jax.nn.silu(normed).astype(jnp.bfloat16)
        grad_act = lax.dot_general(cotangent, out_weight, (((1,), (1,)), ((), ())), preferred_element_type=jnp.float32).astype(jnp.bfloat16)
        weight_sum = weight_sum + lax.dot_general(activation, cotangent, (((0,), (0,)), ((), ())), preferred_element_type=jnp.float32)
        sig_norm = jax.nn.sigmoid(normed)
        grad_normed = grad_act.astype(jnp.float32) * sig_norm * (1.0 + normed * (1.0 - sig_norm))
        gain_sum = gain_sum + lax.optimization_barrier(jnp.sum(grad_normed * centred, axis=0))
        grad_centred = grad_normed * gain_float
        grad_conv = (grad_centred - lax.optimization_barrier(jnp.mean(grad_centred, axis=1, keepdims=True)) - centred * lax.optimization_barrier(jnp.mean(grad_centred * centred, axis=1, keepdims=True))) * inv_scale
        kernel_rows = [lax.optimization_barrier(jnp.sum(grad_conv * shift_down(gated_float, offset), axis=0)) for offset in range(CONV_W)]
        kernel_sum = kernel_sum + jnp.stack(kernel_rows, axis=0)
        grad_gated = jnp.zeros(grad_conv.shape, jnp.float32)
        for offset in range(CONV_W):
            grad_gated = grad_gated + taps_float[offset] * shift_up(grad_conv, offset)
        grad_gated = grad_gated.astype(jnp.bfloat16).astype(jnp.float32)
        value_grads.append((grad_gated * sigmoid_gate).astype(jnp.bfloat16))
        gate_grads.append((grad_gated * values_in * sigmoid_gate * (1.0 - sigmoid_gate)).astype(jnp.bfloat16))
    factor = float(TOKENS) ** (-0.5)
    return (jnp.stack(value_grads, axis=0), jnp.stack(gate_grads, axis=0), weight_sum * factor, kernel_sum * factor, gain_sum * factor)
```

```python
import functools

import jax
import jax.numpy as jnp
from jax import lax
from jax.experimental import pallas as pl
from jax.experimental.pallas import tpu as pltpu
from jax.sharding import PartitionSpec as P

epsilon = 1e-05
LANES = 128
HALVES = 2
f32 = jnp.float32
bf16 = jnp.bfloat16


def general_kernel(
    S, N, T, C, K, HB, ids,
    cot, val, gate, w, taps,
    gv, gg, gw, kout, gout,
    cot_all, ext, cen, gc, gext, kall, act, act_all, ga_send, ga, wpart, rbuf,
    kg, krecv, ksum, k2recv, send_sem, recv_sem,
):
    s = lax.axis_index("sp")
    d = lax.axis_index("dp")
    chunks = C // LANES
    cps = chunks // S
    cpd = chunks // N
    block = C // (S * N)
    RB = min(T, 128)
    total = S * N
    me = s * N + d
    partner = d + 1 - 2 * lax.rem(d, 2)
    factor = float(S * N * T) ** (-0.5)
    hrows = T // HALVES
    waits = []

    def copy(src, dst, i, to_s, to_d):
        return pltpu.make_async_remote_copy(
            src_ref=src, dst_ref=dst, send_sem=send_sem.at[i], recv_sem=recv_sem.at[i],
            device_id={"sp": to_s, "dp": to_d}, device_id_type=pl.DeviceIdType.MESH,
        )

    def send(src, dst, i, to_s, to_d):
        c = copy(src, dst, i, to_s, to_d)
        c.start()
        waits.append(c)

    def arrived(dst, i):
        copy(dst, dst, i, s, partner).wait_recv()

    barrier = pltpu.get_barrier_semaphore()

    def greet(j, _):
        other = lax.rem(me + j, total)
        pl.semaphore_signal(
            barrier, inc=1, device_id={"sp": other // N, "dp": lax.rem(other, N)},
            device_id_type=pl.DeviceIdType.MESH,
        )
        return _

    lax.fori_loop(1, total, greet, 0)
    def gate_chunk(cb, _):
        cols = pl.ds(pl.multiple_of(cb * LANES, LANES), LANES)
        sig = jax.nn.sigmoid(gate[:, cols].astype(f32))
        ext[cb, pl.ds(HB, T), :] = (val[:, cols].astype(f32) * sig).astype(bf16).astype(f32)
        return _

    lax.fori_loop(0, chunks, gate_chunk, 0)
    pl.semaphore_wait(barrier, total - 1)

    for j in range(1, S):
        send(taps, kall.at[pl.ds(s * cps, cps)], ids["taps"] + j, lax.rem(s + j, S), d)
    following = lax.rem(s + 1, S)
    preceding = lax.rem(s + S - 1, S)
    send(ext.at[:, pl.ds(T, HB), :], ext.at[:, pl.ds(0, HB), :], ids["front"], following, d)
    for j in range(1, N // 2):
        for h in range(HALVES):
            rows = pl.ds(h * hrows, hrows)
            send(cot.at[rows], cot_all.at[d, rows], ids["mirror"] + j * HALVES + h, s, lax.rem(d + 2 * j, N))
    send(cot, cot_all.at[d], ids["partner"], s, partner)
    kall[pl.ds(s * cps, cps)] = taps[...]
    cot_all[d] = cot[...]
    for j in range(1, S):
        arrived(kall.at[pl.ds(lax.rem(s + S - j, S) * cps, cps)], ids["taps"] + j)
    arrived(ext.at[:, pl.ds(0, HB), :], ids["front"])

    @pl.when(s == 0)
    def _():
        ext[:, pl.ds(0, HB), :] = jnp.zeros((chunks, HB, LANES), f32)

    def conv_chunk(cb, sums):
        tf = kall[cb].astype(f32)
        parts = []
        for rb in range(T // RB):
            acc = jnp.zeros((RB, LANES), f32)
            for k in range(K):
                acc = acc + tf[k : k + 1] * ext[cb, pl.ds(HB - k + rb * RB, RB), :]
            cen[cb, pl.ds(rb * RB, RB), :] = acc
            parts.append(jnp.sum(acc, axis=1, keepdims=True))
        return sums + jnp.concatenate(parts, axis=0)

    column = jnp.zeros((T, 1), f32)
    mean = lax.fori_loop(0, chunks, conv_chunk, column) / C

    def square_chunk(cb, sums):
        dev = cen[cb] - mean
        return sums + dev * dev

    squares = lax.fori_loop(0, chunks, square_chunk, jnp.zeros((T, LANES), f32))
    inv = lax.rsqrt(jnp.sum(squares, axis=1, keepdims=True) / C + epsilon)

    def relay():
        for j in range(1, N // 2):
            origin = lax.rem(d + N - 2 * j, N)
            for h in range(HALVES):
                piece = cot_all.at[origin, pl.ds(h * hrows, hrows)]
                arrived(piece, ids["mirror"] + j * HALVES + h)
                send(piece, piece, ids["relay"] + j * HALVES + h, s, partner)

    def act_chunk(cb, _):
        centred = (cen[cb] - mean) * inv
        cen[cb] = centred
        normed = centred * kall[cb].astype(f32)[K : K + 1]
        act[cb] = (normed * jax.nn.sigmoid(normed)).astype(bf16)
        return _

    lax.fori_loop(0, chunks, act_chunk, 0)
    for j in range(1, N):
        to = lax.rem(d + j, N)
        send(act.at[pl.ds(to * cpd, cpd)], act_all.at[d], ids["act"] + j, s, to)
    act_all[d] = act[pl.ds(d * cpd, cpd)]

    def project(source, slot):
        def pair(m, _):
            rows = pl.ds(pl.multiple_of(m * 2 * LANES, 2 * LANES), 2 * LANES)
            out = lax.dot_general(
                cot_all[source], w[rows, :], (((1,), (1,)), ((), ())), preferred_element_type=f32
            ).astype(bf16)
            ga_send[slot, 2 * m] = out[:, :LANES]
            ga_send[slot, 2 * m + 1] = out[:, LANES:]
            return _

        lax.fori_loop(0, cpd // 2, pair, 0)

    mine = pl.ds(d * cpd, cpd)
    project(d, 0)
    ga[mine] = ga_send[0]
    arrived(cot_all.at[partner], ids["partner"])
    project(partner, 1)
    send(ga_send.at[1], ga.at[mine], ids["ga"] + 1, s, partner)
    relay()
    for j in range(1, N // 2):
        origin = lax.rem(d + N - 2 * j, N)
        project(origin, 2 * j)
        send(ga_send.at[2 * j], ga.at[mine], ids["ga"] + 2 * j, s, origin)
    for j in range(1, N // 2):
        origin = lax.rem(partner + N - 2 * j, N)
        for h in range(HALVES):
            arrived(cot_all.at[origin, pl.ds(h * hrows, hrows)], ids["relay"] + j * HALVES + h)
        project(origin, 2 * j + 1)
        send(ga_send.at[2 * j + 1], ga.at[mine], ids["ga"] + 2 * j + 1, s, origin)

    for j in range(1, N):
        arrived(act_all.at[lax.rem(d + N - j, N)], ids["act"] + j)
    NT = min(C, 512)

    def weight_tile(i, _):
        m, n = i // (C // NT), lax.rem(i, C // NT)
        cols = pl.ds(pl.multiple_of(n * NT, NT), NT)
        acc = jnp.zeros((LANES, NT), f32)
        for q in range(N):
            acc = acc + lax.dot_general(
                act_all[q, m], cot_all[q, :, cols], (((0,), (0,)), ((), ())),
                preferred_element_type=f32,
            )
        wpart[pl.ds(pl.multiple_of(m * LANES, LANES), LANES), cols] = acc.astype(bf16)
        return _

    lax.fori_loop(0, cpd * (C // NT), weight_tile, 0)

    def block_of(j):
        i = lax.rem(s + j, S)
        owner = d * S + i
        rows = pl.ds(pl.multiple_of(i * block, block), block)
        return owner, rows, pltpu.make_async_remote_copy(
            src_ref=wpart.at[rows], dst_ref=rbuf.at[s], send_sem=send_sem.at[ids["rs"] + j],
            recv_sem=recv_sem.at[ids["rs"] + s],
            device_id={"sp": owner // N, "dp": lax.rem(owner, N)},
            device_id_type=pl.DeviceIdType.MESH,
        )

    def send_blocks(first, last):
        for j in range(first, last):
            owner, rows, c = block_of(j)

            @pl.when(owner != me)
            def _():
                c.start()

            @pl.when(owner == me)
            def _():
                rbuf[s] = wpart[rows, :]

    send_blocks(0, S // 2)

    for j in range(1, N // 2):
        arrived(ga.at[pl.ds(lax.rem(d + 2 * j, N) * cpd, cpd)], ids["ga"] + 2 * j)
        arrived(ga.at[pl.ds(lax.rem(partner + 2 * j, N) * cpd, cpd)], ids["ga"] + 2 * j + 1)
    arrived(ga.at[pl.ds(partner * cpd, cpd)], ids["ga"] + 1)

    def grad_chunk(cb, sums):
        one, two = sums
        centred = cen[cb]
        gain = kall[cb].astype(f32)[K : K + 1]
        normed = centred * gain
        sg = jax.nn.sigmoid(normed)
        grad = ga[cb].astype(f32) * sg * (1.0 + normed * (1.0 - sg))
        kg[cb, pl.ds(K, 1), :] = jnp.sum(grad * centred, axis=0, keepdims=True)
        grad = grad * gain
        gc[cb] = grad
        return one + grad, two + grad * centred

    zero = jnp.zeros((T, LANES), f32)
    one, two = lax.fori_loop(0, chunks, grad_chunk, (zero, zero))
    first = jnp.sum(one, axis=1, keepdims=True) / C
    second = jnp.sum(two, axis=1, keepdims=True) / C

    def conv_grad(cb, _):
        gext[cb, pl.ds(0, T), :] = (gc[cb] - first - cen[cb] * second) * inv
        return _

    lax.fori_loop(0, chunks, conv_grad, 0)
    send(gext.at[:, pl.ds(0, HB), :], gext.at[:, pl.ds(T, HB), :], ids["back"], preceding, d)

    def taps_chunk(cb, _):
        for k in range(K):
            acc = jnp.zeros((8, LANES), f32)
            for rb in range(T // RB):
                prod = gext[cb, pl.ds(rb * RB, RB), :] * ext[cb, pl.ds(HB - k + rb * RB, RB), :]
                acc = acc + jnp.sum(prod.reshape(RB // 8, 8, LANES), axis=0)
            kg[cb, pl.ds(k, 1), :] = jnp.sum(acc, axis=0, keepdims=True)
        return _

    lax.fori_loop(0, chunks, taps_chunk, 0)
    for j in range(1, S):
        to = lax.rem(s + j, S)
        send(kg.at[pl.ds(to * cps, cps)], krecv.at[j], ids["kg"] + j, to, d)
    send_blocks(S // 2, S)

    arrived(gext.at[:, pl.ds(T, HB), :], ids["back"])

    @pl.when(s == S - 1)
    def _():
        gext[:, pl.ds(T, HB), :] = jnp.zeros((chunks, HB, LANES), f32)

    def gated_chunk(cb, _):
        cols = pl.ds(pl.multiple_of(cb * LANES, LANES), LANES)
        tf = kall[cb].astype(f32)
        for rb in range(T // RB):
            rows = pl.ds(rb * RB, RB)
            acc = jnp.zeros((RB, LANES), f32)
            for k in range(K):
                acc = acc + tf[k : k + 1] * gext[cb, pl.ds(k + rb * RB, RB), :]
            acc = acc.astype(bf16).astype(f32)
            sig = jax.nn.sigmoid(gate[rows, cols].astype(f32))
            gv[rows, cols] = (acc * sig).astype(bf16)
            gg[rows, cols] = (acc * val[rows, cols].astype(f32) * sig * (1.0 - sig)).astype(bf16)
        return _

    lax.fori_loop(0, chunks, gated_chunk, 0)

    acc = kg[pl.ds(s * cps, cps)]
    for j in range(1, S):
        arrived(krecv.at[j], ids["kg"] + j)
        acc = acc + krecv[j]
    ksum[...] = acc
    for j in range(1, N):
        send(ksum, k2recv.at[j], ids["k2"] + j, s, lax.rem(d + j, N))
    for j in range(1, N):
        arrived(k2recv.at[j], ids["k2"] + j)
        acc = acc + k2recv[j]
    for c in range(cps):
        cols = slice(c * LANES, (c + 1) * LANES)
        kout[:, cols] = (acc[c] * factor)[:K]
        gout[:, cols] = (acc[c] * factor)[K : K + 1]

    home = me // S
    for q in range(S):
        @pl.when(jnp.logical_or(q != s, home != d))
        def _():
            arrived(rbuf.at[q], ids["rs"] + q)

    def sum_tile(n, _):
        cols = pl.ds(pl.multiple_of(n * LANES, LANES), LANES)
        acc = rbuf[0, :, cols].astype(f32)
        for q in range(1, S):
            acc = acc + rbuf[q, :, cols].astype(f32)
        gw[:, cols] = acc * factor
        return _

    lax.fori_loop(0, chunks, sum_tile, 0)
    for j in range(S):
        owner, rows, c = block_of(j)

        @pl.when(owner != me)
        def _():
            c.wait_send()

    for c in waits:
        c.wait_send()


def pair_kernel(
    S, N, Y, T, C, K, HB, ids,
    cot_in, val_in, gate_in, w_in, taps,
    gv_out, gg_out, gw, kout, gout,
    cot, val, gate, w, w_p, cot_m, cot_p, fsend, frecv, bsend, brecv, ext, cen, gc, gext, kall,
    act, act_m, act_p, ga_s, ga, wacc, wpart, yrecv, ysum, zrecv, fin, fbuf, gv, gg,
    kg, krecv, ksum, k2recv, send_sem, recv_sem, load_sem, store_sem,
):
    s = lax.axis_index("sp")
    d = lax.axis_index("dp")
    X, Z, H = N // 2, S // Y, C // 2
    x, c = d // 2, lax.rem(d, 2)
    y, z = lax.rem(s, Y), s // Y
    other = 1 - c
    partner = d + 1 - 2 * c
    chunks = C // LANES
    cps = chunks // S
    cpd = chunks // N
    block = C // (S * N)
    M = chunks // X
    RB = min(T, 128)
    PT = T // HALVES
    factor = float(S * N * T) ** (-0.5)
    waits = []

    def copy(src, dst, i, to_s, to_d, j=None):
        return pltpu.make_async_remote_copy(
            src_ref=src, dst_ref=dst, send_sem=send_sem.at[i],
            recv_sem=recv_sem.at[i if j is None else j],
            device_id={"sp": to_s, "dp": to_d}, device_id_type=pl.DeviceIdType.MESH,
        )

    def send(src, dst, i, to_s, to_d, j=None):
        r = copy(src, dst, i, to_s, to_d, j)
        r.start()
        waits.append(r)

    def arrived(dst, i):
        copy(dst, dst, i, s, partner).wait_recv()

    loads = [
        pltpu.make_async_copy(a, b, load_sem.at[i])
        for i, (a, b) in enumerate(((gate_in, gate), (val_in, val), (cot_in, cot), (w_in, w)))
    ]
    for l in loads:
        l.start()

    barrier = pltpu.get_barrier_semaphore()

    def greet_s(j, _):
        pl.semaphore_signal(
            barrier, inc=1, device_id={"sp": lax.rem(s + j, S), "dp": d},
            device_id_type=pl.DeviceIdType.MESH,
        )
        return _

    def greet_d(j, _):
        pl.semaphore_signal(
            barrier, inc=1, device_id={"sp": s, "dp": lax.rem(d + j, N)},
            device_id_type=pl.DeviceIdType.MESH,
        )
        return _

    lax.fori_loop(1, N, greet_d, 0)
    lax.fori_loop(1, S, greet_s, 0)
    loads[0].wait()
    loads[1].wait()

    def gate_chunk(cb, _):
        cols = pl.ds(pl.multiple_of(cb * LANES, LANES), LANES)
        sig = jax.nn.sigmoid(gate[:, cols].astype(f32))
        gated = (val[:, cols].astype(f32) * sig).astype(bf16)
        ext[cb, pl.ds(HB, T), :] = gated.astype(f32)
        fsend[cb] = gated[T - HB :]
        return _

    with jax.named_scope("gate"):
        lax.fori_loop(0, chunks, gate_chunk, 0)
    loads[2].wait()
    with jax.named_scope("barrierwait"):
        pl.semaphore_wait(barrier, S + N - 2)

    for j in range(1, S):
        send(taps, kall.at[pl.ds(s * cps, cps)], ids["taps"] + j, lax.rem(s + j, S), d)
    front = copy(fsend, frecv, ids["front"], lax.rem(s + 1, S), d)

    @pl.when(s < S - 1)
    def _():
        front.start()

    for j in range(1, X):
        for h in range(HALVES):
            rows = pl.ds(h * PT, PT)
            send(
                cot.at[rows], cot_m.at[j - 1, rows], ids["cot"] + j * HALVES + h,
                s, lax.rem(d + 2 * j, N),
            )
    half = pl.ds(pl.multiple_of(c * H, LANES), H)
    ohalf = pl.ds(pl.multiple_of(other * H, LANES), H)
    loads[3].wait()
    send(w, w_p, ids["w"], s, partner)
    send(cot.at[:, ohalf], cot_p.at[0], ids["cotp"], s, partner)
    kall[pl.ds(s * cps, cps)] = taps[...]

    def project(rows_of, weights, out, base):
        def pair(m, _):
            rows = pl.ds(pl.multiple_of(m * 2 * LANES, 2 * LANES), 2 * LANES)
            prod = lax.dot_general(
                rows_of[...], weights[rows, :], (((1,), (1,)), ((), ())), preferred_element_type=f32
            ).astype(bf16)
            out[base + 2 * m] = prod[:, :LANES]
            out[base + 2 * m + 1] = prod[:, LANES:]
            return _

        lax.fori_loop(0, cpd // 2, pair, 0)

    with jax.named_scope("proj_own"):
        project(cot, w, ga, d * cpd)
    with jax.named_scope("tapswait"):
        for j in range(1, S):
            arrived(kall.at[pl.ds(lax.rem(s + S - j, S) * cps, cps)], ids["taps"] + j)

        @pl.when(s > 0)
        def _():
            arrived(frecv, ids["front"])

    @pl.when(s == 0)
    def _():
        ext[:, pl.ds(0, HB), :] = jnp.zeros((chunks, HB, LANES), f32)

    @pl.when(s > 0)
    def _():
        ext[:, pl.ds(0, HB), :] = frecv[...].astype(f32)

    def conv_chunk(cb, sums):
        tf = kall[cb].astype(f32)
        parts = []
        for rb in range(T // RB):
            acc = jnp.zeros((RB, LANES), f32)
            for k in range(K):
                acc = acc + tf[k : k + 1] * ext[cb, pl.ds(HB - k + rb * RB, RB), :]
            cen[cb, pl.ds(rb * RB, RB), :] = acc
            parts.append(jnp.sum(acc, axis=1, keepdims=True))
        return sums + jnp.concatenate(parts, axis=0)

    column = jnp.zeros((T, 1), f32)
    with jax.named_scope("conv"):
        mean = lax.fori_loop(0, chunks, conv_chunk, column) / C

    def square_chunk(cb, sums):
        dev = cen[cb] - mean
        return sums + dev * dev

    with jax.named_scope("square"):
        squares = lax.fori_loop(0, chunks, square_chunk, jnp.zeros((T, LANES), f32))
    inv = lax.rsqrt(jnp.sum(squares, axis=1, keepdims=True) / C + epsilon)

    def act_chunk(cb, _):
        centred = (cen[cb] - mean) * inv
        cen[cb] = centred
        normed = centred * kall[cb].astype(f32)[K : K + 1]
        act[lax.rem(cb, X), cb // X] = (normed * jax.nn.sigmoid(normed)).astype(bf16)
        return _

    with jax.named_scope("act"):
        lax.fori_loop(0, chunks, act_chunk, 0)
    for j in range(1, X):
        send(act.at[lax.rem(x + j, X)], act_m.at[j - 1], ids["act"] + j, s, lax.rem(d + 2 * j, N))
    send(act.at[x], act_p.at[0], ids["actp"], s, partner)

    with jax.named_scope("proj_p"):
        arrived(w_p, ids["w"])
        project(cot, w_p, ga, partner * cpd)

    dims = (((0,), (0,)), ((), ()))
    NT = min(H, 512)
    tiles = H // NT

    def dot(a, b):
        return lax.dot_general(a, b, dims, preferred_element_type=f32)

    def local_tile(i, _):
        m, n = i // tiles, lax.rem(i, tiles)
        cols = pl.ds(pl.multiple_of(n * NT, NT), NT)
        own = pl.ds(pl.multiple_of(c * H + n * NT, NT), NT)
        wacc[m, :, cols] = dot(act[x, m], cot[:, own]) + dot(act_p[0, m], cot_p[0, :, cols])
        return _

    with jax.named_scope("wlocalwait"):
        arrived(cot_p.at[0], ids["cotp"])
        arrived(act_p.at[0], ids["actp"])
    with jax.named_scope("wlocal"):
        lax.fori_loop(0, M * tiles, local_tile, 0)

    for h in range(HALVES):
        rows = pl.ds(h * PT, PT)
        for j in range(1, X):
            with jax.named_scope("cotwait"):
                arrived(cot_m.at[j - 1, rows], ids["cot"] + j * HALVES + h)
            send(
                cot_m.at[j - 1, rows, ohalf], cot_p.at[j, rows], ids["cotp"] + j * HALVES + h,
                s, partner,
            )
            with jax.named_scope("proj_m"):
                piece = ga_s.at[j - 1, :, rows]
                project(cot_m.at[j - 1, rows], w, piece, c * cpd)
                project(cot_m.at[j - 1, rows], w_p, piece, other * cpd)
            send(
                piece, ga.at[pl.ds(x * 2 * cpd, 2 * cpd), rows], ids["ga"] + j * HALVES + h,
                s, lax.rem(d + 2 * (X - j), N),
            )

    with jax.named_scope("actwait"):
        for j in range(1, X):
            arrived(act_m.at[j - 1], ids["act"] + j)
            send(act_m.at[j - 1], act_p.at[j], ids["actp"] + j, s, partner)
        for j in range(1, X):
            arrived(act_p.at[j], ids["actp"] + j)
            for h in range(HALVES):
                arrived(cot_p.at[j, pl.ds(h * PT, PT)], ids["cotp"] + j * HALVES + h)

    def remote_part(m, n):
        cols = pl.ds(pl.multiple_of(n * NT, NT), NT)
        own = pl.ds(pl.multiple_of(c * H + n * NT, NT), NT)
        acc = wacc[m, :, cols]
        for j in range(1, X):
            acc = acc + dot(act_m[j - 1, m], cot_m[j - 1, :, own]) + dot(act_p[j, m], cot_p[j, :, cols])
        return cols, acc

    def plane(k):
        return jnp.where(z < Z // 2, lax.rem(z + Z - 1 - k, Z), lax.rem(z + 1 + k, Z))

    with jax.named_scope("wremote"):
        for k in range(Z):
            for j in range(1, Y):
                to_y = lax.rem(y + j, Y)
                m = plane(k) * Y + to_y
                i = (j - 1) * Z + k

                def send_tile(n, _):
                    cols, acc = remote_part(m, n)
                    wpart[i, :, cols] = acc.astype(bf16)
                    return _

                lax.fori_loop(0, tiles, send_tile, 0)
                send(wpart.at[i], yrecv.at[i], ids["y"] + i, z * Y + to_y, d)

        def own_tile(i, _):
            m = (i // tiles) * Y + y
            cols, acc = remote_part(m, lax.rem(i, tiles))
            wacc[m, :, cols] = acc
            return _

        lax.fori_loop(0, Z * tiles, own_tile, 0)

    def reduce_y(k):
        with jax.named_scope("ywait%d" % k):
            for j in range(1, Y):
                arrived(yrecv.at[(j - 1) * Z + k], ids["y"] + (j - 1) * Z + k)
        to_z = plane(k)
        m = to_z * Y + y

        def tile(n, _):
            cols = pl.ds(pl.multiple_of(n * LANES, LANES), LANES)
            acc = wacc[m, :, cols]
            for j in range(1, Y):
                acc = acc + yrecv[(j - 1) * Z + k, :, cols].astype(f32)
            if k < Z - 1:
                ysum[k, :, cols] = acc.astype(bf16)
            else:
                wacc[m, :, cols] = acc
            return _

        lax.fori_loop(0, H // LANES, tile, 0)
        if k < Z - 1:
            slot = lax.rem(z - to_z + Z, Z)
            send(ysum.at[k], zrecv.at[slot - 1], ids["z"] + 1 + k, to_z * Y + y, d, ids["z"] + slot)

    with jax.named_scope("gawait"):
        for j in range(1, X):
            for h in range(HALVES):
                rows = pl.ds(h * PT, PT)
                origin = lax.rem(x + j, X)
                arrived(ga.at[pl.ds(origin * 2 * cpd, 2 * cpd), rows], ids["ga"] + j * HALVES + h)

    def grad_chunk(cb, sums):
        one, two = sums
        centred = cen[cb]
        gain = kall[cb].astype(f32)[K : K + 1]
        normed = centred * gain
        sg = jax.nn.sigmoid(normed)
        grad = ga[cb].astype(f32) * sg * (1.0 + normed * (1.0 - sg))
        kg[cb, pl.ds(K, 1), :] = jnp.sum(grad * centred, axis=0, keepdims=True)
        grad = grad * gain
        gc[cb] = grad
        return one + grad, two + grad * centred

    zero = jnp.zeros((T, LANES), f32)
    with jax.named_scope("gradchunk"):
        one, two = lax.fori_loop(0, chunks, grad_chunk, (zero, zero))
    first = jnp.sum(one, axis=1, keepdims=True) / C
    second = jnp.sum(two, axis=1, keepdims=True) / C

    def conv_grad(cb, _):
        grad = (gc[cb] - first - cen[cb] * second) * inv
        gext[cb, pl.ds(0, T), :] = grad
        bsend[cb] = grad[:HB].astype(bf16)
        return _

    with jax.named_scope("convgrad"):
        lax.fori_loop(0, chunks, conv_grad, 0)
    back = copy(bsend, brecv, ids["back"], lax.rem(s + S - 1, S), d)

    @pl.when(s > 0)
    def _():
        back.start()

    reduce_y(0)

    def taps_chunk(cb, _):
        for k in range(K):
            acc = jnp.zeros((8, LANES), f32)
            for rb in range(T // RB):
                prod = gext[cb, pl.ds(rb * RB, RB), :] * ext[cb, pl.ds(HB - k + rb * RB, RB), :]
                acc = acc + jnp.sum(prod.reshape(RB // 8, 8, LANES), axis=0)
            kg[cb, pl.ds(k, 1), :] = jnp.sum(acc, axis=0, keepdims=True)
        return _

    with jax.named_scope("taps"):
        lax.fori_loop(0, chunks, taps_chunk, 0)
    for j in range(1, S):
        to = lax.rem(s + j, S)
        send(kg.at[pl.ds(to * cps, cps)], krecv.at[j], ids["kg"] + j, to, d)
    for k in range(1, Z - 1):
        reduce_y(k)

    with jax.named_scope("backwait"):
        @pl.when(s < S - 1)
        def _():
            arrived(brecv, ids["back"])

    @pl.when(s == S - 1)
    def _():
        gext[:, pl.ds(T, HB), :] = jnp.zeros((chunks, HB, LANES), f32)

    @pl.when(s < S - 1)
    def _():
        gext[:, pl.ds(T, HB), :] = brecv[...].astype(f32)

    stores = []
    for rb in range(T // RB):
        rows = pl.ds(rb * RB, RB)

        def gated_chunk(cb, _):
            cols = pl.ds(pl.multiple_of(cb * LANES, LANES), LANES)
            tf = kall[cb].astype(f32)
            acc = jnp.zeros((RB, LANES), f32)
            for k in range(K):
                acc = acc + tf[k : k + 1] * gext[cb, pl.ds(k + rb * RB, RB), :]
            acc = acc.astype(bf16).astype(f32)
            sig = jax.nn.sigmoid(gate[rows, cols].astype(f32))
            gv[rows, cols] = (acc * sig).astype(bf16)
            gg[rows, cols] = (acc * val[rows, cols].astype(f32) * sig * (1.0 - sig)).astype(bf16)
            return _

        with jax.named_scope("gated"):
            lax.fori_loop(0, chunks, gated_chunk, 0)
        for i, (a, b) in enumerate(((gv, gv_out), (gg, gg_out))):
            st = pltpu.make_async_copy(a.at[rows], b.at[rows], store_sem.at[2 * rb + i])
            st.start()
            stores.append(st)

    reduce_y(Z - 1)

    with jax.named_scope("kgwait"):
        for j in range(1, S):
            arrived(krecv.at[j], ids["kg"] + j)
    acc = kg[pl.ds(s * cps, cps)]
    for j in range(1, S):
        acc = acc + krecv[j]
    ksum[...] = acc
    for j in range(1, N):
        send(ksum, k2recv.at[j], ids["k2"] + j, s, lax.rem(d + j, N))

    with jax.named_scope("zwait"):
        for j in range(1, Z):
            arrived(zrecv.at[j - 1], ids["z"] + j)

    def final_tile(n, _):
        cols = pl.ds(pl.multiple_of(n * LANES, LANES), LANES)
        acc = wacc[s, :, cols]
        for j in range(1, Z):
            acc = acc + zrecv[j - 1, :, cols].astype(f32)
        acc = acc * factor
        fin[0, :, cols] = acc[:block]
        fin[1, :, cols] = acc[block:]
        return _

    with jax.named_scope("final"):
        lax.fori_loop(0, H // LANES, final_tile, 0)
    send(fin.at[other], fbuf, ids["fin"], s, partner)
    gw[:, half] = fin[c]

    with jax.named_scope("k2wait"):
        for j in range(1, N):
            arrived(k2recv.at[j], ids["k2"] + j)
            acc = acc + k2recv[j]
    for q in range(cps):
        cols = slice(q * LANES, (q + 1) * LANES)
        kout[:, cols] = (acc[q] * factor)[:K]
        gout[:, cols] = (acc[q] * factor)[K : K + 1]

    arrived(fbuf, ids["fin"])
    gw[:, ohalf] = fbuf[...]
    for r in waits:
        r.wait_send()

    @pl.when(s < S - 1)
    def _():
        front.wait_send()

    @pl.when(s > 0)
    def _():
        back.wait_send()

    for st in stores:
        st.wait()


def number(*sizes):
    ids, count = {}, 0
    for name, size in sizes:
        ids[name] = count
        count += size
    return ids, count


def pair_call(S, N, Y, T, C, K, HB, KP, cot, val, gate, w, packed):
    X, Z, H = N // 2, S // Y, C // 2
    chunks, cps, cpd, block = C // LANES, C // LANES // S, C // LANES // N, C // (S * N)
    M, CR = chunks // X, C // N
    ids, count = number(
        ("taps", S), ("front", 1), ("back", 1), ("w", 1), ("cot", X * HALVES), ("cotp", X * HALVES),
        ("act", X), ("actp", X), ("ga", X * HALVES), ("y", (Y - 1) * Z), ("z", Z), ("fin", 1),
        ("kg", S), ("k2", N),
    )
    vm = pl.BlockSpec(memory_space=pltpu.VMEM)
    hbm = pl.BlockSpec(memory_space=pl.ANY)
    return pl.pallas_call(
        functools.partial(pair_kernel, S, N, Y, T, C, K, HB, ids),
        out_shape=(
            jax.ShapeDtypeStruct((T, C), bf16),
            jax.ShapeDtypeStruct((T, C), bf16),
            jax.ShapeDtypeStruct((block, C), f32),
            jax.ShapeDtypeStruct((K, C // S), f32),
            jax.ShapeDtypeStruct((1, C // S), f32),
        ),
        in_specs=[hbm] * 4 + [vm],
        out_specs=(hbm, hbm, vm, vm, vm),
        scratch_shapes=[
            pltpu.VMEM((T, C), bf16),
            pltpu.VMEM((T, C), bf16),
            pltpu.VMEM((T, C), bf16),
            pltpu.VMEM((CR, C), bf16),
            pltpu.VMEM((CR, C), bf16),
            pltpu.VMEM((X - 1, T, C), bf16),
            pltpu.VMEM((X, T, H), bf16),
            pltpu.VMEM((chunks, HB, LANES), bf16),
            pltpu.VMEM((chunks, HB, LANES), bf16),
            pltpu.VMEM((chunks, HB, LANES), bf16),
            pltpu.VMEM((chunks, HB, LANES), bf16),
            pltpu.VMEM((chunks, T + HB, LANES), f32),
            pltpu.VMEM((chunks, T, LANES), f32),
            pltpu.VMEM((chunks, T, LANES), f32),
            pltpu.VMEM((chunks, T + HB, LANES), f32),
            pltpu.VMEM((chunks, KP, LANES), bf16),
            pltpu.VMEM((X, M, T, LANES), bf16),
            pltpu.VMEM((X - 1, M, T, LANES), bf16),
            pltpu.VMEM((X, M, T, LANES), bf16),
            pltpu.VMEM((X - 1, 2 * cpd, T, LANES), bf16),
            pltpu.VMEM((chunks, T, LANES), bf16),
            pltpu.VMEM((M, LANES, H), f32),
            pltpu.VMEM(((Y - 1) * Z, LANES, H), bf16),
            pltpu.VMEM(((Y - 1) * Z, LANES, H), bf16),
            pltpu.VMEM((Z - 1, LANES, H), bf16),
            pltpu.VMEM((Z - 1, LANES, H), bf16),
            pltpu.VMEM((2, block, H), f32),
            pltpu.VMEM((block, H), f32),
            pltpu.VMEM((T, C), bf16),
            pltpu.VMEM((T, C), bf16),
            pltpu.VMEM((chunks, KP, LANES), f32),
            pltpu.VMEM((S, cps, KP, LANES), f32),
            pltpu.VMEM((cps, KP, LANES), f32),
            pltpu.VMEM((N, cps, KP, LANES), f32),
            pltpu.SemaphoreType.DMA((count,)),
            pltpu.SemaphoreType.DMA((count,)),
            pltpu.SemaphoreType.DMA((4,)),
            pltpu.SemaphoreType.DMA((2 * (T // min(T, 128)),)),
        ],
        compiler_params=pltpu.CompilerParams(
            collective_id=0, has_side_effects=True, vmem_limit_bytes=62 * 1024 * 1024
        ),
        name="block_backward",
    )(cot, val, gate, w, packed)


def general_call(S, N, T, C, K, HB, KP, cot, val, gate, w, packed):
    chunks, cps, cpd, block = C // LANES, C // LANES // S, C // LANES // N, C // (S * N)
    ids, count = number(
        ("taps", S), ("front", 1), ("back", 1), ("partner", 1), ("mirror", N // 2 * HALVES),
        ("relay", N // 2 * HALVES), ("act", N), ("ga", N), ("rs", S), ("kg", S), ("k2", N),
    )
    vm = pl.BlockSpec(memory_space=pltpu.VMEM)
    return pl.pallas_call(
        functools.partial(general_kernel, S, N, T, C, K, HB, ids),
        out_shape=(
            jax.ShapeDtypeStruct((T, C), bf16),
            jax.ShapeDtypeStruct((T, C), bf16),
            jax.ShapeDtypeStruct((block, C), f32),
            jax.ShapeDtypeStruct((K, C // S), f32),
            jax.ShapeDtypeStruct((1, C // S), f32),
        ),
        in_specs=[vm] * 5,
        out_specs=(vm,) * 5,
        scratch_shapes=[
            pltpu.VMEM((N, T, C), bf16),
            pltpu.VMEM((chunks, T + HB, LANES), f32),
            pltpu.VMEM((chunks, T, LANES), f32),
            pltpu.VMEM((chunks, T, LANES), f32),
            pltpu.VMEM((chunks, T + HB, LANES), f32),
            pltpu.VMEM((chunks, KP, LANES), bf16),
            pltpu.VMEM((chunks, T, LANES), bf16),
            pltpu.VMEM((N, cpd, T, LANES), bf16),
            pltpu.VMEM((N, cpd, T, LANES), bf16),
            pltpu.VMEM((chunks, T, LANES), bf16),
            pltpu.VMEM((cpd * LANES, C), bf16),
            pltpu.VMEM((S, block, C), bf16),
            pltpu.VMEM((chunks, KP, LANES), f32),
            pltpu.VMEM((S, cps, KP, LANES), f32),
            pltpu.VMEM((cps, KP, LANES), f32),
            pltpu.VMEM((N, cps, KP, LANES), f32),
            pltpu.SemaphoreType.DMA((count,)),
            pltpu.SemaphoreType.DMA((count,)),
        ],
        compiler_params=pltpu.CompilerParams(
            collective_id=0, has_side_effects=True, vmem_limit_bytes=60 * 1024 * 1024
        ),
        name="block_backward",
    )(cot, val, gate, w, packed)


def shards(out_cotangent, value_pre, gate_pre, out_weight, conv_kernel, norm_gain):
    S, N = lax.axis_size("sp"), lax.axis_size("dp")
    _, T, C = out_cotangent.shape
    K = conv_kernel.shape[0]
    chunks, cps = C // LANES, C // LANES // S
    HB = -(-(K - 1) // 16) * 16
    KP = -(-(K + 1) // 16) * 16
    packed = jnp.concatenate(
        [conv_kernel, norm_gain[None], jnp.zeros((KP - K - 1, C // S), bf16)], axis=0
    )
    packed = jnp.transpose(packed.reshape(KP, cps, LANES), (1, 0, 2))
    args = (out_cotangent[0], value_pre[0], gate_pre[0], out_weight, packed)
    X = N // 2
    if N % 2 == 0 and X > 1 and S % X == 0 and S > X and chunks == S * X:
        outs = pair_call(S, N, X, T, C, K, HB, KP, *args)
    else:
        outs = general_call(S, N, T, C, K, HB, KP, *args)
    grad_value, grad_gate, grad_weight, grad_taps, grad_gain = outs
    return grad_value[None], grad_gate[None], grad_weight, grad_taps, grad_gain[0]


def solution(mesh):
    placed = (
        P("dp", "sp", None),
        P("dp", "sp", None),
        P("dp", "sp", None),
        P("dp", None),
        P(None, "sp"),
        P("sp"),
    )
    return jax.shard_map(
        shards,
        mesh=mesh,
        in_specs=placed,
        out_specs=(
            P("dp", "sp", None),
            P("dp", "sp", None),
            P(("sp", "dp"), None),
            P(None, "sp"),
            P("sp"),
        ),
        check_vma=False,
    )
```

```python
import functools

import jax
import jax.numpy as jnp
from jax import lax
from jax.experimental import pallas as pl
from jax.experimental.pallas import tpu as pltpu
from jax.sharding import PartitionSpec as P

epsilon = 1e-05
LANES = 128
HALVES = 2
BLOCKS = 4
f32 = jnp.float32
bf16 = jnp.bfloat16


def general_kernel(
    S, N, T, C, K, HB, ids,
    cot, val, gate, w, taps,
    gv, gg, gw, kout, gout,
    cot_all, ext, cen, gc, gext, kall, act, act_all, ga_send, ga, wpart, rbuf,
    kg, krecv, ksum, k2recv, send_sem, recv_sem,
):
    s = lax.axis_index("sp")
    d = lax.axis_index("dp")
    chunks = C // LANES
    cps = chunks // S
    cpd = chunks // N
    block = C // (S * N)
    RB = min(T, 128)
    total = S * N
    me = s * N + d
    partner = d + 1 - 2 * lax.rem(d, 2)
    factor = float(S * N * T) ** (-0.5)
    hrows = T // HALVES
    waits = []

    def copy(src, dst, i, to_s, to_d):
        return pltpu.make_async_remote_copy(
            src_ref=src, dst_ref=dst, send_sem=send_sem.at[i], recv_sem=recv_sem.at[i],
            device_id={"sp": to_s, "dp": to_d}, device_id_type=pl.DeviceIdType.MESH,
        )

    def send(src, dst, i, to_s, to_d):
        c = copy(src, dst, i, to_s, to_d)
        c.start()
        waits.append(c)

    def arrived(dst, i):
        copy(dst, dst, i, s, partner).wait_recv()

    barrier = pltpu.get_barrier_semaphore()

    def greet(j, _):
        other = lax.rem(me + j, total)
        pl.semaphore_signal(
            barrier, inc=1, device_id={"sp": other // N, "dp": lax.rem(other, N)},
            device_id_type=pl.DeviceIdType.MESH,
        )
        return _

    lax.fori_loop(1, total, greet, 0)
    def gate_chunk(cb, _):
        cols = pl.ds(pl.multiple_of(cb * LANES, LANES), LANES)
        sig = jax.nn.sigmoid(gate[:, cols].astype(f32))
        ext[cb, pl.ds(HB, T), :] = (val[:, cols].astype(f32) * sig).astype(bf16).astype(f32)
        return _

    lax.fori_loop(0, chunks, gate_chunk, 0)
    pl.semaphore_wait(barrier, total - 1)

    for j in range(1, S):
        send(taps, kall.at[pl.ds(s * cps, cps)], ids["taps"] + j, lax.rem(s + j, S), d)
    following = lax.rem(s + 1, S)
    preceding = lax.rem(s + S - 1, S)
    send(ext.at[:, pl.ds(T, HB), :], ext.at[:, pl.ds(0, HB), :], ids["front"], following, d)
    for j in range(1, N // 2):
        for h in range(HALVES):
            rows = pl.ds(h * hrows, hrows)
            send(cot.at[rows], cot_all.at[d, rows], ids["mirror"] + j * HALVES + h, s, lax.rem(d + 2 * j, N))
    send(cot, cot_all.at[d], ids["partner"], s, partner)
    kall[pl.ds(s * cps, cps)] = taps[...]
    cot_all[d] = cot[...]
    for j in range(1, S):
        arrived(kall.at[pl.ds(lax.rem(s + S - j, S) * cps, cps)], ids["taps"] + j)
    arrived(ext.at[:, pl.ds(0, HB), :], ids["front"])

    @pl.when(s == 0)
    def _():
        ext[:, pl.ds(0, HB), :] = jnp.zeros((chunks, HB, LANES), f32)

    def conv_chunk(cb, sums):
        tf = kall[cb].astype(f32)
        parts = []
        for rb in range(T // RB):
            acc = jnp.zeros((RB, LANES), f32)
            for k in range(K):
                acc = acc + tf[k : k + 1] * ext[cb, pl.ds(HB - k + rb * RB, RB), :]
            cen[cb, pl.ds(rb * RB, RB), :] = acc
            parts.append(jnp.sum(acc, axis=1, keepdims=True))
        return sums + jnp.concatenate(parts, axis=0)

    column = jnp.zeros((T, 1), f32)
    mean = lax.fori_loop(0, chunks, conv_chunk, column) / C

    def square_chunk(cb, sums):
        dev = cen[cb] - mean
        return sums + dev * dev

    squares = lax.fori_loop(0, chunks, square_chunk, jnp.zeros((T, LANES), f32))
    inv = lax.rsqrt(jnp.sum(squares, axis=1, keepdims=True) / C + epsilon)

    def relay():
        for j in range(1, N // 2):
            origin = lax.rem(d + N - 2 * j, N)
            for h in range(HALVES):
                piece = cot_all.at[origin, pl.ds(h * hrows, hrows)]
                arrived(piece, ids["mirror"] + j * HALVES + h)
                send(piece, piece, ids["relay"] + j * HALVES + h, s, partner)

    def act_chunk(cb, _):
        centred = (cen[cb] - mean) * inv
        cen[cb] = centred
        normed = centred * kall[cb].astype(f32)[K : K + 1]
        act[cb] = (normed * jax.nn.sigmoid(normed)).astype(bf16)
        return _

    lax.fori_loop(0, chunks, act_chunk, 0)
    for j in range(1, N):
        to = lax.rem(d + j, N)
        send(act.at[pl.ds(to * cpd, cpd)], act_all.at[d], ids["act"] + j, s, to)
    act_all[d] = act[pl.ds(d * cpd, cpd)]

    def project(source, slot):
        def pair(m, _):
            rows = pl.ds(pl.multiple_of(m * 2 * LANES, 2 * LANES), 2 * LANES)
            out = lax.dot_general(
                cot_all[source], w[rows, :], (((1,), (1,)), ((), ())), preferred_element_type=f32
            ).astype(bf16)
            ga_send[slot, 2 * m] = out[:, :LANES]
            ga_send[slot, 2 * m + 1] = out[:, LANES:]
            return _

        lax.fori_loop(0, cpd // 2, pair, 0)

    mine = pl.ds(d * cpd, cpd)
    project(d, 0)
    ga[mine] = ga_send[0]
    arrived(cot_all.at[partner], ids["partner"])
    project(partner, 1)
    send(ga_send.at[1], ga.at[mine], ids["ga"] + 1, s, partner)
    relay()
    for j in range(1, N // 2):
        origin = lax.rem(d + N - 2 * j, N)
        project(origin, 2 * j)
        send(ga_send.at[2 * j], ga.at[mine], ids["ga"] + 2 * j, s, origin)
    for j in range(1, N // 2):
        origin = lax.rem(partner + N - 2 * j, N)
        for h in range(HALVES):
            arrived(cot_all.at[origin, pl.ds(h * hrows, hrows)], ids["relay"] + j * HALVES + h)
        project(origin, 2 * j + 1)
        send(ga_send.at[2 * j + 1], ga.at[mine], ids["ga"] + 2 * j + 1, s, origin)

    for j in range(1, N):
        arrived(act_all.at[lax.rem(d + N - j, N)], ids["act"] + j)
    NT = min(C, 512)

    def weight_tile(i, _):
        m, n = i // (C // NT), lax.rem(i, C // NT)
        cols = pl.ds(pl.multiple_of(n * NT, NT), NT)
        acc = jnp.zeros((LANES, NT), f32)
        for q in range(N):
            acc = acc + lax.dot_general(
                act_all[q, m], cot_all[q, :, cols], (((0,), (0,)), ((), ())),
                preferred_element_type=f32,
            )
        wpart[pl.ds(pl.multiple_of(m * LANES, LANES), LANES), cols] = acc.astype(bf16)
        return _

    lax.fori_loop(0, cpd * (C // NT), weight_tile, 0)

    def block_of(j):
        i = lax.rem(s + j, S)
        owner = d * S + i
        rows = pl.ds(pl.multiple_of(i * block, block), block)
        return owner, rows, pltpu.make_async_remote_copy(
            src_ref=wpart.at[rows], dst_ref=rbuf.at[s], send_sem=send_sem.at[ids["rs"] + j],
            recv_sem=recv_sem.at[ids["rs"] + s],
            device_id={"sp": owner // N, "dp": lax.rem(owner, N)},
            device_id_type=pl.DeviceIdType.MESH,
        )

    def send_blocks(first, last):
        for j in range(first, last):
            owner, rows, c = block_of(j)

            @pl.when(owner != me)
            def _():
                c.start()

            @pl.when(owner == me)
            def _():
                rbuf[s] = wpart[rows, :]

    send_blocks(0, S // 2)

    for j in range(1, N // 2):
        arrived(ga.at[pl.ds(lax.rem(d + 2 * j, N) * cpd, cpd)], ids["ga"] + 2 * j)
        arrived(ga.at[pl.ds(lax.rem(partner + 2 * j, N) * cpd, cpd)], ids["ga"] + 2 * j + 1)
    arrived(ga.at[pl.ds(partner * cpd, cpd)], ids["ga"] + 1)

    def grad_chunk(cb, sums):
        one, two = sums
        centred = cen[cb]
        gain = kall[cb].astype(f32)[K : K + 1]
        normed = centred * gain
        sg = jax.nn.sigmoid(normed)
        grad = ga[cb].astype(f32) * sg * (1.0 + normed * (1.0 - sg))
        kg[cb, pl.ds(K, 1), :] = jnp.sum(grad * centred, axis=0, keepdims=True)
        grad = grad * gain
        gc[cb] = grad
        return one + grad, two + grad * centred

    zero = jnp.zeros((T, LANES), f32)
    one, two = lax.fori_loop(0, chunks, grad_chunk, (zero, zero))
    first = jnp.sum(one, axis=1, keepdims=True) / C
    second = jnp.sum(two, axis=1, keepdims=True) / C

    def conv_grad(cb, _):
        gext[cb, pl.ds(0, T), :] = (gc[cb] - first - cen[cb] * second) * inv
        return _

    lax.fori_loop(0, chunks, conv_grad, 0)
    send(gext.at[:, pl.ds(0, HB), :], gext.at[:, pl.ds(T, HB), :], ids["back"], preceding, d)

    def taps_chunk(cb, _):
        for k in range(K):
            acc = jnp.zeros((8, LANES), f32)
            for rb in range(T // RB):
                prod = gext[cb, pl.ds(rb * RB, RB), :] * ext[cb, pl.ds(HB - k + rb * RB, RB), :]
                acc = acc + jnp.sum(prod.reshape(RB // 8, 8, LANES), axis=0)
            kg[cb, pl.ds(k, 1), :] = jnp.sum(acc, axis=0, keepdims=True)
        return _

    lax.fori_loop(0, chunks, taps_chunk, 0)
    for j in range(1, S):
        to = lax.rem(s + j, S)
        send(kg.at[pl.ds(to * cps, cps)], krecv.at[j], ids["kg"] + j, to, d)
    send_blocks(S // 2, S)

    arrived(gext.at[:, pl.ds(T, HB), :], ids["back"])

    @pl.when(s == S - 1)
    def _():
        gext[:, pl.ds(T, HB), :] = jnp.zeros((chunks, HB, LANES), f32)

    def gated_chunk(cb, _):
        cols = pl.ds(pl.multiple_of(cb * LANES, LANES), LANES)
        tf = kall[cb].astype(f32)
        for rb in range(T // RB):
            rows = pl.ds(rb * RB, RB)
            acc = jnp.zeros((RB, LANES), f32)
            for k in range(K):
                acc = acc + tf[k : k + 1] * gext[cb, pl.ds(k + rb * RB, RB), :]
            acc = acc.astype(bf16).astype(f32)
            sig = jax.nn.sigmoid(gate[rows, cols].astype(f32))
            gv[rows, cols] = (acc * sig).astype(bf16)
            gg[rows, cols] = (acc * val[rows, cols].astype(f32) * sig * (1.0 - sig)).astype(bf16)
        return _

    lax.fori_loop(0, chunks, gated_chunk, 0)

    acc = kg[pl.ds(s * cps, cps)]
    for j in range(1, S):
        arrived(krecv.at[j], ids["kg"] + j)
        acc = acc + krecv[j]
    ksum[...] = acc
    for j in range(1, N):
        send(ksum, k2recv.at[j], ids["k2"] + j, s, lax.rem(d + j, N))
    for j in range(1, N):
        arrived(k2recv.at[j], ids["k2"] + j)
        acc = acc + k2recv[j]
    for c in range(cps):
        cols = slice(c * LANES, (c + 1) * LANES)
        kout[:, cols] = (acc[c] * factor)[:K]
        gout[:, cols] = (acc[c] * factor)[K : K + 1]

    home = me // S
    for q in range(S):
        @pl.when(jnp.logical_or(q != s, home != d))
        def _():
            arrived(rbuf.at[q], ids["rs"] + q)

    def sum_tile(n, _):
        cols = pl.ds(pl.multiple_of(n * LANES, LANES), LANES)
        acc = rbuf[0, :, cols].astype(f32)
        for q in range(1, S):
            acc = acc + rbuf[q, :, cols].astype(f32)
        gw[:, cols] = acc * factor
        return _

    lax.fori_loop(0, chunks, sum_tile, 0)
    for j in range(S):
        owner, rows, c = block_of(j)

        @pl.when(owner != me)
        def _():
            c.wait_send()

    for c in waits:
        c.wait_send()


def pair_kernel(
    S, N, Y, T, C, K, HB, ids,
    cot_in, val_in, gate_in, w_in, kernel, gain,
    gv_out, gg_out, gw, kout,
    taps, cot, val, gate, w, w_p, cot_m, cot_p, fsend, frecv, bsend, brecv, ext, cen, gc, gext, kall,
    act, act_m, act_p, ga_s, ga, wacc, wpart, yrecv, ysum, zmid, zrecv, fin, fbuf, gv, gg,
    invs, kacc, kg, kgb, krecv, ksum, k2recv, send_sem, recv_sem, load_sem, store_sem, ready,
):
    s = lax.axis_index("sp")
    d = lax.axis_index("dp")
    X, Z, H = N // 2, S // Y, C // 2
    x, c = d // 2, lax.rem(d, 2)
    y, z = lax.rem(s, Y), s // Y
    other = 1 - c
    partner = d + 1 - 2 * c
    chunks = C // LANES
    cps = chunks // S
    cpd = chunks // N
    block = C // (S * N)
    M = chunks // X
    RB = min(T, 128)
    TB = T // BLOCKS
    factor = float(S * N * T) ** (-0.5)
    waits = []

    def copy(src, dst, i, to_s, to_d, j=None):
        return pltpu.make_async_remote_copy(
            src_ref=src, dst_ref=dst, send_sem=send_sem.at[i],
            recv_sem=recv_sem.at[i if j is None else j],
            device_id={"sp": to_s, "dp": to_d}, device_id_type=pl.DeviceIdType.MESH,
        )

    def send(src, dst, i, to_s, to_d, j=None):
        r = copy(src, dst, i, to_s, to_d, j)
        r.start()
        waits.append(r)

    def arrived(dst, i):
        copy(dst, dst, i, s, partner).wait_recv()

    loads = [
        pltpu.make_async_copy(a, b, load_sem.at[i])
        for i, (a, b) in enumerate(((gate_in, gate), (val_in, val), (cot_in, cot), (w_in, w)))
    ]
    for l in loads:
        l.start()

    barrier = pltpu.get_barrier_semaphore()

    def signal(sem, to_s, to_d):
        pl.semaphore_signal(
            sem, inc=1, device_id={"sp": to_s, "dp": to_d}, device_id_type=pl.DeviceIdType.MESH
        )

    def along_z(action):
        @pl.when(z > 0)
        def _():
            action(0, s - Y)

        @pl.when(z < Z - 1)
        def _():
            action(1, s + Y)

    signal(barrier, s, partner)
    for j in range(1, X):
        signal(barrier, s, lax.rem(d + 2 * j, N))
    for j in range(1, Y):
        signal(barrier, z * Y + lax.rem(y + j, Y), d)
    along_z(lambda side, to_s: signal(barrier, to_s, d))
    KP = taps.shape[1]
    for q in range(cps):
        cols = slice(q * LANES, (q + 1) * LANES)
        taps[q] = jnp.concatenate(
            [kernel[:, cols].astype(f32), gain[cols].astype(f32).reshape(1, LANES)]
            + [jnp.zeros((KP - K - 1, LANES), f32)] * (KP > K + 1),
            axis=0,
        ).astype(bf16)
    loads[0].wait()
    loads[1].wait()

    def gate_chunk(cb, _):
        cols = pl.ds(pl.multiple_of(cb * LANES, LANES), LANES)
        sig = jax.nn.sigmoid(gate[:, cols].astype(f32))
        gated = (val[:, cols].astype(f32) * sig).astype(bf16)
        ext[cb, pl.ds(HB, T), :] = gated.astype(f32)
        fsend[cb] = gated[T - HB :]
        return _

    with jax.named_scope("gate"):
        lax.fori_loop(0, chunks, gate_chunk, 0)
    loads[2].wait()
    with jax.named_scope("barrierwait"):
        pl.semaphore_wait(barrier, X + Y - 1 + jnp.where(z > 0, 1, 0) + jnp.where(z < Z - 1, 1, 0))

    for j in range(1, X):
        for b in range(BLOCKS):
            rows = pl.ds(b * TB, TB)
            send(
                cot.at[rows], cot_m.at[j - 1, rows], ids["cot"] + j * BLOCKS + b,
                s, lax.rem(d + 2 * j, N),
            )
    half = pl.ds(pl.multiple_of(c * H, LANES), H)
    ohalf = pl.ds(pl.multiple_of(other * H, LANES), H)
    loads[3].wait()
    send(w, w_p, ids["w"], s, partner)
    send(cot.at[:, ohalf], cot_p.at[0], ids["cotp"], s, partner)
    kall[pl.ds(s * cps, cps)] = taps[...]
    with jax.named_scope("ready"):
        for r in range(Z - 2):
            along_z(lambda side, to_s: signal(ready.at[2 * r + 1 - side], to_s, d))
            along_z(lambda side, to_s: pl.semaphore_wait(ready.at[2 * r + side], 1))
        for j in range(1, Y):
            signal(ready.at[2 * (Z - 2)], z * Y + lax.rem(y + j, Y), d)
        pl.semaphore_wait(ready.at[2 * (Z - 2)], Y - 1)
    for j in range(1, S):
        send(taps, kall.at[pl.ds(s * cps, cps)], ids["taps"] + j, lax.rem(s + j, S), d)
    front = copy(fsend, frecv, ids["front"], lax.rem(s + 1, S), d)

    @pl.when(s < S - 1)
    def _():
        front.start()


    def project(rows_of, weights, out, base):
        def pair(m, _):
            rows = pl.ds(pl.multiple_of(m * 2 * LANES, 2 * LANES), 2 * LANES)
            prod = lax.dot_general(
                rows_of[...], weights[rows, :], (((1,), (1,)), ((), ())), preferred_element_type=f32
            ).astype(bf16)
            out[base + 2 * m] = prod[:, :LANES]
            out[base + 2 * m + 1] = prod[:, LANES:]
            return _

        lax.fori_loop(0, cpd // 2, pair, 0)

    with jax.named_scope("proj_own"):
        project(cot, w, ga, d * cpd)
    with jax.named_scope("tapswait"):
        for j in range(1, S):
            arrived(kall.at[pl.ds(lax.rem(s + S - j, S) * cps, cps)], ids["taps"] + j)

        @pl.when(s > 0)
        def _():
            arrived(frecv, ids["front"])

    @pl.when(s == 0)
    def _():
        ext[:, pl.ds(0, HB), :] = jnp.zeros((chunks, HB, LANES), f32)

    @pl.when(s > 0)
    def _():
        ext[:, pl.ds(0, HB), :] = frecv[...].astype(f32)

    def conv_chunk(cb, sums):
        tf = kall[cb].astype(f32)
        parts = []
        for rb in range(T // RB):
            acc = jnp.zeros((RB, LANES), f32)
            for k in range(K):
                acc = acc + tf[k : k + 1] * ext[cb, pl.ds(HB - k + rb * RB, RB), :]
            cen[cb, pl.ds(rb * RB, RB), :] = acc
            parts.append(jnp.sum(acc, axis=1, keepdims=True))
        return sums + jnp.concatenate(parts, axis=0)

    column = jnp.zeros((T, 1), f32)
    with jax.named_scope("conv"):
        mean = lax.fori_loop(0, chunks, conv_chunk, column) / C

    def square_chunk(cb, sums):
        dev = cen[cb] - mean
        return sums + dev * dev

    with jax.named_scope("square"):
        squares = lax.fori_loop(0, chunks, square_chunk, jnp.zeros((T, LANES), f32))
    inv = lax.rsqrt(jnp.sum(squares, axis=1, keepdims=True) / C + epsilon)

    def act_chunk(cb, _):
        centred = (cen[cb] - mean) * inv
        cen[cb] = centred
        normed = centred * kall[cb].astype(f32)[K : K + 1]
        act[lax.rem(cb, X), cb // X] = (normed * jax.nn.sigmoid(normed)).astype(bf16)
        return _

    with jax.named_scope("act"):
        lax.fori_loop(0, chunks, act_chunk, 0)
    invs[...] = jnp.broadcast_to(inv, (T, LANES))
    send(act.at[x], act_p.at[0], ids["actp"], s, partner)

    near = Z // 2
    low = z < near
    inner_z = jnp.where(low, near - 1, near)
    inner = z == inner_z

    def plane(k):
        if k < near:
            return jnp.where(low, Z - 1 - k, k)
        return jnp.where(low, 0, near) + lax.rem(z + 1 + k, near)

    def send_act(k):
        piece = pl.ds(plane(k) * Y, Y)
        for j in range(1, X):
            send(
                act.at[lax.rem(x + j, X), piece], act_m.at[j - 1, piece], ids["act"] + j * Z + k,
                s, lax.rem(d + 2 * j, N),
            )

    def relay_mirror(b):
        rows = pl.ds(b * TB, TB)
        for j in range(1, X):
            with jax.named_scope("cotwait%d" % b):
                arrived(cot_m.at[j - 1, rows], ids["cot"] + j * BLOCKS + b)
            send(
                cot_m.at[j - 1, rows, ohalf], cot_p.at[j, rows], ids["cotp"] + j * BLOCKS + b,
                s, partner,
            )

    def project_mirror(b):
        rows = pl.ds(b * TB, TB)
        for j in range(1, X):
            with jax.named_scope("proj_m%d" % b):
                piece = ga_s.at[j - 1, :, rows]
                project(cot_m.at[j - 1, rows], w, piece, c * cpd)
                project(cot_m.at[j - 1, rows], w_p, piece, other * cpd)
            send(
                piece, ga.at[pl.ds(x * 2 * cpd, 2 * cpd), rows], ids["ga"] + j * BLOCKS + b,
                s, lax.rem(d + 2 * (X - j), N),
            )

    dims = (((0,), (0,)), ((), ()))
    NT = min(H, 512)
    tiles = H // NT

    def dot(a, b):
        return lax.dot_general(a, b, dims, preferred_element_type=f32)

    def local_part(m, n):
        cols = pl.ds(pl.multiple_of(n * NT, NT), NT)
        own = pl.ds(pl.multiple_of(c * H + n * NT, NT), NT)
        wacc[m, :, cols] = dot(act[x, m], cot[:, own]) + dot(act_p[0, m], cot_p[0, :, cols])

    def local_plane(k):
        def tile(i, _):
            local_part(plane(k) * Y + i // tiles, lax.rem(i, tiles))
            return _

        with jax.named_scope("wlocal%d" % k):
            if k == 0:
                arrived(cot_p.at[0], ids["cotp"])
                arrived(act_p.at[0], ids["actp"])
            lax.fori_loop(0, Y * tiles, tile, 0)

    def remote_part(m, n):
        cols = pl.ds(pl.multiple_of(n * NT, NT), NT)
        own = pl.ds(pl.multiple_of(c * H + n * NT, NT), NT)
        acc = wacc[m, :, cols]
        for j in range(1, X):
            acc = acc + dot(act_m[j - 1, m], cot_m[j - 1, :, own]) + dot(act_p[j, m], cot_p[j, :, cols])
        return cols, acc

    def weight_plane(k):
        piece = pl.ds(plane(k) * Y, Y)
        with jax.named_scope("actwait%d" % k):
            for j in range(1, X):
                arrived(act_m.at[j - 1, piece], ids["act"] + j * Z + k)
                send(act_m.at[j - 1, piece], act_p.at[j, piece], ids["actp"] + j * Z + k, s, partner)
            for j in range(1, X):
                arrived(act_p.at[j, piece], ids["actp"] + j * Z + k)
                for b in range(BLOCKS if k == 0 else 0):
                    arrived(cot_p.at[j, pl.ds(b * TB, TB)], ids["cotp"] + j * BLOCKS + b)
        with jax.named_scope("wremote%d" % k):
            for j in range(1, Y):
                to_y = lax.rem(y + j, Y)
                i = (j - 1) * Z + k

                def send_tile(n, _):
                    cols, acc = remote_part(plane(k) * Y + to_y, n)
                    wpart[i, :, cols] = acc.astype(bf16)
                    return _

                lax.fori_loop(0, tiles, send_tile, 0)
                send(wpart.at[i], yrecv.at[i], ids["y"] + i, z * Y + to_y, d)

            def own_tile(n, _):
                m = plane(k) * Y + y
                cols, acc = remote_part(m, n)
                wacc[m, :, cols] = acc
                return _

            lax.fori_loop(0, tiles, own_tile, 0)

    def reduce_y(k):
        with jax.named_scope("ywait%d" % k):
            for j in range(1, Y):
                arrived(yrecv.at[(j - 1) * Z + k], ids["y"] + (j - 1) * Z + k)
        to_z = plane(k)
        m = to_z * Y + y

        def tile(n, _):
            cols = pl.ds(pl.multiple_of(n * LANES, LANES), LANES)
            acc = wacc[m, :, cols]
            for j in range(1, Y):
                acc = acc + yrecv[(j - 1) * Z + k, :, cols].astype(f32)
            if k < Z - 1:
                ysum[k, :, cols] = acc.astype(bf16)
            if k != Z - 2:
                wacc[m, :, cols] = acc
            return _

        lax.fori_loop(0, H // LANES, tile, 0)
        if k < near:
            r = copy(ysum.at[k], zmid.at[k], ids["z"] + k, inner_z * Y + y, d)

            @pl.when(jnp.logical_not(inner))
            def _():
                r.start()

            outer.append(r)
        elif k < Z - 1:
            send(ysum.at[k], zrecv.at[0], ids["z"] + near, to_z * Y + y, d)

    def reduce_z(k):
        to_z = plane(k)
        m = to_z * Y + y

        def tile(n, _):
            cols = pl.ds(pl.multiple_of(n * LANES, LANES), LANES)
            ysum[k, :, cols] = (wacc[m, :, cols] + zmid[k, :, cols].astype(f32)).astype(bf16)
            return _

        r = copy(ysum.at[k], zrecv.at[1], ids["z"] + k, to_z * Y + y, d, ids["z"] + near + 1)

        @pl.when(inner)
        def _():
            with jax.named_scope("zmid%d" % k):
                arrived(zmid.at[k], ids["z"] + k)
            lax.fori_loop(0, H // LANES, tile, 0)
            r.start()

    outer = []

    def fold(v):
        return jnp.sum(v.reshape(v.shape[0] // 8, 8, LANES), axis=0)

    def gradient(b):
        rows = pl.ds(b * TB, TB)
        with jax.named_scope("gawait%d" % b):
            for j in range(1, X):
                origin = lax.rem(x + j, X)
                arrived(ga.at[pl.ds(origin * 2 * cpd, 2 * cpd), rows], ids["ga"] + j * BLOCKS + b)

        def grad_chunk(cb, sums):
            one, two = sums
            centred = cen[cb, rows, :]
            gain = kall[cb].astype(f32)[K : K + 1]
            normed = centred * gain
            sg = jax.nn.sigmoid(normed)
            grad = ga[cb, rows, :].astype(f32) * sg * (1.0 + normed * (1.0 - sg))
            scaled = grad * centred
            kacc[cb, K] = fold(scaled) if b == 0 else kacc[cb, K] + fold(scaled)
            gc[cb, rows, :] = grad * gain
            return one + grad * gain, two + scaled * gain

        zero = jnp.zeros((TB, LANES), f32)
        with jax.named_scope("gradchunk%d" % b):
            one, two = lax.fori_loop(0, chunks, grad_chunk, (zero, zero))
        first = jnp.sum(one, axis=1, keepdims=True) / C
        second = jnp.sum(two, axis=1, keepdims=True) / C
        scale = invs[rows, :]

        def conv_grad(cb, _):
            grad = (gc[cb, rows, :] - first - cen[cb, rows, :] * second) * scale
            gext[cb, rows, :] = grad
            if b == 0:
                bsend[cb] = grad[:HB].astype(bf16)
            return _

        with jax.named_scope("convgrad%d" % b):
            lax.fori_loop(0, chunks, conv_grad, 0)

    def taps_grad(b):
        def taps_chunk(cb, _):
            grad = gext[cb, pl.ds(b * TB, TB), :]
            for k in range(K):
                acc = fold(grad * ext[cb, pl.ds(HB - k + b * TB, TB), :])
                if b > 0:
                    acc = acc + kacc[cb, k]
                if b < BLOCKS - 1:
                    kacc[cb, k] = acc
                else:
                    kg[cb, pl.ds(k, 1), :] = jnp.sum(acc, axis=0, keepdims=True)
            if b == BLOCKS - 1:
                kg[cb, pl.ds(K, 1), :] = jnp.sum(kacc[cb, K], axis=0, keepdims=True)
                kgb[cb] = kg[cb].astype(bf16)
            return _

        with jax.named_scope("taps%d" % b):
            lax.fori_loop(0, chunks, taps_chunk, 0)

    stores = []

    def gated_grad(b):
        rows = pl.ds(b * TB, TB)

        def gated_chunk(cb, _):
            cols = pl.ds(pl.multiple_of(cb * LANES, LANES), LANES)
            tf = kall[cb].astype(f32)
            acc = jnp.zeros((TB, LANES), f32)
            for k in range(K):
                acc = acc + tf[k : k + 1] * gext[cb, pl.ds(k + b * TB, TB), :]
            acc = acc.astype(bf16).astype(f32)
            sig = jax.nn.sigmoid(gate[rows, cols].astype(f32))
            gv[rows, cols] = (acc * sig).astype(bf16)
            gg[rows, cols] = (acc * val[rows, cols].astype(f32) * sig * (1.0 - sig)).astype(bf16)
            return _

        with jax.named_scope("gated%d" % b):
            lax.fori_loop(0, chunks, gated_chunk, 0)
        for i, (src, dst) in enumerate(((gv, gv_out), (gg, gg_out))):
            st = pltpu.make_async_copy(src.at[rows], dst.at[rows], store_sem.at[2 * b + i])
            st.start()
            stores.append(st)

    back = copy(bsend, brecv, ids["back"], lax.rem(s + S - 1, S), d)
    back = copy(bsend, brecv, ids["back"], lax.rem(s + S - 1, S), d)
    arrived(w_p, ids["w"])
    send_act(0)
    send_act(1)
    relay_mirror(0)
    project_mirror(0)
    send_act(2)
    relay_mirror(1)
    project_mirror(1)
    send_act(3)
    relay_mirror(2)
    project_mirror(2)
    local_plane(0)
    relay_mirror(3)
    with jax.named_scope("proj_p"):
        project(cot, w_p, ga, partner * cpd)
    weight_plane(0)
    project_mirror(3)
    for k in (1, 2):
        local_plane(k)
        weight_plane(k)
    reduce_y(0)
    gradient(0)

    @pl.when(s > 0)
    def _():
        back.start()

    taps_grad(0)
    local_plane(3)
    weight_plane(3)
    gradient(1)
    taps_grad(1)
    reduce_y(1)
    gradient(2)
    taps_grad(2)
    reduce_z(0)
    gradient(3)
    taps_grad(3)
    for j in range(1, S):
        to = lax.rem(s + j, S)
        send(kgb.at[pl.ds(to * cps, cps)], krecv.at[j], ids["kg"] + j, to, d)
    reduce_y(2)
    gated_grad(0)
    reduce_z(1)
    gated_grad(1)
    gated_grad(2)
    with jax.named_scope("backwait"):
        @pl.when(s < S - 1)
        def _():
            arrived(brecv, ids["back"])

    @pl.when(s == S - 1)
    def _():
        gext[:, pl.ds(T, HB), :] = jnp.zeros((chunks, HB, LANES), f32)

    @pl.when(s < S - 1)
    def _():
        gext[:, pl.ds(T, HB), :] = brecv[...].astype(f32)

    gated_grad(3)
    with jax.named_scope("kgwait"):
        for j in range(1, S):
            arrived(krecv.at[j], ids["kg"] + j)
    acc = kg[pl.ds(s * cps, cps)]
    for j in range(1, S):
        acc = acc + krecv[j].astype(f32)
    ksum[...] = acc
    for j in range(1, N):
        send(ksum, k2recv.at[j], ids["k2"] + j, s, lax.rem(d + j, N))

    reduce_y(3)
    with jax.named_scope("zwait"):
        for q in range(2):
            arrived(zrecv.at[q], ids["z"] + near + q)

    def final_tile(n, _):
        cols = pl.ds(pl.multiple_of(n * LANES, LANES), LANES)
        acc = wacc[s, :, cols]
        for q in range(2):
            acc = acc + zrecv[q, :, cols].astype(f32)
        acc = acc * factor
        fin[0, :, cols] = acc[:block]
        fin[1, :, cols] = acc[block:]
        return _

    with jax.named_scope("final"):
        lax.fori_loop(0, H // LANES, final_tile, 0)
    send(fin.at[other], fbuf, ids["fin"], s, partner)
    gw[:, half] = fin[c]

    with jax.named_scope("k2wait"):
        for j in range(1, N):
            arrived(k2recv.at[j], ids["k2"] + j)
            acc = acc + k2recv[j]
    for q in range(cps):
        cols = slice(q * LANES, (q + 1) * LANES)
        kout[:, cols] = acc[q] * factor

    arrived(fbuf, ids["fin"])
    gw[:, ohalf] = fbuf[...]
    for r in waits + outer:
        r.wait_send()

    @pl.when(s < S - 1)
    def _():
        front.wait_send()

    @pl.when(s > 0)
    def _():
        back.wait_send()

    for st in stores:
        st.wait()


def number(*sizes):
    ids, count = {}, 0
    for name, size in sizes:
        ids[name] = count
        count += size
    return ids, count


def hand_over(K, gv_in, gg_in, gw_in, k_in, gv, gg, gw, kout, gout, a, b, c, sem):
    T = gv_in.shape[0]
    pieces = []
    for n in range(2):
        rows = pl.ds(n * (T // 2), T // 2)
        pieces += [(gv_in.at[rows], a.at[rows], gv.at[rows]), (gg_in.at[rows], b.at[rows], gg.at[rows])]
    pieces.append((gw_in, c, gw))
    loads = [pltpu.make_async_copy(p[0], p[1], sem.at[0, i]) for i, p in enumerate(pieces)]
    stores = [pltpu.make_async_copy(p[1], p[2], sem.at[1, i]) for i, p in enumerate(pieces)]
    for l in loads:
        l.start()
    kout[...] = k_in[:K]
    gout[...] = k_in[K : K + 1]
    for l, st in zip(loads, stores):
        l.wait()
        st.start()
    for st in stores:
        st.wait()


def pair_call(S, N, Y, T, C, K, HB, KP, cot, val, gate, w, kernel, gain):
    X, Z, H = N // 2, S // Y, C // 2
    chunks, cps, cpd, block = C // LANES, C // LANES // S, C // LANES // N, C // (S * N)
    M, CR = chunks // X, C // N
    ids, count = number(
        ("taps", S), ("front", 1), ("back", 1), ("w", 1), ("cot", X * BLOCKS), ("cotp", X * BLOCKS),
        ("act", X * Z), ("actp", X * Z), ("ga", X * BLOCKS), ("y", (Y - 1) * Z), ("z", Z // 2 + 2), ("fin", 1),
        ("kg", S), ("k2", N),
    )
    vm = pl.BlockSpec(memory_space=pltpu.VMEM)
    hbm = pl.BlockSpec(memory_space=pl.ANY)
    partial = pl.pallas_call(
        functools.partial(pair_kernel, S, N, Y, T, C, K, HB, ids),
        out_shape=(
            jax.ShapeDtypeStruct((T, C), bf16),
            jax.ShapeDtypeStruct((T, C), bf16),
            jax.ShapeDtypeStruct((block, C), f32),
            jax.ShapeDtypeStruct((KP, C // S), f32),
        ),
        in_specs=[hbm] * 4 + [vm] * 2,
        out_specs=(hbm, hbm, vm, vm),
        scratch_shapes=[
            pltpu.VMEM((cps, KP, LANES), bf16),
            pltpu.VMEM((T, C), bf16),
            pltpu.VMEM((T, C), bf16),
            pltpu.VMEM((T, C), bf16),
            pltpu.VMEM((CR, C), bf16),
            pltpu.VMEM((CR, C), bf16),
            pltpu.VMEM((X - 1, T, C), bf16),
            pltpu.VMEM((X, T, H), bf16),
            pltpu.VMEM((chunks, HB, LANES), bf16),
            pltpu.VMEM((chunks, HB, LANES), bf16),
            pltpu.VMEM((chunks, HB, LANES), bf16),
            pltpu.VMEM((chunks, HB, LANES), bf16),
            pltpu.VMEM((chunks, T + HB, LANES), f32),
            pltpu.VMEM((chunks, T, LANES), f32),
            pltpu.VMEM((chunks, T, LANES), f32),
            pltpu.VMEM((chunks, T + HB, LANES), f32),
            pltpu.VMEM((chunks, KP, LANES), bf16),
            pltpu.VMEM((X, M, T, LANES), bf16),
            pltpu.VMEM((X - 1, M, T, LANES), bf16),
            pltpu.VMEM((X, M, T, LANES), bf16),
            pltpu.VMEM((X - 1, 2 * cpd, T, LANES), bf16),
            pltpu.VMEM((chunks, T, LANES), bf16),
            pltpu.VMEM((M, LANES, H), f32),
            pltpu.VMEM(((Y - 1) * Z, LANES, H), bf16),
            pltpu.VMEM(((Y - 1) * Z, LANES, H), bf16),
            pltpu.VMEM((Z - 1, LANES, H), bf16),
            pltpu.VMEM((Z // 2, LANES, H), bf16),
            pltpu.VMEM((2, LANES, H), bf16),
            pltpu.VMEM((2, block, H), f32),
            pltpu.VMEM((block, H), f32),
            pltpu.VMEM((T, C), bf16),
            pltpu.VMEM((T, C), bf16),
            pltpu.VMEM((T, LANES), f32),
            pltpu.VMEM((chunks, K + 1, 8, LANES), f32),
            pltpu.VMEM((chunks, KP, LANES), f32),
            pltpu.VMEM((chunks, KP, LANES), bf16),
            pltpu.VMEM((S, cps, KP, LANES), bf16),
            pltpu.VMEM((cps, KP, LANES), f32),
            pltpu.VMEM((N, cps, KP, LANES), f32),
            pltpu.SemaphoreType.DMA((count,)),
            pltpu.SemaphoreType.DMA((count,)),
            pltpu.SemaphoreType.DMA((4,)),
            pltpu.SemaphoreType.DMA((2 * BLOCKS,)),
            pltpu.SemaphoreType.REGULAR((2 * (Z - 2) + 1,)),
        ],
        compiler_params=pltpu.CompilerParams(
            collective_id=0, has_side_effects=True, vmem_limit_bytes=62 * 1024 * 1024
        ),
        name="block_backward",
    )(cot, val, gate, w, kernel, gain)
    return pl.pallas_call(
        functools.partial(hand_over, K),
        out_shape=(
            jax.ShapeDtypeStruct((T, C), bf16),
            jax.ShapeDtypeStruct((T, C), bf16),
            jax.ShapeDtypeStruct((block, C), f32),
            jax.ShapeDtypeStruct((K, C // S), f32),
            jax.ShapeDtypeStruct((1, C // S), f32),
        ),
        in_specs=[hbm] * 3 + [vm],
        out_specs=(hbm, hbm, hbm, vm, vm),
        scratch_shapes=[
            pltpu.VMEM((T, C), bf16),
            pltpu.VMEM((T, C), bf16),
            pltpu.VMEM((block, C), f32),
            pltpu.SemaphoreType.DMA((2, 5)),
        ],
        name="hand_over",
    )(*partial)


def general_call(S, N, T, C, K, HB, KP, cot, val, gate, w, packed):
    chunks, cps, cpd, block = C // LANES, C // LANES // S, C // LANES // N, C // (S * N)
    ids, count = number(
        ("taps", S), ("front", 1), ("back", 1), ("partner", 1), ("mirror", N // 2 * HALVES),
        ("relay", N // 2 * HALVES), ("act", N), ("ga", N), ("rs", S), ("kg", S), ("k2", N),
    )
    vm = pl.BlockSpec(memory_space=pltpu.VMEM)
    return pl.pallas_call(
        functools.partial(general_kernel, S, N, T, C, K, HB, ids),
        out_shape=(
            jax.ShapeDtypeStruct((T, C), bf16),
            jax.ShapeDtypeStruct((T, C), bf16),
            jax.ShapeDtypeStruct((block, C), f32),
            jax.ShapeDtypeStruct((K, C // S), f32),
            jax.ShapeDtypeStruct((1, C // S), f32),
        ),
        in_specs=[vm] * 5,
        out_specs=(vm,) * 5,
        scratch_shapes=[
            pltpu.VMEM((N, T, C), bf16),
            pltpu.VMEM((chunks, T + HB, LANES), f32),
            pltpu.VMEM((chunks, T, LANES), f32),
            pltpu.VMEM((chunks, T, LANES), f32),
            pltpu.VMEM((chunks, T + HB, LANES), f32),
            pltpu.VMEM((chunks, KP, LANES), bf16),
            pltpu.VMEM((chunks, T, LANES), bf16),
            pltpu.VMEM((N, cpd, T, LANES), bf16),
            pltpu.VMEM((N, cpd, T, LANES), bf16),
            pltpu.VMEM((chunks, T, LANES), bf16),
            pltpu.VMEM((cpd * LANES, C), bf16),
            pltpu.VMEM((S, block, C), bf16),
            pltpu.VMEM((chunks, KP, LANES), f32),
            pltpu.VMEM((S, cps, KP, LANES), f32),
            pltpu.VMEM((cps, KP, LANES), f32),
            pltpu.VMEM((N, cps, KP, LANES), f32),
            pltpu.SemaphoreType.DMA((count,)),
            pltpu.SemaphoreType.DMA((count,)),
        ],
        compiler_params=pltpu.CompilerParams(
            collective_id=0, has_side_effects=True, vmem_limit_bytes=60 * 1024 * 1024
        ),
        name="block_backward",
    )(cot, val, gate, w, packed)


def shards(out_cotangent, value_pre, gate_pre, out_weight, conv_kernel, norm_gain):
    S, N = lax.axis_size("sp"), lax.axis_size("dp")
    _, T, C = out_cotangent.shape
    K = conv_kernel.shape[0]
    chunks, cps = C // LANES, C // LANES // S
    HB = -(-(K - 1) // 16) * 16
    KP = -(-(K + 1) // 16) * 16
    args = (out_cotangent[0], value_pre[0], gate_pre[0], out_weight)
    X = N // 2
    if N == 2 * X > 2 and S == 2 * 2 * X and chunks == S * X:
        outs = pair_call(S, N, X, T, C, K, HB, KP, *args, conv_kernel, norm_gain)
    else:
        packed = jnp.concatenate(
            [conv_kernel, norm_gain[None], jnp.zeros((KP - K - 1, C // S), bf16)], axis=0
        )
        packed = jnp.transpose(packed.reshape(KP, cps, LANES), (1, 0, 2))
        outs = general_call(S, N, T, C, K, HB, KP, *args, packed)
    grad_value, grad_gate, grad_weight, grad_taps, grad_gain = outs
    return grad_value[None], grad_gate[None], grad_weight, grad_taps, grad_gain[0]


def solution(mesh):
    placed = (
        P("dp", "sp", None),
        P("dp", "sp", None),
        P("dp", "sp", None),
        P("dp", None),
        P(None, "sp"),
        P("sp"),
    )
    return jax.shard_map(
        shards,
        mesh=mesh,
        in_specs=placed,
        out_specs=(
            P("dp", "sp", None),
            P("dp", "sp", None),
            P(("sp", "dp"), None),
            P(None, "sp"),
            P("sp"),
        ),
        check_vma=False,
    )
```

```python
import functools

import jax
import jax.numpy as jnp
from jax import lax
from jax.experimental import pallas as pl
from jax.experimental.pallas import tpu as pltpu
from jax.sharding import PartitionSpec as P

epsilon = 1e-05
LANES = 128
HALVES = 2
BLOCKS = 4
f32 = jnp.float32
bf16 = jnp.bfloat16


def general_kernel(
    S, N, T, C, K, HB, ids,
    cot, val, gate, w, taps,
    gv, gg, gw, kout, gout,
    cot_all, ext, cen, gc, gext, kall, act, act_all, ga_send, ga, wpart, rbuf,
    kg, krecv, ksum, k2recv, send_sem, recv_sem,
):
    s = lax.axis_index("sp")
    d = lax.axis_index("dp")
    chunks = C // LANES
    cps = chunks // S
    cpd = chunks // N
    block = C // (S * N)
    RB = min(T, 128)
    total = S * N
    me = s * N + d
    partner = d + 1 - 2 * lax.rem(d, 2)
    factor = float(S * N * T) ** (-0.5)
    hrows = T // HALVES
    waits = []

    def copy(src, dst, i, to_s, to_d):
        return pltpu.make_async_remote_copy(
            src_ref=src, dst_ref=dst, send_sem=send_sem.at[i], recv_sem=recv_sem.at[i],
            device_id={"sp": to_s, "dp": to_d}, device_id_type=pl.DeviceIdType.MESH,
        )

    def send(src, dst, i, to_s, to_d):
        c = copy(src, dst, i, to_s, to_d)
        c.start()
        waits.append(c)

    def arrived(dst, i):
        copy(dst, dst, i, s, partner).wait_recv()

    barrier = pltpu.get_barrier_semaphore()

    def greet(j, _):
        other = lax.rem(me + j, total)
        pl.semaphore_signal(
            barrier, inc=1, device_id={"sp": other // N, "dp": lax.rem(other, N)},
            device_id_type=pl.DeviceIdType.MESH,
        )
        return _

    lax.fori_loop(1, total, greet, 0)
    def gate_chunk(cb, _):
        cols = pl.ds(pl.multiple_of(cb * LANES, LANES), LANES)
        sig = jax.nn.sigmoid(gate[:, cols].astype(f32))
        ext[cb, pl.ds(HB, T), :] = (val[:, cols].astype(f32) * sig).astype(bf16).astype(f32)
        return _

    lax.fori_loop(0, chunks, gate_chunk, 0)
    pl.semaphore_wait(barrier, total - 1)

    for j in range(1, S):
        send(taps, kall.at[pl.ds(s * cps, cps)], ids["taps"] + j, lax.rem(s + j, S), d)
    following = lax.rem(s + 1, S)
    preceding = lax.rem(s + S - 1, S)
    send(ext.at[:, pl.ds(T, HB), :], ext.at[:, pl.ds(0, HB), :], ids["front"], following, d)
    for j in range(1, N // 2):
        for h in range(HALVES):
            rows = pl.ds(h * hrows, hrows)
            send(cot.at[rows], cot_all.at[d, rows], ids["mirror"] + j * HALVES + h, s, lax.rem(d + 2 * j, N))
    send(cot, cot_all.at[d], ids["partner"], s, partner)
    kall[pl.ds(s * cps, cps)] = taps[...]
    cot_all[d] = cot[...]
    for j in range(1, S):
        arrived(kall.at[pl.ds(lax.rem(s + S - j, S) * cps, cps)], ids["taps"] + j)
    arrived(ext.at[:, pl.ds(0, HB), :], ids["front"])

    @pl.when(s == 0)
    def _():
        ext[:, pl.ds(0, HB), :] = jnp.zeros((chunks, HB, LANES), f32)

    def conv_chunk(cb, sums):
        tf = kall[cb].astype(f32)
        parts = []
        for rb in range(T // RB):
            acc = jnp.zeros((RB, LANES), f32)
            for k in range(K):
                acc = acc + tf[k : k + 1] * ext[cb, pl.ds(HB - k + rb * RB, RB), :]
            cen[cb, pl.ds(rb * RB, RB), :] = acc
            parts.append(jnp.sum(acc, axis=1, keepdims=True))
        return sums + jnp.concatenate(parts, axis=0)

    column = jnp.zeros((T, 1), f32)
    mean = lax.fori_loop(0, chunks, conv_chunk, column) / C

    def square_chunk(cb, sums):
        dev = cen[cb] - mean
        return sums + dev * dev

    squares = lax.fori_loop(0, chunks, square_chunk, jnp.zeros((T, LANES), f32))
    inv = lax.rsqrt(jnp.sum(squares, axis=1, keepdims=True) / C + epsilon)

    def relay():
        for j in range(1, N // 2):
            origin = lax.rem(d + N - 2 * j, N)
            for h in range(HALVES):
                piece = cot_all.at[origin, pl.ds(h * hrows, hrows)]
                arrived(piece, ids["mirror"] + j * HALVES + h)
                send(piece, piece, ids["relay"] + j * HALVES + h, s, partner)

    def act_chunk(cb, _):
        centred = (cen[cb] - mean) * inv
        cen[cb] = centred
        normed = centred * kall[cb].astype(f32)[K : K + 1]
        act[cb] = (normed * jax.nn.sigmoid(normed)).astype(bf16)
        return _

    lax.fori_loop(0, chunks, act_chunk, 0)
    for j in range(1, N):
        to = lax.rem(d + j, N)
        send(act.at[pl.ds(to * cpd, cpd)], act_all.at[d], ids["act"] + j, s, to)
    act_all[d] = act[pl.ds(d * cpd, cpd)]

    def project(source, slot):
        def pair(m, _):
            rows = pl.ds(pl.multiple_of(m * 2 * LANES, 2 * LANES), 2 * LANES)
            out = lax.dot_general(
                cot_all[source], w[rows, :], (((1,), (1,)), ((), ())), preferred_element_type=f32
            ).astype(bf16)
            ga_send[slot, 2 * m] = out[:, :LANES]
            ga_send[slot, 2 * m + 1] = out[:, LANES:]
            return _

        lax.fori_loop(0, cpd // 2, pair, 0)

    mine = pl.ds(d * cpd, cpd)
    project(d, 0)
    ga[mine] = ga_send[0]
    arrived(cot_all.at[partner], ids["partner"])
    project(partner, 1)
    send(ga_send.at[1], ga.at[mine], ids["ga"] + 1, s, partner)
    relay()
    for j in range(1, N // 2):
        origin = lax.rem(d + N - 2 * j, N)
        project(origin, 2 * j)
        send(ga_send.at[2 * j], ga.at[mine], ids["ga"] + 2 * j, s, origin)
    for j in range(1, N // 2):
        origin = lax.rem(partner + N - 2 * j, N)
        for h in range(HALVES):
            arrived(cot_all.at[origin, pl.ds(h * hrows, hrows)], ids["relay"] + j * HALVES + h)
        project(origin, 2 * j + 1)
        send(ga_send.at[2 * j + 1], ga.at[mine], ids["ga"] + 2 * j + 1, s, origin)

    for j in range(1, N):
        arrived(act_all.at[lax.rem(d + N - j, N)], ids["act"] + j)
    NT = min(C, 512)

    def weight_tile(i, _):
        m, n = i // (C // NT), lax.rem(i, C // NT)
        cols = pl.ds(pl.multiple_of(n * NT, NT), NT)
        acc = jnp.zeros((LANES, NT), f32)
        for q in range(N):
            acc = acc + lax.dot_general(
                act_all[q, m], cot_all[q, :, cols], (((0,), (0,)), ((), ())),
                preferred_element_type=f32,
            )
        wpart[pl.ds(pl.multiple_of(m * LANES, LANES), LANES), cols] = acc.astype(bf16)
        return _

    lax.fori_loop(0, cpd * (C // NT), weight_tile, 0)

    def block_of(j):
        i = lax.rem(s + j, S)
        owner = d * S + i
        rows = pl.ds(pl.multiple_of(i * block, block), block)
        return owner, rows, pltpu.make_async_remote_copy(
            src_ref=wpart.at[rows], dst_ref=rbuf.at[s], send_sem=send_sem.at[ids["rs"] + j],
            recv_sem=recv_sem.at[ids["rs"] + s],
            device_id={"sp": owner // N, "dp": lax.rem(owner, N)},
            device_id_type=pl.DeviceIdType.MESH,
        )

    def send_blocks(first, last):
        for j in range(first, last):
            owner, rows, c = block_of(j)

            @pl.when(owner != me)
            def _():
                c.start()

            @pl.when(owner == me)
            def _():
                rbuf[s] = wpart[rows, :]

    send_blocks(0, S // 2)

    for j in range(1, N // 2):
        arrived(ga.at[pl.ds(lax.rem(d + 2 * j, N) * cpd, cpd)], ids["ga"] + 2 * j)
        arrived(ga.at[pl.ds(lax.rem(partner + 2 * j, N) * cpd, cpd)], ids["ga"] + 2 * j + 1)
    arrived(ga.at[pl.ds(partner * cpd, cpd)], ids["ga"] + 1)

    def grad_chunk(cb, sums):
        one, two = sums
        centred = cen[cb]
        gain = kall[cb].astype(f32)[K : K + 1]
        normed = centred * gain
        sg = jax.nn.sigmoid(normed)
        grad = ga[cb].astype(f32) * sg * (1.0 + normed * (1.0 - sg))
        kg[cb, pl.ds(K, 1), :] = jnp.sum(grad * centred, axis=0, keepdims=True)
        grad = grad * gain
        gc[cb] = grad
        return one + grad, two + grad * centred

    zero = jnp.zeros((T, LANES), f32)
    one, two = lax.fori_loop(0, chunks, grad_chunk, (zero, zero))
    first = jnp.sum(one, axis=1, keepdims=True) / C
    second = jnp.sum(two, axis=1, keepdims=True) / C

    def conv_grad(cb, _):
        gext[cb, pl.ds(0, T), :] = (gc[cb] - first - cen[cb] * second) * inv
        return _

    lax.fori_loop(0, chunks, conv_grad, 0)
    send(gext.at[:, pl.ds(0, HB), :], gext.at[:, pl.ds(T, HB), :], ids["back"], preceding, d)

    def taps_chunk(cb, _):
        for k in range(K):
            acc = jnp.zeros((8, LANES), f32)
            for rb in range(T // RB):
                prod = gext[cb, pl.ds(rb * RB, RB), :] * ext[cb, pl.ds(HB - k + rb * RB, RB), :]
                acc = acc + jnp.sum(prod.reshape(RB // 8, 8, LANES), axis=0)
            kg[cb, pl.ds(k, 1), :] = jnp.sum(acc, axis=0, keepdims=True)
        return _

    lax.fori_loop(0, chunks, taps_chunk, 0)
    for j in range(1, S):
        to = lax.rem(s + j, S)
        send(kg.at[pl.ds(to * cps, cps)], krecv.at[j], ids["kg"] + j, to, d)
    send_blocks(S // 2, S)

    arrived(gext.at[:, pl.ds(T, HB), :], ids["back"])

    @pl.when(s == S - 1)
    def _():
        gext[:, pl.ds(T, HB), :] = jnp.zeros((chunks, HB, LANES), f32)

    def gated_chunk(cb, _):
        cols = pl.ds(pl.multiple_of(cb * LANES, LANES), LANES)
        tf = kall[cb].astype(f32)
        for rb in range(T // RB):
            rows = pl.ds(rb * RB, RB)
            acc = jnp.zeros((RB, LANES), f32)
            for k in range(K):
                acc = acc + tf[k : k + 1] * gext[cb, pl.ds(k + rb * RB, RB), :]
            acc = acc.astype(bf16).astype(f32)
            sig = jax.nn.sigmoid(gate[rows, cols].astype(f32))
            gv[rows, cols] = (acc * sig).astype(bf16)
            gg[rows, cols] = (acc * val[rows, cols].astype(f32) * sig * (1.0 - sig)).astype(bf16)
        return _

    lax.fori_loop(0, chunks, gated_chunk, 0)

    acc = kg[pl.ds(s * cps, cps)]
    for j in range(1, S):
        arrived(krecv.at[j], ids["kg"] + j)
        acc = acc + krecv[j]
    ksum[...] = acc
    for j in range(1, N):
        send(ksum, k2recv.at[j], ids["k2"] + j, s, lax.rem(d + j, N))
    for j in range(1, N):
        arrived(k2recv.at[j], ids["k2"] + j)
        acc = acc + k2recv[j]
    for c in range(cps):
        cols = slice(c * LANES, (c + 1) * LANES)
        kout[:, cols] = (acc[c] * factor)[:K]
        gout[:, cols] = (acc[c] * factor)[K : K + 1]

    home = me // S
    for q in range(S):
        @pl.when(jnp.logical_or(q != s, home != d))
        def _():
            arrived(rbuf.at[q], ids["rs"] + q)

    def sum_tile(n, _):
        cols = pl.ds(pl.multiple_of(n * LANES, LANES), LANES)
        acc = rbuf[0, :, cols].astype(f32)
        for q in range(1, S):
            acc = acc + rbuf[q, :, cols].astype(f32)
        gw[:, cols] = acc * factor
        return _

    lax.fori_loop(0, chunks, sum_tile, 0)
    for j in range(S):
        owner, rows, c = block_of(j)

        @pl.when(owner != me)
        def _():
            c.wait_send()

    for c in waits:
        c.wait_send()


def pair_kernel(
    S, N, Y, T, C, K, HB, ids,
    cot_in, val_in, gate_in, w_in, kernel, gain,
    gv_out, gg_out, gw, kout,
    taps, cot, val, gate, w, w_p, cot_m, cot_p, fsend, frecv, bsend, brecv, ext, cen, gc, gext, kall,
    act, act_m, act_p, ga_s, ga, wacc, wpart, yrecv, ysum, zmid, zrecv, fin, fbuf, gv, gg,
    means, invs, sum1, sum2, kacc, kg, kgb, krecv, ksum, k2recv, send_sem, recv_sem, load_sem, store_sem, ready,
):
    s = lax.axis_index("sp")
    d = lax.axis_index("dp")
    X, Z, H = N // 2, S // Y, C // 2
    x, c = d // 2, lax.rem(d, 2)
    y, z = lax.rem(s, Y), s // Y
    other = 1 - c
    partner = d + 1 - 2 * c
    chunks = C // LANES
    cps = chunks // S
    cpd = chunks // N
    block = C // (S * N)
    M = chunks // X
    RB = min(T, 128)
    TB = T // BLOCKS
    factor = float(S * N * T) ** (-0.5)
    waits = []

    def copy(src, dst, i, to_s, to_d, j=None):
        return pltpu.make_async_remote_copy(
            src_ref=src, dst_ref=dst, send_sem=send_sem.at[i],
            recv_sem=recv_sem.at[i if j is None else j],
            device_id={"sp": to_s, "dp": to_d}, device_id_type=pl.DeviceIdType.MESH,
        )

    def send(src, dst, i, to_s, to_d, j=None):
        r = copy(src, dst, i, to_s, to_d, j)
        r.start()
        waits.append(r)

    def arrived(dst, i):
        copy(dst, dst, i, s, partner).wait_recv()

    loads = [
        pltpu.make_async_copy(a, b, load_sem.at[i])
        for i, (a, b) in enumerate(((gate_in, gate), (val_in, val), (cot_in, cot), (w_in, w)))
    ]
    for l in loads:
        l.start()

    barrier = pltpu.get_barrier_semaphore()

    def signal(sem, to_s, to_d):
        pl.semaphore_signal(
            sem, inc=1, device_id={"sp": to_s, "dp": to_d}, device_id_type=pl.DeviceIdType.MESH
        )

    def along_z(action):
        @pl.when(z > 0)
        def _():
            action(0, s - Y)

        @pl.when(z < Z - 1)
        def _():
            action(1, s + Y)

    signal(barrier, s, partner)
    for j in range(1, X):
        signal(barrier, s, lax.rem(d + 2 * j, N))
    for j in range(1, Y):
        signal(barrier, z * Y + lax.rem(y + j, Y), d)
    along_z(lambda side, to_s: signal(barrier, to_s, d))
    KP = taps.shape[1]
    for q in range(cps):
        cols = slice(q * LANES, (q + 1) * LANES)
        taps[q] = jnp.concatenate(
            [kernel[:, cols].astype(f32), gain[cols].astype(f32).reshape(1, LANES)]
            + [jnp.zeros((KP - K - 1, LANES), f32)] * (KP > K + 1),
            axis=0,
        ).astype(bf16)
    loads[0].wait()
    loads[1].wait()

    def gate_chunk(cb, _):
        cols = pl.ds(pl.multiple_of(cb * LANES, LANES), LANES)
        sig = jax.nn.sigmoid(gate[:, cols].astype(f32))
        gated = (val[:, cols].astype(f32) * sig).astype(bf16)
        ext[cb, pl.ds(HB, T), :] = gated.astype(f32)
        fsend[cb] = gated[T - HB :]
        return _

    with jax.named_scope("gate"):
        lax.fori_loop(0, chunks, gate_chunk, 0)
    loads[2].wait()
    with jax.named_scope("barrierwait"):
        pl.semaphore_wait(barrier, X + Y - 1 + jnp.where(z > 0, 1, 0) + jnp.where(z < Z - 1, 1, 0))

    parts = ((0, H - H // BLOCKS), (H - H // BLOCKS, H // BLOCKS))

    def strip(side, p):
        return pl.ds(pl.multiple_of(side * H + parts[p][0], LANES), parts[p][1])

    def send_cot(p):
        for j in range(1, X):
            for side in range(2):
                send(
                    cot.at[:, strip(side, p)], cot_m.at[j - 1, :, strip(side, p)],
                    ids["cot"] + (j * 2 + p) * 2 + side, s, lax.rem(d + 2 * j, N),
                )

    send_cot(0)
    half = pl.ds(pl.multiple_of(c * H, LANES), H)
    ohalf = pl.ds(pl.multiple_of(other * H, LANES), H)
    loads[3].wait()
    send(w, w_p, ids["w"], s, partner)
    send(cot.at[:, ohalf], cot_p.at[0], ids["cotp"], s, partner)
    kall[pl.ds(s * cps, cps)] = taps[...]
    with jax.named_scope("ready"):
        for r in range(Z - 2):
            along_z(lambda side, to_s: signal(ready.at[2 * r + 1 - side], to_s, d))
            along_z(lambda side, to_s: pl.semaphore_wait(ready.at[2 * r + side], 1))
        for j in range(1, Y):
            signal(ready.at[2 * (Z - 2)], z * Y + lax.rem(y + j, Y), d)
        pl.semaphore_wait(ready.at[2 * (Z - 2)], Y - 1)
    for j in range(1, S):
        send(taps, kall.at[pl.ds(s * cps, cps)], ids["taps"] + j, lax.rem(s + j, S), d)
    front = copy(fsend, frecv, ids["front"], lax.rem(s + 1, S), d)

    @pl.when(s < S - 1)
    def _():
        front.start()


    def project(rows_of, weights, out, base):
        def pair(m, _):
            rows = pl.ds(pl.multiple_of(m * 2 * LANES, 2 * LANES), 2 * LANES)
            prod = lax.dot_general(
                rows_of[...], weights[rows, :], (((1,), (1,)), ((), ())), preferred_element_type=f32
            ).astype(bf16)
            out[base + 2 * m] = prod[:, :LANES]
            out[base + 2 * m + 1] = prod[:, LANES:]
            return _

        lax.fori_loop(0, cpd // 2, pair, 0)

    with jax.named_scope("proj_own"):
        project(cot, w, ga, d * cpd)
    with jax.named_scope("tapswait"):
        for j in range(1, S):
            arrived(kall.at[pl.ds(lax.rem(s + S - j, S) * cps, cps)], ids["taps"] + j)

        @pl.when(s > 0)
        def _():
            arrived(frecv, ids["front"])

    @pl.when(s == 0)
    def _():
        ext[:, pl.ds(0, HB), :] = jnp.zeros((chunks, HB, LANES), f32)

    @pl.when(s > 0)
    def _():
        ext[:, pl.ds(0, HB), :] = frecv[...].astype(f32)

    def convolve(cb, rb):
        tf = kall[cb].astype(f32)
        acc = jnp.zeros((RB, LANES), f32)
        for k in range(K):
            acc = acc + tf[k : k + 1] * ext[cb, pl.ds(HB - k + rb * RB, RB), :]
        cen[cb, pl.ds(rb * RB, RB), :] = acc
        return acc

    def conv_chunk(cb, _):
        for rb in range(T // RB):
            rows = pl.ds(rb * RB, RB)
            dev = convolve(cb, rb) - means[rows, :]
            sum1[rows, :] = sum1[rows, :] + dev
            sum2[rows, :] = sum2[rows, :] + dev * dev
        return _

    with jax.named_scope("conv"):
        for rb in range(T // RB):
            rows = pl.ds(rb * RB, RB)
            acc = convolve(0, rb)
            start = jnp.broadcast_to(jnp.sum(acc, axis=1, keepdims=True) / LANES, (RB, LANES))
            means[rows, :] = start
            sum1[rows, :] = acc - start
            sum2[rows, :] = (acc - start) * (acc - start)
        lax.fori_loop(1, chunks, conv_chunk, 0)
    with jax.named_scope("moments"):
        shift = jnp.sum(sum1[...], axis=1, keepdims=True) / C
        variance = jnp.sum(sum2[...], axis=1, keepdims=True) / C - shift * shift
        means[...] = means[...] + shift
        invs[...] = jnp.broadcast_to(lax.rsqrt(variance + epsilon), (T, LANES))

    def act_chunk(cb, _):
        centred = (cen[cb] - means[...]) * invs[...]
        cen[cb] = centred
        normed = centred * kall[cb].astype(f32)[K : K + 1]
        act[lax.rem(cb, X), cb // X] = (normed * jax.nn.sigmoid(normed)).T.astype(bf16)
        return _

    with jax.named_scope("act"):
        lax.fori_loop(0, chunks, act_chunk, 0)
    send(act.at[x], act_p.at[0], ids["actp"], s, partner)

    near = Z // 2
    low = z < near
    inner_z = jnp.where(low, near - 1, near)
    inner = z == inner_z

    def plane(k):
        if k < near:
            return jnp.where(low, Z - 1 - k, k)
        return jnp.where(low, 0, near) + lax.rem(z + 1 + k, near)

    def send_act(k):
        piece = pl.ds(plane(k) * Y, Y)
        for j in range(1, X):
            send(
                act.at[lax.rem(x + j, X), piece], act_m.at[j - 1, piece], ids["act"] + j * Z + k,
                s, lax.rem(d + 2 * j, N),
            )

    def relay_mirror(p):
        with jax.named_scope("cotwait%d" % p):
            for j in range(1, X):
                for side in range(2):
                    arrived(cot_m.at[j - 1, :, strip(side, p)], ids["cot"] + (j * 2 + p) * 2 + side)
                send(
                    cot_m.at[j - 1, :, strip(other, p)], cot_p.at[j, :, strip(0, p)],
                    ids["cotp"] + j * 2 + p, s, partner,
                )

    def project_mirror():
        for j in range(1, X):
            with jax.named_scope("proj_m"):
                project(cot_m.at[j - 1], w, ga_s.at[j - 1], c * cpd)
                project(cot_m.at[j - 1], w_p, ga_s.at[j - 1], other * cpd)
            for b in range(BLOCKS):
                rows = pl.ds(b * TB, TB)
                send(
                    ga_s.at[j - 1, :, rows], ga.at[pl.ds(x * 2 * cpd, 2 * cpd), rows],
                    ids["ga"] + j * BLOCKS + b, s, lax.rem(d + 2 * (X - j), N),
                )

    dims = (((1,), (0,)), ((), ()))

    def dot(a, b):
        return lax.dot_general(a, b, dims, preferred_element_type=f32)

    LT = H // 2

    def local_plane(k):
        def tile(i, _):
            m, n = plane(k) * Y + i // 2, lax.rem(i, 2)
            cols = pl.ds(pl.multiple_of(n * LT, LT), LT)
            own = pl.ds(pl.multiple_of(c * H + n * LT, LT), LT)
            wacc[m, :, cols] = dot(act[x, m], cot[:, own]) + dot(act_p[0, m], cot_p[0, :, cols])
            return _

        with jax.named_scope("wlocal%d" % k):
            if k == 0:
                arrived(cot_p.at[0], ids["cotp"])
                arrived(act_p.at[0], ids["actp"])
            lax.fori_loop(0, Y * 2, tile, 0)

    NT = H // BLOCKS

    def remote_part(m, n):
        cols = pl.ds(pl.multiple_of(n * NT, NT), NT)
        own = pl.ds(pl.multiple_of(c * H + n * NT, NT), NT)
        acc = wacc[m, :, cols]
        for j in range(1, X):
            acc = acc + dot(act_m[j - 1, m], cot_m[j - 1, :, own]) + dot(act_p[j, m], cot_p[j, :, cols])
        return cols, acc

    def relay_act(k):
        piece = pl.ds(plane(k) * Y, Y)
        with jax.named_scope("actwait%d" % k):
            for j in range(1, X):
                arrived(act_m.at[j - 1, piece], ids["act"] + j * Z + k)
                send(act_m.at[j - 1, piece], act_p.at[j, piece], ids["actp"] + j * Z + k, s, partner)

    def weight_part(k, p):
        piece = pl.ds(plane(k) * Y, Y)
        off, size = parts[p]
        with jax.named_scope("relaywait%d%d" % (k, p)):
            for j in range(1, X):
                if p == 0:
                    arrived(act_p.at[j, piece], ids["actp"] + j * Z + k)
                if k == 0:
                    arrived(cot_p.at[j, :, strip(0, p)], ids["cotp"] + j * 2 + p)
        with jax.named_scope("wremote%d%d" % (k, p)):
            for j in range(1, Y):
                to_y = lax.rem(y + j, Y)
                i = (j - 1) * Z + k

                def send_tile(n, _):
                    cols, acc = remote_part(plane(k) * Y + to_y, n)
                    wpart[i, :, cols] = acc.astype(bf16)
                    return _

                lax.fori_loop(off // NT, (off + size) // NT, send_tile, 0)
                send(
                    wpart.at[i, :, strip(0, p)], yrecv.at[i, :, strip(0, p)],
                    ids["y"] + i * 2 + p, z * Y + to_y, d,
                )

            def own_tile(n, _):
                m = plane(k) * Y + y
                cols, acc = remote_part(m, n)
                wacc[m, :, cols] = acc
                return _

            lax.fori_loop(off // NT, (off + size) // NT, own_tile, 0)

    def reduce_y(k, p):
        for q in (p,) if k < near else (0, 1):
            with jax.named_scope("ywait%d%d" % (k, q)):
                for j in range(1, Y):
                    i = (j - 1) * Z + k
                    arrived(yrecv.at[i, :, strip(0, q)], ids["y"] + i * 2 + q)
        to_z = plane(k)
        m = to_z * Y + y

        def tile(n, _):
            cols = pl.ds(pl.multiple_of(n * LANES, LANES), LANES)
            acc = wacc[m, :, cols]
            for j in range(1, Y):
                acc = acc + yrecv[(j - 1) * Z + k, :, cols].astype(f32)
            if k < Z - 1:
                ysum[k, :, cols] = acc.astype(bf16)
            if k != Z - 2:
                wacc[m, :, cols] = acc
            return _

        off, size = parts[p] if k < near else (0, H)
        lax.fori_loop(off // LANES, (off + size) // LANES, tile, 0)
        if k < near:
            r = copy(
                ysum.at[k, :, strip(0, p)], zmid.at[k, :, strip(0, p)], ids["zmid"] + k * 2 + p,
                inner_z * Y + y, d,
            )

            @pl.when(jnp.logical_not(inner))
            def _():
                r.start()

            outer.append(r)
        elif k < Z - 1:
            send(ysum.at[k], zrecv.at[0], ids["znear"], to_z * Y + y, d)

    def reduce_z(k, p):
        to_z = plane(k)
        m = to_z * Y + y
        off, size = parts[p]

        def tile(n, _):
            cols = pl.ds(pl.multiple_of(n * LANES, LANES), LANES)
            ysum[k, :, cols] = (wacc[m, :, cols] + zmid[k, :, cols].astype(f32)).astype(bf16)
            return _

        @pl.when(inner)
        def _():
            with jax.named_scope("zmid%d%d" % (k, p)):
                arrived(zmid.at[k, :, strip(0, p)], ids["zmid"] + k * 2 + p)
            lax.fori_loop(off // LANES, (off + size) // LANES, tile, 0)
            copy(
                ysum.at[k, :, strip(0, p)], zrecv.at[1, :, strip(0, p)], ids["zmid"] + k * 2 + p,
                to_z * Y + y, d, ids["zfar"] + p,
            ).start()

    outer = []

    def fold(v):
        return jnp.sum(v.reshape(v.shape[0] // 8, 8, LANES), axis=0)

    def gradient(b):
        rows = pl.ds(b * TB, TB)
        with jax.named_scope("gawait%d" % b):
            for j in range(1, X):
                origin = lax.rem(x + j, X)
                arrived(ga.at[pl.ds(origin * 2 * cpd, 2 * cpd), rows], ids["ga"] + j * BLOCKS + b)

        def grad_chunk(cb, sums):
            one, two = sums
            centred = cen[cb, rows, :]
            gain = kall[cb].astype(f32)[K : K + 1]
            normed = centred * gain
            sg = jax.nn.sigmoid(normed)
            grad = ga[cb, rows, :].astype(f32) * sg * (1.0 + normed * (1.0 - sg))
            scaled = grad * centred
            kacc[cb, K] = fold(scaled) if b == 0 else kacc[cb, K] + fold(scaled)
            gc[cb, rows, :] = grad * gain
            return one + grad * gain, two + scaled * gain

        zero = jnp.zeros((TB, LANES), f32)
        with jax.named_scope("gradchunk%d" % b):
            one, two = lax.fori_loop(0, chunks, grad_chunk, (zero, zero))
        first = jnp.sum(one, axis=1, keepdims=True) / C
        second = jnp.sum(two, axis=1, keepdims=True) / C
        scale = invs[rows, :]

        def conv_grad(cb, _):
            grad = (gc[cb, rows, :] - first - cen[cb, rows, :] * second) * scale
            gext[cb, rows, :] = grad
            if b == 0:
                bsend[cb] = grad[:HB].astype(bf16)
            return _

        with jax.named_scope("convgrad%d" % b):
            lax.fori_loop(0, chunks, conv_grad, 0)

    def taps_grad(b):
        def taps_chunk(cb, _):
            grad = gext[cb, pl.ds(b * TB, TB), :]
            for k in range(K):
                acc = fold(grad * ext[cb, pl.ds(HB - k + b * TB, TB), :])
                if b > 0:
                    acc = acc + kacc[cb, k]
                if b < BLOCKS - 1:
                    kacc[cb, k] = acc
                else:
                    kg[cb, pl.ds(k, 1), :] = jnp.sum(acc, axis=0, keepdims=True)
            if b == BLOCKS - 1:
                kg[cb, pl.ds(K, 1), :] = jnp.sum(kacc[cb, K], axis=0, keepdims=True)
                kgb[cb] = kg[cb].astype(bf16)
            return _

        with jax.named_scope("taps%d" % b):
            lax.fori_loop(0, chunks, taps_chunk, 0)

    stores = []

    def gated_grad(b):
        rows = pl.ds(b * TB, TB)

        def gated_chunk(cb, _):
            cols = pl.ds(pl.multiple_of(cb * LANES, LANES), LANES)
            tf = kall[cb].astype(f32)
            acc = jnp.zeros((TB, LANES), f32)
            for k in range(K):
                acc = acc + tf[k : k + 1] * gext[cb, pl.ds(k + b * TB, TB), :]
            acc = acc.astype(bf16).astype(f32)
            sig = jax.nn.sigmoid(gate[rows, cols].astype(f32))
            gv[rows, cols] = (acc * sig).astype(bf16)
            gg[rows, cols] = (acc * val[rows, cols].astype(f32) * sig * (1.0 - sig)).astype(bf16)
            return _

        with jax.named_scope("gated%d" % b):
            lax.fori_loop(0, chunks, gated_chunk, 0)
        for i, (src, dst) in enumerate(((gv, gv_out), (gg, gg_out))):
            st = pltpu.make_async_copy(src.at[rows], dst.at[rows], store_sem.at[2 * b + i])
            st.start()
            stores.append(st)

    back = copy(bsend, brecv, ids["back"], lax.rem(s + S - 1, S), d)
    send_act(0)
    send_act(1)
    send_cot(1)
    send_act(2)
    send_act(3)
    arrived(w_p, ids["w"])
    with jax.named_scope("proj_p"):
        project(cot, w_p, ga, partner * cpd)
    local_plane(0)
    local_plane(1)
    local_plane(2)
    relay_mirror(0)
    relay_act(0)
    weight_part(0, 0)
    relay_act(1)
    local_plane(3)
    weight_part(1, 0)
    reduce_y(0, 0)
    relay_mirror(1)
    project_mirror()
    weight_part(0, 1)
    weight_part(1, 1)
    relay_act(2)
    reduce_y(1, 0)
    weight_part(2, 0)
    weight_part(2, 1)
    reduce_z(0, 0)
    reduce_y(0, 1)
    relay_act(3)
    reduce_y(1, 1)
    weight_part(3, 0)
    weight_part(3, 1)
    gradient(0)

    @pl.when(s > 0)
    def _():
        back.start()

    taps_grad(0)
    reduce_z(1, 0)
    gradient(1)
    taps_grad(1)
    reduce_z(0, 1)
    reduce_z(1, 1)
    reduce_y(2, 0)
    gradient(2)
    taps_grad(2)
    gradient(3)
    taps_grad(3)
    for j in range(1, S):
        to = lax.rem(s + j, S)
        send(kgb.at[pl.ds(to * cps, cps)], krecv.at[j], ids["kg"] + j, to, d)
    reduce_y(3, 0)
    gated_grad(0)
    gated_grad(1)
    with jax.named_scope("zwait"):
        arrived(zrecv.at[0], ids["znear"])
        for p in range(2):
            arrived(zrecv.at[1, :, strip(0, p)], ids["zfar"] + p)

    def final_tile(n, _):
        cols = pl.ds(pl.multiple_of(n * LANES, LANES), LANES)
        acc = wacc[s, :, cols]
        for q in range(2):
            acc = acc + zrecv[q, :, cols].astype(f32)
        acc = acc * factor
        fin[0, :, cols] = acc[:block]
        fin[1, :, cols] = acc[block:]
        return _

    with jax.named_scope("final"):
        lax.fori_loop(0, H // LANES, final_tile, 0)
    send(fin.at[other], fbuf, ids["fin"], s, partner)
    gw[:, half] = fin[c]
    gated_grad(2)
    with jax.named_scope("backwait"):
        @pl.when(s < S - 1)
        def _():
            arrived(brecv, ids["back"])

    @pl.when(s == S - 1)
    def _():
        gext[:, pl.ds(T, HB), :] = jnp.zeros((chunks, HB, LANES), f32)

    @pl.when(s < S - 1)
    def _():
        gext[:, pl.ds(T, HB), :] = brecv[...].astype(f32)

    with jax.named_scope("kgwait"):
        for j in range(1, S):
            arrived(krecv.at[j], ids["kg"] + j)
    acc = kg[pl.ds(s * cps, cps)]
    for j in range(1, S):
        acc = acc + krecv[j].astype(f32)
    ksum[...] = acc
    for j in range(1, N):
        send(ksum, k2recv.at[j], ids["k2"] + j, s, lax.rem(d + j, N))
    gated_grad(3)
    with jax.named_scope("k2wait"):
        for j in range(1, N):
            arrived(k2recv.at[j], ids["k2"] + j)
            acc = acc + k2recv[j]
    for q in range(cps):
        cols = slice(q * LANES, (q + 1) * LANES)
        kout[:, cols] = acc[q] * factor

    arrived(fbuf, ids["fin"])
    gw[:, ohalf] = fbuf[...]
    for r in waits + outer:
        r.wait_send()

    @pl.when(s < S - 1)
    def _():
        front.wait_send()

    @pl.when(s > 0)
    def _():
        back.wait_send()

    for st in stores:
        st.wait()


def number(*sizes):
    ids, count = {}, 0
    for name, size in sizes:
        ids[name] = count
        count += size
    return ids, count


def hand_over(K, gv_in, gg_in, gw_in, k_in, gv, gg, gw, kout, gout, a, b, c, sem):
    T = gv_in.shape[0]
    pieces = []
    for n in range(2):
        rows = pl.ds(n * (T // 2), T // 2)
        pieces += [(gv_in.at[rows], a.at[rows], gv.at[rows]), (gg_in.at[rows], b.at[rows], gg.at[rows])]
    pieces.append((gw_in, c, gw))
    loads = [pltpu.make_async_copy(p[0], p[1], sem.at[0, i]) for i, p in enumerate(pieces)]
    stores = [pltpu.make_async_copy(p[1], p[2], sem.at[1, i]) for i, p in enumerate(pieces)]
    for l in loads:
        l.start()
    kout[...] = k_in[:K]
    gout[...] = k_in[K : K + 1]
    for l, st in zip(loads, stores):
        l.wait()
        st.start()
    for st in stores:
        st.wait()


def pair_call(S, N, Y, T, C, K, HB, KP, cot, val, gate, w, kernel, gain):
    X, Z, H = N // 2, S // Y, C // 2
    chunks, cps, cpd, block = C // LANES, C // LANES // S, C // LANES // N, C // (S * N)
    M, CR = chunks // X, C // N
    ids, count = number(
        ("taps", S), ("front", 1), ("back", 1), ("w", 1), ("cot", X * 4), ("cotp", X * 2),
        ("act", X * Z), ("actp", X * Z), ("ga", X * BLOCKS), ("y", (Y - 1) * Z * 2), ("zmid", Z), ("znear", 1), ("zfar", 2),
        ("fin", 1),
        ("kg", S), ("k2", N),
    )
    vm = pl.BlockSpec(memory_space=pltpu.VMEM)
    hbm = pl.BlockSpec(memory_space=pl.ANY)
    partial = pl.pallas_call(
        functools.partial(pair_kernel, S, N, Y, T, C, K, HB, ids),
        out_shape=(
            jax.ShapeDtypeStruct((T, C), bf16),
            jax.ShapeDtypeStruct((T, C), bf16),
            jax.ShapeDtypeStruct((block, C), f32),
            jax.ShapeDtypeStruct((KP, C // S), f32),
        ),
        in_specs=[hbm] * 4 + [vm] * 2,
        out_specs=(hbm, hbm, vm, vm),
        scratch_shapes=[
            pltpu.VMEM((cps, KP, LANES), bf16),
            pltpu.VMEM((T, C), bf16),
            pltpu.VMEM((T, C), bf16),
            pltpu.VMEM((T, C), bf16),
            pltpu.VMEM((CR, C), bf16),
            pltpu.VMEM((CR, C), bf16),
            pltpu.VMEM((X - 1, T, C), bf16),
            pltpu.VMEM((X, T, H), bf16),
            pltpu.VMEM((chunks, HB, LANES), bf16),
            pltpu.VMEM((chunks, HB, LANES), bf16),
            pltpu.VMEM((chunks, HB, LANES), bf16),
            pltpu.VMEM((chunks, HB, LANES), bf16),
            pltpu.VMEM((chunks, T + HB, LANES), f32),
            pltpu.VMEM((chunks, T, LANES), f32),
            pltpu.VMEM((chunks, T, LANES), f32),
            pltpu.VMEM((chunks, T + HB, LANES), f32),
            pltpu.VMEM((chunks, KP, LANES), bf16),
            pltpu.VMEM((X, M, LANES, T), bf16),
            pltpu.VMEM((X - 1, M, LANES, T), bf16),
            pltpu.VMEM((X, M, LANES, T), bf16),
            pltpu.VMEM((X - 1, 2 * cpd, T, LANES), bf16),
            pltpu.VMEM((chunks, T, LANES), bf16),
            pltpu.VMEM((M, LANES, H), f32),
            pltpu.VMEM(((Y - 1) * Z, LANES, H), bf16),
            pltpu.VMEM(((Y - 1) * Z, LANES, H), bf16),
            pltpu.VMEM((Z - 1, LANES, H), bf16),
            pltpu.VMEM((Z // 2, LANES, H), bf16),
            pltpu.VMEM((2, LANES, H), bf16),
            pltpu.VMEM((2, block, H), f32),
            pltpu.VMEM((block, H), f32),
            pltpu.VMEM((T, C), bf16),
            pltpu.VMEM((T, C), bf16),
            pltpu.VMEM((T, LANES), f32),
            pltpu.VMEM((T, LANES), f32),
            pltpu.VMEM((T, LANES), f32),
            pltpu.VMEM((T, LANES), f32),
            pltpu.VMEM((chunks, K + 1, 8, LANES), f32),
            pltpu.VMEM((chunks, KP, LANES), f32),
            pltpu.VMEM((chunks, KP, LANES), bf16),
            pltpu.VMEM((S, cps, KP, LANES), bf16),
            pltpu.VMEM((cps, KP, LANES), f32),
            pltpu.VMEM((N, cps, KP, LANES), f32),
            pltpu.SemaphoreType.DMA((count,)),
            pltpu.SemaphoreType.DMA((count,)),
            pltpu.SemaphoreType.DMA((4,)),
            pltpu.SemaphoreType.DMA((2 * BLOCKS,)),
            pltpu.SemaphoreType.REGULAR((2 * (Z - 2) + 1,)),
        ],
        compiler_params=pltpu.CompilerParams(
            collective_id=0, has_side_effects=True, vmem_limit_bytes=62 * 1024 * 1024
        ),
        name="block_backward",
    )(cot, val, gate, w, kernel, gain)
    return pl.pallas_call(
        functools.partial(hand_over, K),
        out_shape=(
            jax.ShapeDtypeStruct((T, C), bf16),
            jax.ShapeDtypeStruct((T, C), bf16),
            jax.ShapeDtypeStruct((block, C), f32),
            jax.ShapeDtypeStruct((K, C // S), f32),
            jax.ShapeDtypeStruct((1, C // S), f32),
        ),
        in_specs=[hbm] * 3 + [vm],
        out_specs=(hbm, hbm, hbm, vm, vm),
        scratch_shapes=[
            pltpu.VMEM((T, C), bf16),
            pltpu.VMEM((T, C), bf16),
            pltpu.VMEM((block, C), f32),
            pltpu.SemaphoreType.DMA((2, 5)),
        ],
        name="hand_over",
    )(*partial)


def general_call(S, N, T, C, K, HB, KP, cot, val, gate, w, packed):
    chunks, cps, cpd, block = C // LANES, C // LANES // S, C // LANES // N, C // (S * N)
    ids, count = number(
        ("taps", S), ("front", 1), ("back", 1), ("partner", 1), ("mirror", N // 2 * HALVES),
        ("relay", N // 2 * HALVES), ("act", N), ("ga", N), ("rs", S), ("kg", S), ("k2", N),
    )
    vm = pl.BlockSpec(memory_space=pltpu.VMEM)
    return pl.pallas_call(
        functools.partial(general_kernel, S, N, T, C, K, HB, ids),
        out_shape=(
            jax.ShapeDtypeStruct((T, C), bf16),
            jax.ShapeDtypeStruct((T, C), bf16),
            jax.ShapeDtypeStruct((block, C), f32),
            jax.ShapeDtypeStruct((K, C // S), f32),
            jax.ShapeDtypeStruct((1, C // S), f32),
        ),
        in_specs=[vm] * 5,
        out_specs=(vm,) * 5,
        scratch_shapes=[
            pltpu.VMEM((N, T, C), bf16),
            pltpu.VMEM((chunks, T + HB, LANES), f32),
            pltpu.VMEM((chunks, T, LANES), f32),
            pltpu.VMEM((chunks, T, LANES), f32),
            pltpu.VMEM((chunks, T + HB, LANES), f32),
            pltpu.VMEM((chunks, KP, LANES), bf16),
            pltpu.VMEM((chunks, T, LANES), bf16),
            pltpu.VMEM((N, cpd, T, LANES), bf16),
            pltpu.VMEM((N, cpd, T, LANES), bf16),
            pltpu.VMEM((chunks, T, LANES), bf16),
            pltpu.VMEM((cpd * LANES, C), bf16),
            pltpu.VMEM((S, block, C), bf16),
            pltpu.VMEM((chunks, KP, LANES), f32),
            pltpu.VMEM((S, cps, KP, LANES), f32),
            pltpu.VMEM((cps, KP, LANES), f32),
            pltpu.VMEM((N, cps, KP, LANES), f32),
            pltpu.SemaphoreType.DMA((count,)),
            pltpu.SemaphoreType.DMA((count,)),
        ],
        compiler_params=pltpu.CompilerParams(
            collective_id=0, has_side_effects=True, vmem_limit_bytes=60 * 1024 * 1024
        ),
        name="block_backward",
    )(cot, val, gate, w, packed)


def shards(out_cotangent, value_pre, gate_pre, out_weight, conv_kernel, norm_gain):
    S, N = lax.axis_size("sp"), lax.axis_size("dp")
    _, T, C = out_cotangent.shape
    K = conv_kernel.shape[0]
    chunks, cps = C // LANES, C // LANES // S
    HB = -(-(K - 1) // 16) * 16
    KP = -(-(K + 1) // 16) * 16
    args = (out_cotangent[0], value_pre[0], gate_pre[0], out_weight)
    X = N // 2
    if N == 2 * X > 2 and S == 2 * 2 * X and chunks == S * X:
        outs = pair_call(S, N, X, T, C, K, HB, KP, *args, conv_kernel, norm_gain)
    else:
        packed = jnp.concatenate(
            [conv_kernel, norm_gain[None], jnp.zeros((KP - K - 1, C // S), bf16)], axis=0
        )
        packed = jnp.transpose(packed.reshape(KP, cps, LANES), (1, 0, 2))
        outs = general_call(S, N, T, C, K, HB, KP, *args, packed)
    grad_value, grad_gate, grad_weight, grad_taps, grad_gain = outs
    return grad_value[None], grad_gate[None], grad_weight, grad_taps, grad_gain[0]


def solution(mesh):
    placed = (
        P("dp", "sp", None),
        P("dp", "sp", None),
        P("dp", "sp", None),
        P("dp", None),
        P(None, "sp"),
        P("sp"),
    )
    return jax.shard_map(
        shards,
        mesh=mesh,
        in_specs=placed,
        out_specs=(
            P("dp", "sp", None),
            P("dp", "sp", None),
            P(("sp", "dp"), None),
            P(None, "sp"),
            P("sp"),
        ),
        check_vma=False,
    )
```

```python
import functools

import jax
import jax.numpy as jnp
from jax import lax
from jax.experimental import pallas as pl
from jax.experimental.pallas import tpu as pltpu
from jax.sharding import PartitionSpec as P

epsilon = 1e-05
LANES = 128
HALVES = 2
BLOCKS = 4
f32 = jnp.float32
bf16 = jnp.bfloat16


def general_kernel(
    S, N, T, C, K, HB, ids,
    cot, val, gate, w, taps,
    gv, gg, gw, kout, gout,
    cot_all, ext, cen, gc, gext, kall, act, act_all, ga_send, ga, wpart, rbuf,
    kg, krecv, ksum, k2recv, send_sem, recv_sem,
):
    s = lax.axis_index("sp")
    d = lax.axis_index("dp")
    chunks = C // LANES
    cps = chunks // S
    cpd = chunks // N
    block = C // (S * N)
    RB = min(T, 128)
    total = S * N
    me = s * N + d
    partner = d + 1 - 2 * lax.rem(d, 2)
    factor = float(S * N * T) ** (-0.5)
    hrows = T // HALVES
    waits = []

    def copy(src, dst, i, to_s, to_d):
        return pltpu.make_async_remote_copy(
            src_ref=src, dst_ref=dst, send_sem=send_sem.at[i], recv_sem=recv_sem.at[i],
            device_id={"sp": to_s, "dp": to_d}, device_id_type=pl.DeviceIdType.MESH,
        )

    def send(src, dst, i, to_s, to_d):
        c = copy(src, dst, i, to_s, to_d)
        c.start()
        waits.append(c)

    def arrived(dst, i):
        copy(dst, dst, i, s, partner).wait_recv()

    barrier = pltpu.get_barrier_semaphore()

    def greet(j, _):
        other = lax.rem(me + j, total)
        pl.semaphore_signal(
            barrier, inc=1, device_id={"sp": other // N, "dp": lax.rem(other, N)},
            device_id_type=pl.DeviceIdType.MESH,
        )
        return _

    lax.fori_loop(1, total, greet, 0)
    def gate_chunk(cb, _):
        cols = pl.ds(pl.multiple_of(cb * LANES, LANES), LANES)
        sig = jax.nn.sigmoid(gate[:, cols].astype(f32))
        ext[cb, pl.ds(HB, T), :] = (val[:, cols].astype(f32) * sig).astype(bf16).astype(f32)
        return _

    lax.fori_loop(0, chunks, gate_chunk, 0)
    pl.semaphore_wait(barrier, total - 1)

    for j in range(1, S):
        send(taps, kall.at[pl.ds(s * cps, cps)], ids["taps"] + j, lax.rem(s + j, S), d)
    following = lax.rem(s + 1, S)
    preceding = lax.rem(s + S - 1, S)
    send(ext.at[:, pl.ds(T, HB), :], ext.at[:, pl.ds(0, HB), :], ids["front"], following, d)
    for j in range(1, N // 2):
        for h in range(HALVES):
            rows = pl.ds(h * hrows, hrows)
            send(cot.at[rows], cot_all.at[d, rows], ids["mirror"] + j * HALVES + h, s, lax.rem(d + 2 * j, N))
    send(cot, cot_all.at[d], ids["partner"], s, partner)
    kall[pl.ds(s * cps, cps)] = taps[...]
    cot_all[d] = cot[...]
    for j in range(1, S):
        arrived(kall.at[pl.ds(lax.rem(s + S - j, S) * cps, cps)], ids["taps"] + j)
    arrived(ext.at[:, pl.ds(0, HB), :], ids["front"])

    @pl.when(s == 0)
    def _():
        ext[:, pl.ds(0, HB), :] = jnp.zeros((chunks, HB, LANES), f32)

    def conv_chunk(cb, sums):
        tf = kall[cb].astype(f32)
        parts = []
        for rb in range(T // RB):
            acc = jnp.zeros((RB, LANES), f32)
            for k in range(K):
                acc = acc + tf[k : k + 1] * ext[cb, pl.ds(HB - k + rb * RB, RB), :]
            cen[cb, pl.ds(rb * RB, RB), :] = acc
            parts.append(jnp.sum(acc, axis=1, keepdims=True))
        return sums + jnp.concatenate(parts, axis=0)

    column = jnp.zeros((T, 1), f32)
    mean = lax.fori_loop(0, chunks, conv_chunk, column) / C

    def square_chunk(cb, sums):
        dev = cen[cb] - mean
        return sums + dev * dev

    squares = lax.fori_loop(0, chunks, square_chunk, jnp.zeros((T, LANES), f32))
    inv = lax.rsqrt(jnp.sum(squares, axis=1, keepdims=True) / C + epsilon)

    def relay():
        for j in range(1, N // 2):
            origin = lax.rem(d + N - 2 * j, N)
            for h in range(HALVES):
                piece = cot_all.at[origin, pl.ds(h * hrows, hrows)]
                arrived(piece, ids["mirror"] + j * HALVES + h)
                send(piece, piece, ids["relay"] + j * HALVES + h, s, partner)

    def act_chunk(cb, _):
        centred = (cen[cb] - mean) * inv
        cen[cb] = centred
        normed = centred * kall[cb].astype(f32)[K : K + 1]
        act[cb] = (normed * jax.nn.sigmoid(normed)).astype(bf16)
        return _

    lax.fori_loop(0, chunks, act_chunk, 0)
    for j in range(1, N):
        to = lax.rem(d + j, N)
        send(act.at[pl.ds(to * cpd, cpd)], act_all.at[d], ids["act"] + j, s, to)
    act_all[d] = act[pl.ds(d * cpd, cpd)]

    def project(source, slot):
        def pair(m, _):
            rows = pl.ds(pl.multiple_of(m * 2 * LANES, 2 * LANES), 2 * LANES)
            out = lax.dot_general(
                cot_all[source], w[rows, :], (((1,), (1,)), ((), ())), preferred_element_type=f32
            ).astype(bf16)
            ga_send[slot, 2 * m] = out[:, :LANES]
            ga_send[slot, 2 * m + 1] = out[:, LANES:]
            return _

        lax.fori_loop(0, cpd // 2, pair, 0)

    mine = pl.ds(d * cpd, cpd)
    project(d, 0)
    ga[mine] = ga_send[0]
    arrived(cot_all.at[partner], ids["partner"])
    project(partner, 1)
    send(ga_send.at[1], ga.at[mine], ids["ga"] + 1, s, partner)
    relay()
    for j in range(1, N // 2):
        origin = lax.rem(d + N - 2 * j, N)
        project(origin, 2 * j)
        send(ga_send.at[2 * j], ga.at[mine], ids["ga"] + 2 * j, s, origin)
    for j in range(1, N // 2):
        origin = lax.rem(partner + N - 2 * j, N)
        for h in range(HALVES):
            arrived(cot_all.at[origin, pl.ds(h * hrows, hrows)], ids["relay"] + j * HALVES + h)
        project(origin, 2 * j + 1)
        send(ga_send.at[2 * j + 1], ga.at[mine], ids["ga"] + 2 * j + 1, s, origin)

    for j in range(1, N):
        arrived(act_all.at[lax.rem(d + N - j, N)], ids["act"] + j)
    NT = min(C, 512)

    def weight_tile(i, _):
        m, n = i // (C // NT), lax.rem(i, C // NT)
        cols = pl.ds(pl.multiple_of(n * NT, NT), NT)
        acc = jnp.zeros((LANES, NT), f32)
        for q in range(N):
            acc = acc + lax.dot_general(
                act_all[q, m], cot_all[q, :, cols], (((0,), (0,)), ((), ())),
                preferred_element_type=f32,
            )
        wpart[pl.ds(pl.multiple_of(m * LANES, LANES), LANES), cols] = acc.astype(bf16)
        return _

    lax.fori_loop(0, cpd * (C // NT), weight_tile, 0)

    def block_of(j):
        i = lax.rem(s + j, S)
        owner = d * S + i
        rows = pl.ds(pl.multiple_of(i * block, block), block)
        return owner, rows, pltpu.make_async_remote_copy(
            src_ref=wpart.at[rows], dst_ref=rbuf.at[s], send_sem=send_sem.at[ids["rs"] + j],
            recv_sem=recv_sem.at[ids["rs"] + s],
            device_id={"sp": owner // N, "dp": lax.rem(owner, N)},
            device_id_type=pl.DeviceIdType.MESH,
        )

    def send_blocks(first, last):
        for j in range(first, last):
            owner, rows, c = block_of(j)

            @pl.when(owner != me)
            def _():
                c.start()

            @pl.when(owner == me)
            def _():
                rbuf[s] = wpart[rows, :]

    send_blocks(0, S // 2)

    for j in range(1, N // 2):
        arrived(ga.at[pl.ds(lax.rem(d + 2 * j, N) * cpd, cpd)], ids["ga"] + 2 * j)
        arrived(ga.at[pl.ds(lax.rem(partner + 2 * j, N) * cpd, cpd)], ids["ga"] + 2 * j + 1)
    arrived(ga.at[pl.ds(partner * cpd, cpd)], ids["ga"] + 1)

    def grad_chunk(cb, sums):
        one, two = sums
        centred = cen[cb]
        gain = kall[cb].astype(f32)[K : K + 1]
        normed = centred * gain
        sg = jax.nn.sigmoid(normed)
        grad = ga[cb].astype(f32) * sg * (1.0 + normed * (1.0 - sg))
        kg[cb, pl.ds(K, 1), :] = jnp.sum(grad * centred, axis=0, keepdims=True)
        grad = grad * gain
        gc[cb] = grad
        return one + grad, two + grad * centred

    zero = jnp.zeros((T, LANES), f32)
    one, two = lax.fori_loop(0, chunks, grad_chunk, (zero, zero))
    first = jnp.sum(one, axis=1, keepdims=True) / C
    second = jnp.sum(two, axis=1, keepdims=True) / C

    def conv_grad(cb, _):
        gext[cb, pl.ds(0, T), :] = (gc[cb] - first - cen[cb] * second) * inv
        return _

    lax.fori_loop(0, chunks, conv_grad, 0)
    send(gext.at[:, pl.ds(0, HB), :], gext.at[:, pl.ds(T, HB), :], ids["back"], preceding, d)

    def taps_chunk(cb, _):
        for k in range(K):
            acc = jnp.zeros((8, LANES), f32)
            for rb in range(T // RB):
                prod = gext[cb, pl.ds(rb * RB, RB), :] * ext[cb, pl.ds(HB - k + rb * RB, RB), :]
                acc = acc + jnp.sum(prod.reshape(RB // 8, 8, LANES), axis=0)
            kg[cb, pl.ds(k, 1), :] = jnp.sum(acc, axis=0, keepdims=True)
        return _

    lax.fori_loop(0, chunks, taps_chunk, 0)
    for j in range(1, S):
        to = lax.rem(s + j, S)
        send(kg.at[pl.ds(to * cps, cps)], krecv.at[j], ids["kg"] + j, to, d)
    send_blocks(S // 2, S)

    arrived(gext.at[:, pl.ds(T, HB), :], ids["back"])

    @pl.when(s == S - 1)
    def _():
        gext[:, pl.ds(T, HB), :] = jnp.zeros((chunks, HB, LANES), f32)

    def gated_chunk(cb, _):
        cols = pl.ds(pl.multiple_of(cb * LANES, LANES), LANES)
        tf = kall[cb].astype(f32)
        for rb in range(T // RB):
            rows = pl.ds(rb * RB, RB)
            acc = jnp.zeros((RB, LANES), f32)
            for k in range(K):
                acc = acc + tf[k : k + 1] * gext[cb, pl.ds(k + rb * RB, RB), :]
            acc = acc.astype(bf16).astype(f32)
            sig = jax.nn.sigmoid(gate[rows, cols].astype(f32))
            gv[rows, cols] = (acc * sig).astype(bf16)
            gg[rows, cols] = (acc * val[rows, cols].astype(f32) * sig * (1.0 - sig)).astype(bf16)
        return _

    lax.fori_loop(0, chunks, gated_chunk, 0)

    acc = kg[pl.ds(s * cps, cps)]
    for j in range(1, S):
        arrived(krecv.at[j], ids["kg"] + j)
        acc = acc + krecv[j]
    ksum[...] = acc
    for j in range(1, N):
        send(ksum, k2recv.at[j], ids["k2"] + j, s, lax.rem(d + j, N))
    for j in range(1, N):
        arrived(k2recv.at[j], ids["k2"] + j)
        acc = acc + k2recv[j]
    for c in range(cps):
        cols = slice(c * LANES, (c + 1) * LANES)
        kout[:, cols] = (acc[c] * factor)[:K]
        gout[:, cols] = (acc[c] * factor)[K : K + 1]

    home = me // S
    for q in range(S):
        @pl.when(jnp.logical_or(q != s, home != d))
        def _():
            arrived(rbuf.at[q], ids["rs"] + q)

    def sum_tile(n, _):
        cols = pl.ds(pl.multiple_of(n * LANES, LANES), LANES)
        acc = rbuf[0, :, cols].astype(f32)
        for q in range(1, S):
            acc = acc + rbuf[q, :, cols].astype(f32)
        gw[:, cols] = acc * factor
        return _

    lax.fori_loop(0, chunks, sum_tile, 0)
    for j in range(S):
        owner, rows, c = block_of(j)

        @pl.when(owner != me)
        def _():
            c.wait_send()

    for c in waits:
        c.wait_send()


def pair_kernel(
    S, N, Y, T, C, K, HB, ids,
    cot_in, val_in, gate_in, w_in, kernel_in, gain_in,
    gv, gg, gw, kout,
    kernel, gain, taps, cot, val, gate, w, w_p, cot_m, cot_p, fsend, frecv, bsend, brecv, ext, cen, gc, gext, kall,
    act, act_m, act_p, ga_s, ga, wacc, wpart, yrecv, ysum, zmid, zrecv, fin, fbuf,
    means, invs, sum1, sum2, kacc, kg, kgb, krecv, ksum, k2recv, send_sem, recv_sem, load_sem, ready,
):
    s = lax.axis_index("sp")
    d = lax.axis_index("dp")
    X, Z, H = N // 2, S // Y, C // 2
    x, c = d // 2, lax.rem(d, 2)
    y, z = lax.rem(s, Y), s // Y
    other = 1 - c
    partner = d + 1 - 2 * c
    chunks = C // LANES
    cps = chunks // S
    cpd = chunks // N
    block = C // (S * N)
    M = chunks // X
    RB = min(T, 128)
    TB = T // BLOCKS
    factor = float(S * N * T) ** (-0.5)
    waits = []

    def copy(src, dst, i, to_s, to_d, j=None):
        return pltpu.make_async_remote_copy(
            src_ref=src, dst_ref=dst, send_sem=send_sem.at[i],
            recv_sem=recv_sem.at[i if j is None else j],
            device_id={"sp": to_s, "dp": to_d}, device_id_type=pl.DeviceIdType.MESH,
        )

    def send(src, dst, i, to_s, to_d, j=None):
        r = copy(src, dst, i, to_s, to_d, j)
        r.start()
        waits.append(r)

    def arrived(dst, i):
        copy(dst, dst, i, s, partner).wait_recv()

    loads = [
        pltpu.make_async_copy(a, b, load_sem.at[i])
        for i, (a, b) in enumerate((
            (gate_in, gate), (val_in, val), (cot_in, cot), (w_in, w), (kernel_in, kernel), (gain_in, gain),
        ))
    ]
    for l in loads:
        l.start()

    barrier = pltpu.get_barrier_semaphore()

    def signal(sem, to_s, to_d):
        pl.semaphore_signal(
            sem, inc=1, device_id={"sp": to_s, "dp": to_d}, device_id_type=pl.DeviceIdType.MESH
        )

    def along_z(action):
        @pl.when(z > 0)
        def _():
            action(0, s - Y)

        @pl.when(z < Z - 1)
        def _():
            action(1, s + Y)

    signal(barrier, s, partner)
    for j in range(1, X):
        signal(barrier, s, lax.rem(d + 2 * j, N))
    for j in range(1, Y):
        signal(barrier, z * Y + lax.rem(y + j, Y), d)
    along_z(lambda side, to_s: signal(barrier, to_s, d))
    loads[2].wait()
    with jax.named_scope("barrierwait"):
        pl.semaphore_wait(barrier, X + Y - 1 + jnp.where(z > 0, 1, 0) + jnp.where(z < Z - 1, 1, 0))

    def pass_on(r):
        along_z(lambda side, to_s: signal(ready.at[2 * r + 1 - side], to_s, d))

    def passed(r):
        along_z(lambda side, to_s: pl.semaphore_wait(ready.at[2 * r + side], 1))

    pass_on(0)
    parts = ((0, H - H // BLOCKS), (H - H // BLOCKS, H // BLOCKS))

    def strip(side, p):
        return pl.ds(pl.multiple_of(side * H + parts[p][0], LANES), parts[p][1])

    def send_cot(p):
        for j in range(1, X):
            for side in range(2):
                send(
                    cot.at[:, strip(side, p)], cot_m.at[j - 1, :, strip(side, p)],
                    ids["cot"] + (j * 2 + p) * 2 + side, s, lax.rem(d + 2 * j, N),
                )

    send_cot(0)
    loads[0].wait()
    loads[1].wait()

    def gate_chunk(cb, _):
        cols = pl.ds(pl.multiple_of(cb * LANES, LANES), LANES)
        sig = jax.nn.sigmoid(gate[:, cols].astype(f32))
        gated = (val[:, cols].astype(f32) * sig).astype(bf16)
        ext[cb, pl.ds(HB, T), :] = gated.astype(f32)
        fsend[cb] = gated[T - HB :]
        return _

    with jax.named_scope("gate"):
        lax.fori_loop(0, chunks, gate_chunk, 0)
    loads[4].wait()
    loads[5].wait()
    KP = taps.shape[1]
    for q in range(cps):
        cols = slice(q * LANES, (q + 1) * LANES)
        taps[q] = jnp.concatenate(
            [kernel[:, cols].astype(f32), gain[cols].astype(f32).reshape(1, LANES)]
            + [jnp.zeros((KP - K - 1, LANES), f32)] * (KP > K + 1),
            axis=0,
        ).astype(bf16)
    half = pl.ds(pl.multiple_of(c * H, LANES), H)
    ohalf = pl.ds(pl.multiple_of(other * H, LANES), H)
    loads[3].wait()
    send(w, w_p, ids["w"], s, partner)
    send(cot.at[:, ohalf], cot_p.at[0], ids["cotp"], s, partner)
    kall[pl.ds(s * cps, cps)] = taps[...]
    with jax.named_scope("ready"):
        for r in range(Z - 2):
            if r > 0:
                pass_on(r)
            passed(r)
        for j in range(1, Y):
            signal(ready.at[2 * (Z - 2)], z * Y + lax.rem(y + j, Y), d)
        pl.semaphore_wait(ready.at[2 * (Z - 2)], Y - 1)
    for j in range(1, S):
        send(taps, kall.at[pl.ds(s * cps, cps)], ids["taps"] + j, lax.rem(s + j, S), d)
    front = copy(fsend, frecv, ids["front"], lax.rem(s + 1, S), d)

    @pl.when(s < S - 1)
    def _():
        front.start()


    def project(rows_of, weights, out, base):
        def pair(m, _):
            rows = pl.ds(pl.multiple_of(m * 2 * LANES, 2 * LANES), 2 * LANES)
            prod = lax.dot_general(
                rows_of[...], weights[rows, :], (((1,), (1,)), ((), ())), preferred_element_type=f32
            ).astype(bf16)
            out[base + 2 * m] = prod[:, :LANES]
            out[base + 2 * m + 1] = prod[:, LANES:]
            return _

        lax.fori_loop(0, cpd // 2, pair, 0)

    with jax.named_scope("proj_own"):
        project(cot, w, ga, d * cpd)
    with jax.named_scope("tapswait"):
        for j in range(1, S):
            arrived(kall.at[pl.ds(lax.rem(s + S - j, S) * cps, cps)], ids["taps"] + j)

        @pl.when(s > 0)
        def _():
            arrived(frecv, ids["front"])

    @pl.when(s == 0)
    def _():
        ext[:, pl.ds(0, HB), :] = jnp.zeros((chunks, HB, LANES), f32)

    @pl.when(s > 0)
    def _():
        ext[:, pl.ds(0, HB), :] = frecv[...].astype(f32)

    def convolve(cb, rb):
        tf = kall[cb].astype(f32)
        acc = jnp.zeros((RB, LANES), f32)
        for k in range(K):
            acc = acc + tf[k : k + 1] * ext[cb, pl.ds(HB - k + rb * RB, RB), :]
        cen[cb, pl.ds(rb * RB, RB), :] = acc
        return acc

    def conv_chunk(cb, _):
        for rb in range(T // RB):
            rows = pl.ds(rb * RB, RB)
            dev = convolve(cb, rb) - means[rows, :]
            sum1[rows, :] = sum1[rows, :] + dev
            sum2[rows, :] = sum2[rows, :] + dev * dev
        return _

    with jax.named_scope("conv"):
        for rb in range(T // RB):
            rows = pl.ds(rb * RB, RB)
            acc = convolve(0, rb)
            start = jnp.broadcast_to(jnp.sum(acc, axis=1, keepdims=True) / LANES, (RB, LANES))
            means[rows, :] = start
            sum1[rows, :] = acc - start
            sum2[rows, :] = (acc - start) * (acc - start)
        lax.fori_loop(1, chunks, conv_chunk, 0)
    with jax.named_scope("moments"):
        shift = jnp.sum(sum1[...], axis=1, keepdims=True) / C
        variance = jnp.sum(sum2[...], axis=1, keepdims=True) / C - shift * shift
        means[...] = means[...] + shift
        invs[...] = jnp.broadcast_to(lax.rsqrt(variance + epsilon), (T, LANES))

    def act_chunk(cb, _):
        centred = (cen[cb] - means[...]) * invs[...]
        cen[cb] = centred
        normed = centred * kall[cb].astype(f32)[K : K + 1]
        act[lax.rem(cb, X), cb // X] = (normed * jax.nn.sigmoid(normed)).T.astype(bf16)
        return _

    with jax.named_scope("act"):
        lax.fori_loop(0, chunks, act_chunk, 0)
    send(act.at[x], act_p.at[0], ids["actp"], s, partner)

    near = Z // 2
    low = z < near
    inner_z = jnp.where(low, near - 1, near)
    inner = z == inner_z

    def plane(k):
        if k < near:
            return jnp.where(low, Z - 1 - k, k)
        return jnp.where(low, 0, near) + lax.rem(z + 1 + k, near)

    def planes(k, own):
        if k < Z - 1:
            return [(plane(k) * Y, Y, 0)]
        return [(plane(k) * Y + lax.rem(y + j, Y), 1, j) for j in (range(1) if own else range(1, Y))]

    def send_act(k, own=False):
        for first, size, n in planes(k, own):
            piece = pl.ds(first, size)
            for j in range(1, X):
                send(
                    act.at[lax.rem(x + j, X), piece], act_m.at[j - 1, piece],
                    ids["act"] + (j * Z + k) * Y + n, s, lax.rem(d + 2 * j, N),
                )

    def relay_mirror(p):
        with jax.named_scope("cotwait%d" % p):
            for j in range(1, X):
                for side in range(2):
                    arrived(cot_m.at[j - 1, :, strip(side, p)], ids["cot"] + (j * 2 + p) * 2 + side)
                send(
                    cot_m.at[j - 1, :, strip(other, p)], cot_p.at[j, :, strip(0, p)],
                    ids["cotp"] + j * 2 + p, s, partner,
                )

    def project_mirror():
        for j in range(1, X):
            with jax.named_scope("proj_m"):
                project(cot_m.at[j - 1], w, ga_s.at[j - 1], c * cpd)
                project(cot_m.at[j - 1], w_p, ga_s.at[j - 1], other * cpd)
            for b in range(BLOCKS):
                rows = pl.ds(b * TB, TB)
                send(
                    ga_s.at[j - 1, :, rows], ga.at[pl.ds(x * 2 * cpd, 2 * cpd), rows],
                    ids["ga"] + j * BLOCKS + b, s, lax.rem(d + 2 * (X - j), N),
                )

    dims = (((1,), (0,)), ((), ()))

    def dot(a, b):
        return lax.dot_general(a, b, dims, preferred_element_type=f32)

    LT = H // 2

    def local_plane(k):
        def tile(i, _):
            m, n = plane(k) * Y + i // 2, lax.rem(i, 2)
            cols = pl.ds(pl.multiple_of(n * LT, LT), LT)
            own = pl.ds(pl.multiple_of(c * H + n * LT, LT), LT)
            wacc[m, :, cols] = dot(act[x, m], cot[:, own]) + dot(act_p[0, m], cot_p[0, :, cols])
            return _

        with jax.named_scope("wlocal%d" % k):
            if k == 0:
                arrived(cot_p.at[0], ids["cotp"])
                arrived(act_p.at[0], ids["actp"])
            lax.fori_loop(0, Y * 2, tile, 0)

    NT = H // BLOCKS

    def remote_part(m, n):
        cols = pl.ds(pl.multiple_of(n * NT, NT), NT)
        own = pl.ds(pl.multiple_of(c * H + n * NT, NT), NT)
        acc = wacc[m, :, cols]
        for j in range(1, X):
            acc = acc + dot(act_m[j - 1, m], cot_m[j - 1, :, own]) + dot(act_p[j, m], cot_p[j, :, cols])
        return cols, acc

    def relay_act(k, own=False):
        with jax.named_scope("actwait%d" % k):
            for first, size, n in planes(k, own):
                piece = pl.ds(first, size)
                for j in range(1, X):
                    i = (j * Z + k) * Y + n
                    arrived(act_m.at[j - 1, piece], ids["act"] + i)
                    send(act_m.at[j - 1, piece], act_p.at[j, piece], ids["actp"] + i, s, partner)

    def relayed(k, own=False):
        with jax.named_scope("relaywait%d" % k):
            for first, size, n in planes(k, own):
                for j in range(1, X):
                    arrived(act_p.at[j, pl.ds(first, size)], ids["actp"] + (j * Z + k) * Y + n)

    def own_part(k, off, size):
        def own_tile(n, _):
            m = plane(k) * Y + y
            cols, acc = remote_part(m, n)
            wacc[m, :, cols] = acc
            return _

        lax.fori_loop(off // NT, (off + size) // NT, own_tile, 0)

    def weight_part(k, p):
        off, size = parts[p]
        if p == 0:
            relayed(k)
        if k == 0:
            for j in range(1, X):
                arrived(cot_p.at[j, :, strip(0, p)], ids["cotp"] + j * 2 + p)
        with jax.named_scope("wremote%d%d" % (k, p)):
            for j in range(1, Y):
                to_y = lax.rem(y + j, Y)
                i = (j - 1) * Z + k

                def send_tile(n, _):
                    cols, acc = remote_part(plane(k) * Y + to_y, n)
                    wpart[i, :, cols] = acc.astype(bf16)
                    return _

                lax.fori_loop(off // NT, (off + size) // NT, send_tile, 0)
                send(
                    wpart.at[i, :, strip(0, p)], yrecv.at[i, :, strip(0, p)],
                    ids["y"] + i * 2 + p, z * Y + to_y, d,
                )

            if k < Z - 1:
                own_part(k, off, size)

    def reduce_y(k, p):
        for q in (p,) if k < Z - 1 else (0, 1):
            with jax.named_scope("ywait%d%d" % (k, q)):
                for j in range(1, Y):
                    i = (j - 1) * Z + k
                    arrived(yrecv.at[i, :, strip(0, q)], ids["y"] + i * 2 + q)
        to_z = plane(k)
        m = to_z * Y + y

        def tile(n, _):
            cols = pl.ds(pl.multiple_of(n * LANES, LANES), LANES)
            acc = wacc[m, :, cols]
            for j in range(1, Y):
                acc = acc + yrecv[(j - 1) * Z + k, :, cols].astype(f32)
            if k < Z - 1:
                ysum[k, :, cols] = acc.astype(bf16)
            if k != Z - 2:
                wacc[m, :, cols] = acc
            return _

        off, size = parts[p] if k < Z - 1 else (0, H)
        lax.fori_loop(off // LANES, (off + size) // LANES, tile, 0)
        if k < near:
            r = copy(
                ysum.at[k, :, strip(0, p)], zmid.at[k, :, strip(0, p)], ids["zmid"] + k * 2 + p,
                inner_z * Y + y, d,
            )

            @pl.when(jnp.logical_not(inner))
            def _():
                r.start()

            outer.append(r)
        elif k < Z - 1:
            send(
                ysum.at[k, :, strip(0, p)], zrecv.at[0, :, strip(0, p)], ids["znear"] + p,
                to_z * Y + y, d,
            )

    def reduce_z(k, p):
        to_z = plane(k)
        m = to_z * Y + y
        off, size = parts[p]

        def tile(n, _):
            cols = pl.ds(pl.multiple_of(n * LANES, LANES), LANES)
            ysum[k, :, cols] = (wacc[m, :, cols] + zmid[k, :, cols].astype(f32)).astype(bf16)
            return _

        @pl.when(inner)
        def _():
            with jax.named_scope("zmid%d%d" % (k, p)):
                arrived(zmid.at[k, :, strip(0, p)], ids["zmid"] + k * 2 + p)
            lax.fori_loop(off // LANES, (off + size) // LANES, tile, 0)
            copy(
                ysum.at[k, :, strip(0, p)], zrecv.at[1, :, strip(0, p)], ids["zmid"] + k * 2 + p,
                to_z * Y + y, d, ids["zfar"] + p,
            ).start()

    outer = []

    def fold(v):
        return jnp.sum(v.reshape(v.shape[0] // 8, 8, LANES), axis=0)

    def gradient(b):
        rows = pl.ds(b * TB, TB)
        with jax.named_scope("gawait%d" % b):
            for j in range(1, X):
                origin = lax.rem(x + j, X)
                arrived(ga.at[pl.ds(origin * 2 * cpd, 2 * cpd), rows], ids["ga"] + j * BLOCKS + b)

        def grad_chunk(cb, sums):
            one, two = sums
            centred = cen[cb, rows, :]
            gain = kall[cb].astype(f32)[K : K + 1]
            normed = centred * gain
            sg = jax.nn.sigmoid(normed)
            grad = ga[cb, rows, :].astype(f32) * sg * (1.0 + normed * (1.0 - sg))
            scaled = grad * centred
            kacc[cb, K] = fold(scaled) if b == 0 else kacc[cb, K] + fold(scaled)
            gc[cb, rows, :] = grad * gain
            return one + grad * gain, two + scaled * gain

        zero = jnp.zeros((TB, LANES), f32)
        with jax.named_scope("gradchunk%d" % b):
            one, two = lax.fori_loop(0, chunks, grad_chunk, (zero, zero))
        first = jnp.sum(one, axis=1, keepdims=True) / C
        second = jnp.sum(two, axis=1, keepdims=True) / C
        scale = invs[rows, :]

        def conv_grad(cb, _):
            grad = (gc[cb, rows, :] - first - cen[cb, rows, :] * second) * scale
            gext[cb, rows, :] = grad
            if b == 0:
                bsend[cb] = grad[:HB].astype(bf16)
            return _

        with jax.named_scope("convgrad%d" % b):
            lax.fori_loop(0, chunks, conv_grad, 0)

    def taps_grad(b):
        def taps_chunk(cb, _):
            grad = gext[cb, pl.ds(b * TB, TB), :]
            for k in range(K):
                acc = fold(grad * ext[cb, pl.ds(HB - k + b * TB, TB), :])
                if b > 0:
                    acc = acc + kacc[cb, k]
                if b < BLOCKS - 1:
                    kacc[cb, k] = acc
                else:
                    kg[cb, pl.ds(k, 1), :] = jnp.sum(acc, axis=0, keepdims=True)
            if b == BLOCKS - 1:
                kg[cb, pl.ds(K, 1), :] = jnp.sum(kacc[cb, K], axis=0, keepdims=True)
                kgb[cb] = kg[cb].astype(bf16)
            return _

        with jax.named_scope("taps%d" % b):
            lax.fori_loop(0, chunks, taps_chunk, 0)

    def gated_grad(b):
        rows = pl.ds(b * TB, TB)

        def gated_chunk(cb, _):
            cols = pl.ds(pl.multiple_of(cb * LANES, LANES), LANES)
            tf = kall[cb].astype(f32)
            acc = jnp.zeros((TB, LANES), f32)
            for k in range(K):
                acc = acc + tf[k : k + 1] * gext[cb, pl.ds(k + b * TB, TB), :]
            acc = acc.astype(bf16).astype(f32)
            sig = jax.nn.sigmoid(gate[rows, cols].astype(f32))
            gv[rows, cols] = (acc * sig).astype(bf16)
            gg[rows, cols] = (acc * val[rows, cols].astype(f32) * sig * (1.0 - sig)).astype(bf16)
            return _

        with jax.named_scope("gated%d" % b):
            lax.fori_loop(0, chunks, gated_chunk, 0)

    back = copy(bsend, brecv, ids["back"], lax.rem(s + S - 1, S), d)
    send_act(0)
    send_act(1)
    send_cot(1)
    send_act(2)
    send_act(3)
    arrived(w_p, ids["w"])
    with jax.named_scope("proj_p"):
        project(cot, w_p, ga, partner * cpd)
    local_plane(0)
    local_plane(1)
    local_plane(2)
    relay_mirror(0)
    relay_act(0)
    weight_part(0, 0)
    relay_act(1)
    local_plane(3)
    weight_part(1, 0)
    relay_mirror(1)
    project_mirror()
    send_act(Z - 1, own=True)
    reduce_y(0, 0)
    weight_part(0, 1)
    weight_part(1, 1)
    relay_act(2)
    relay_act(3)
    weight_part(2, 0)
    weight_part(2, 1)
    reduce_y(1, 0)
    reduce_z(0, 0)
    reduce_y(0, 1)
    reduce_y(1, 1)
    weight_part(3, 0)
    weight_part(3, 1)
    gradient(0)

    @pl.when(s > 0)
    def _():
        back.start()

    taps_grad(0)
    gradient(1)
    taps_grad(1)
    reduce_z(1, 0)
    gradient(2)
    taps_grad(2)
    reduce_y(2, 0)
    reduce_z(0, 1)
    reduce_z(1, 1)
    gradient(3)
    taps_grad(3)
    for j in range(1, S):
        to = lax.rem(s + j, S)
        send(kgb.at[pl.ds(to * cps, cps)], krecv.at[j], ids["kg"] + j, to, d)
    reduce_y(2, 1)
    relay_act(3, own=True)
    gated_grad(0)
    relayed(3, own=True)
    own_part(3, 0, H)
    reduce_y(3, 0)
    gated_grad(1)
    gated_grad(2)
    with jax.named_scope("drain"):
        for r in waits + outer:
            r.wait_send()
        waits.clear()
        outer.clear()
    with jax.named_scope("kgwait"):
        for j in range(1, S):
            arrived(krecv.at[j], ids["kg"] + j)
    acc = kg[pl.ds(s * cps, cps)]
    for j in range(1, S):
        acc = acc + krecv[j].astype(f32)
    ksum[...] = acc
    for j in range(1, N):
        send(ksum, k2recv.at[j], ids["k2"] + j, s, lax.rem(d + j, N))
    with jax.named_scope("zwait"):
        for p in range(2):
            arrived(zrecv.at[0, :, strip(0, p)], ids["znear"] + p)
            arrived(zrecv.at[1, :, strip(0, p)], ids["zfar"] + p)

    def final_tile(n, _):
        cols = pl.ds(pl.multiple_of(n * LANES, LANES), LANES)
        acc = wacc[s, :, cols]
        for q in range(2):
            acc = acc + zrecv[q, :, cols].astype(f32)
        acc = acc * factor
        fin[0, :, cols] = acc[:block]
        fin[1, :, cols] = acc[block:]
        return _

    with jax.named_scope("final"):
        lax.fori_loop(0, H // LANES, final_tile, 0)
    send(fin.at[other], fbuf, ids["fin"], s, partner)
    gw[:, half] = fin[c]
    with jax.named_scope("backwait"):
        @pl.when(s < S - 1)
        def _():
            arrived(brecv, ids["back"])

    @pl.when(s == S - 1)
    def _():
        gext[:, pl.ds(T, HB), :] = jnp.zeros((chunks, HB, LANES), f32)

    @pl.when(s < S - 1)
    def _():
        gext[:, pl.ds(T, HB), :] = brecv[...].astype(f32)

    gated_grad(3)
    with jax.named_scope("k2wait"):
        for j in range(1, N):
            arrived(k2recv.at[j], ids["k2"] + j)
            acc = acc + k2recv[j]
    for q in range(cps):
        cols = slice(q * LANES, (q + 1) * LANES)
        kout[:, cols] = acc[q] * factor

    arrived(fbuf, ids["fin"])
    gw[:, ohalf] = fbuf[...]
    for r in waits:
        r.wait_send()

    @pl.when(s < S - 1)
    def _():
        front.wait_send()

    @pl.when(s > 0)
    def _():
        back.wait_send()


def number(*sizes):
    ids, count = {}, 0
    for name, size in sizes:
        ids[name] = count
        count += size
    return ids, count


def hand_over(K, gv_in, gg_in, gw_in, k_in, gv, gg, gw, kout, gout, sem):
    pieces = ((gv_in, gv), (gg_in, gg), (gw_in, gw))
    stores = [pltpu.make_async_copy(a, b, sem.at[i]) for i, (a, b) in enumerate(pieces)]
    for st in stores:
        st.start()
    kout[...] = k_in[:K]
    gout[...] = k_in[K : K + 1]
    for st in stores:
        st.wait()


def pair_call(S, N, Y, T, C, K, HB, KP, cot, val, gate, w, kernel, gain):
    X, Z, H = N // 2, S // Y, C // 2
    chunks, cps, cpd, block = C // LANES, C // LANES // S, C // LANES // N, C // (S * N)
    M, CR = chunks // X, C // N
    ids, count = number(
        ("taps", S), ("front", 1), ("back", 1), ("w", 1), ("cot", X * 4), ("cotp", X * 2),
        ("act", X * Z * Y), ("actp", X * Z * Y), ("ga", X * BLOCKS), ("y", (Y - 1) * Z * 2), ("zmid", Z), ("znear", 2), ("zfar", 2),
        ("fin", 1),
        ("kg", S), ("k2", N),
    )
    vm = pl.BlockSpec(memory_space=pltpu.VMEM)
    hbm = pl.BlockSpec(memory_space=pl.ANY)
    partial = pl.pallas_call(
        functools.partial(pair_kernel, S, N, Y, T, C, K, HB, ids),
        out_shape=(
            jax.ShapeDtypeStruct((T, C), bf16),
            jax.ShapeDtypeStruct((T, C), bf16),
            jax.ShapeDtypeStruct((block, C), f32),
            jax.ShapeDtypeStruct((KP, C // S), f32),
        ),
        in_specs=[hbm] * 6,
        out_specs=(vm,) * 4,
        scratch_shapes=[
            pltpu.VMEM((K, C // S), bf16),
            pltpu.VMEM((C // S,), bf16),
            pltpu.VMEM((cps, KP, LANES), bf16),
            pltpu.VMEM((T, C), bf16),
            pltpu.VMEM((T, C), bf16),
            pltpu.VMEM((T, C), bf16),
            pltpu.VMEM((CR, C), bf16),
            pltpu.VMEM((CR, C), bf16),
            pltpu.VMEM((X - 1, T, C), bf16),
            pltpu.VMEM((X, T, H), bf16),
            pltpu.VMEM((chunks, HB, LANES), bf16),
            pltpu.VMEM((chunks, HB, LANES), bf16),
            pltpu.VMEM((chunks, HB, LANES), bf16),
            pltpu.VMEM((chunks, HB, LANES), bf16),
            pltpu.VMEM((chunks, T + HB, LANES), f32),
            pltpu.VMEM((chunks, T, LANES), f32),
            pltpu.VMEM((chunks, T, LANES), f32),
            pltpu.VMEM((chunks, T + HB, LANES), f32),
            pltpu.VMEM((chunks, KP, LANES), bf16),
            pltpu.VMEM((X, M, LANES, T), bf16),
            pltpu.VMEM((X - 1, M, LANES, T), bf16),
            pltpu.VMEM((X, M, LANES, T), bf16),
            pltpu.VMEM((X - 1, 2 * cpd, T, LANES), bf16),
            pltpu.VMEM((chunks, T, LANES), bf16),
            pltpu.VMEM((M, LANES, H), f32),
            pltpu.VMEM(((Y - 1) * Z, LANES, H), bf16),
            pltpu.VMEM(((Y - 1) * Z, LANES, H), bf16),
            pltpu.VMEM((Z - 1, LANES, H), bf16),
            pltpu.VMEM((Z // 2, LANES, H), bf16),
            pltpu.VMEM((2, LANES, H), bf16),
            pltpu.VMEM((2, block, H), f32),
            pltpu.VMEM((block, H), f32),
            pltpu.VMEM((T, LANES), f32),
            pltpu.VMEM((T, LANES), f32),
            pltpu.VMEM((T, LANES), f32),
            pltpu.VMEM((T, LANES), f32),
            pltpu.VMEM((chunks, K + 1, 8, LANES), f32),
            pltpu.VMEM((chunks, KP, LANES), f32),
            pltpu.VMEM((chunks, KP, LANES), bf16),
            pltpu.VMEM((S, cps, KP, LANES), bf16),
            pltpu.VMEM((cps, KP, LANES), f32),
            pltpu.VMEM((N, cps, KP, LANES), f32),
            pltpu.SemaphoreType.DMA((count,)),
            pltpu.SemaphoreType.DMA((count,)),
            pltpu.SemaphoreType.DMA((6,)),
            pltpu.SemaphoreType.REGULAR((2 * (Z - 2) + 1,)),
        ],
        compiler_params=pltpu.CompilerParams(
            collective_id=0, has_side_effects=True, vmem_limit_bytes=48 * 1024 * 1024
        ),
        name="block_backward",
    )(*(pltpu.with_memory_space_constraint(a, pltpu.HBM) for a in (cot, val, gate, w, kernel, gain)))
    return pl.pallas_call(
        functools.partial(hand_over, K),
        out_shape=(
            jax.ShapeDtypeStruct((T, C), bf16),
            jax.ShapeDtypeStruct((T, C), bf16),
            jax.ShapeDtypeStruct((block, C), f32),
            jax.ShapeDtypeStruct((K, C // S), f32),
            jax.ShapeDtypeStruct((1, C // S), f32),
        ),
        in_specs=[vm] * 4,
        out_specs=(hbm, hbm, hbm, vm, vm),
        scratch_shapes=[
            pltpu.SemaphoreType.DMA((3,)),
        ],
        compiler_params=pltpu.CompilerParams(vmem_limit_bytes=16 * T * LANES),
        name="hand_over",
    )(*partial)


def general_call(S, N, T, C, K, HB, KP, cot, val, gate, w, packed):
    chunks, cps, cpd, block = C // LANES, C // LANES // S, C // LANES // N, C // (S * N)
    ids, count = number(
        ("taps", S), ("front", 1), ("back", 1), ("partner", 1), ("mirror", N // 2 * HALVES),
        ("relay", N // 2 * HALVES), ("act", N), ("ga", N), ("rs", S), ("kg", S), ("k2", N),
    )
    vm = pl.BlockSpec(memory_space=pltpu.VMEM)
    return pl.pallas_call(
        functools.partial(general_kernel, S, N, T, C, K, HB, ids),
        out_shape=(
            jax.ShapeDtypeStruct((T, C), bf16),
            jax.ShapeDtypeStruct((T, C), bf16),
            jax.ShapeDtypeStruct((block, C), f32),
            jax.ShapeDtypeStruct((K, C // S), f32),
            jax.ShapeDtypeStruct((1, C // S), f32),
        ),
        in_specs=[vm] * 5,
        out_specs=(vm,) * 5,
        scratch_shapes=[
            pltpu.VMEM((N, T, C), bf16),
            pltpu.VMEM((chunks, T + HB, LANES), f32),
            pltpu.VMEM((chunks, T, LANES), f32),
            pltpu.VMEM((chunks, T, LANES), f32),
            pltpu.VMEM((chunks, T + HB, LANES), f32),
            pltpu.VMEM((chunks, KP, LANES), bf16),
            pltpu.VMEM((chunks, T, LANES), bf16),
            pltpu.VMEM((N, cpd, T, LANES), bf16),
            pltpu.VMEM((N, cpd, T, LANES), bf16),
            pltpu.VMEM((chunks, T, LANES), bf16),
            pltpu.VMEM((cpd * LANES, C), bf16),
            pltpu.VMEM((S, block, C), bf16),
            pltpu.VMEM((chunks, KP, LANES), f32),
            pltpu.VMEM((S, cps, KP, LANES), f32),
            pltpu.VMEM((cps, KP, LANES), f32),
            pltpu.VMEM((N, cps, KP, LANES), f32),
            pltpu.SemaphoreType.DMA((count,)),
            pltpu.SemaphoreType.DMA((count,)),
        ],
        compiler_params=pltpu.CompilerParams(
            collective_id=0, has_side_effects=True, vmem_limit_bytes=60 * 1024 * 1024
        ),
        name="block_backward",
    )(cot, val, gate, w, packed)


def shards(out_cotangent, value_pre, gate_pre, out_weight, conv_kernel, norm_gain):
    S, N = lax.axis_size("sp"), lax.axis_size("dp")
    _, T, C = out_cotangent.shape
    K = conv_kernel.shape[0]
    chunks, cps = C // LANES, C // LANES // S
    HB = -(-(K - 1) // 16) * 16
    KP = -(-(K + 1) // 16) * 16
    args = (out_cotangent[0], value_pre[0], gate_pre[0], out_weight)
    X = N // 2
    if N == 2 * X > 2 and S == 2 * 2 * X and chunks == S * X:
        outs = pair_call(S, N, X, T, C, K, HB, KP, *args, conv_kernel, norm_gain)
    else:
        packed = jnp.concatenate(
            [conv_kernel, norm_gain[None], jnp.zeros((KP - K - 1, C // S), bf16)], axis=0
        )
        packed = jnp.transpose(packed.reshape(KP, cps, LANES), (1, 0, 2))
        outs = general_call(S, N, T, C, K, HB, KP, *args, packed)
    grad_value, grad_gate, grad_weight, grad_taps, grad_gain = outs
    return grad_value[None], grad_gate[None], grad_weight, grad_taps, grad_gain[0]


def solution(mesh):
    placed = (
        P("dp", "sp", None),
        P("dp", "sp", None),
        P("dp", "sp", None),
        P("dp", None),
        P(None, "sp"),
        P("sp"),
    )
    return jax.shard_map(
        shards,
        mesh=mesh,
        in_specs=placed,
        out_specs=(
            P("dp", "sp", None),
            P("dp", "sp", None),
            P(("sp", "dp"), None),
            P(None, "sp"),
            P("sp"),
        ),
        check_vma=False,
    )
```

```python
import functools

import jax
import jax.numpy as jnp
from jax import lax
from jax.experimental import pallas as pl
from jax.experimental.pallas import tpu as pltpu
from jax.sharding import PartitionSpec as P

epsilon = 1e-05
LANES = 128
HALVES = 2
BLOCKS = 4
f32 = jnp.float32
bf16 = jnp.bfloat16


def general_kernel(
    S, N, T, C, K, HB, ids,
    cot, val, gate, w, taps,
    gv, gg, gw, kout, gout,
    cot_all, ext, cen, gc, gext, kall, act, act_all, ga_send, ga, wpart, rbuf,
    kg, krecv, ksum, k2recv, send_sem, recv_sem,
):
    s = lax.axis_index("sp")
    d = lax.axis_index("dp")
    chunks = C // LANES
    cps = chunks // S
    cpd = chunks // N
    block = C // (S * N)
    RB = min(T, 128)
    total = S * N
    me = s * N + d
    partner = d + 1 - 2 * lax.rem(d, 2)
    factor = float(S * N * T) ** (-0.5)
    hrows = T // HALVES
    waits = []

    def copy(src, dst, i, to_s, to_d):
        return pltpu.make_async_remote_copy(
            src_ref=src, dst_ref=dst, send_sem=send_sem.at[i], recv_sem=recv_sem.at[i],
            device_id={"sp": to_s, "dp": to_d}, device_id_type=pl.DeviceIdType.MESH,
        )

    def send(src, dst, i, to_s, to_d):
        c = copy(src, dst, i, to_s, to_d)
        c.start()
        waits.append(c)

    def arrived(dst, i):
        copy(dst, dst, i, s, partner).wait_recv()

    barrier = pltpu.get_barrier_semaphore()

    def greet(j, _):
        other = lax.rem(me + j, total)
        pl.semaphore_signal(
            barrier, inc=1, device_id={"sp": other // N, "dp": lax.rem(other, N)},
            device_id_type=pl.DeviceIdType.MESH,
        )
        return _

    lax.fori_loop(1, total, greet, 0)
    def gate_chunk(cb, _):
        cols = pl.ds(pl.multiple_of(cb * LANES, LANES), LANES)
        sig = jax.nn.sigmoid(gate[:, cols].astype(f32))
        ext[cb, pl.ds(HB, T), :] = (val[:, cols].astype(f32) * sig).astype(bf16).astype(f32)
        return _

    lax.fori_loop(0, chunks, gate_chunk, 0)
    pl.semaphore_wait(barrier, total - 1)

    for j in range(1, S):
        send(taps, kall.at[pl.ds(s * cps, cps)], ids["taps"] + j, lax.rem(s + j, S), d)
    following = lax.rem(s + 1, S)
    preceding = lax.rem(s + S - 1, S)
    send(ext.at[:, pl.ds(T, HB), :], ext.at[:, pl.ds(0, HB), :], ids["front"], following, d)
    for j in range(1, N // 2):
        for h in range(HALVES):
            rows = pl.ds(h * hrows, hrows)
            send(cot.at[rows], cot_all.at[d, rows], ids["mirror"] + j * HALVES + h, s, lax.rem(d + 2 * j, N))
    send(cot, cot_all.at[d], ids["partner"], s, partner)
    kall[pl.ds(s * cps, cps)] = taps[...]
    cot_all[d] = cot[...]
    for j in range(1, S):
        arrived(kall.at[pl.ds(lax.rem(s + S - j, S) * cps, cps)], ids["taps"] + j)
    arrived(ext.at[:, pl.ds(0, HB), :], ids["front"])

    @pl.when(s == 0)
    def _():
        ext[:, pl.ds(0, HB), :] = jnp.zeros((chunks, HB, LANES), f32)

    def conv_chunk(cb, sums):
        tf = kall[cb].astype(f32)
        parts = []
        for rb in range(T // RB):
            acc = jnp.zeros((RB, LANES), f32)
            for k in range(K):
                acc = acc + tf[k : k + 1] * ext[cb, pl.ds(HB - k + rb * RB, RB), :]
            cen[cb, pl.ds(rb * RB, RB), :] = acc
            parts.append(jnp.sum(acc, axis=1, keepdims=True))
        return sums + jnp.concatenate(parts, axis=0)

    column = jnp.zeros((T, 1), f32)
    mean = lax.fori_loop(0, chunks, conv_chunk, column) / C

    def square_chunk(cb, sums):
        dev = cen[cb] - mean
        return sums + dev * dev

    squares = lax.fori_loop(0, chunks, square_chunk, jnp.zeros((T, LANES), f32))
    inv = lax.rsqrt(jnp.sum(squares, axis=1, keepdims=True) / C + epsilon)

    def relay():
        for j in range(1, N // 2):
            origin = lax.rem(d + N - 2 * j, N)
            for h in range(HALVES):
                piece = cot_all.at[origin, pl.ds(h * hrows, hrows)]
                arrived(piece, ids["mirror"] + j * HALVES + h)
                send(piece, piece, ids["relay"] + j * HALVES + h, s, partner)

    def act_chunk(cb, _):
        centred = (cen[cb] - mean) * inv
        cen[cb] = centred
        normed = centred * kall[cb].astype(f32)[K : K + 1]
        act[cb] = (normed * jax.nn.sigmoid(normed)).astype(bf16)
        return _

    lax.fori_loop(0, chunks, act_chunk, 0)
    for j in range(1, N):
        to = lax.rem(d + j, N)
        send(act.at[pl.ds(to * cpd, cpd)], act_all.at[d], ids["act"] + j, s, to)
    act_all[d] = act[pl.ds(d * cpd, cpd)]

    def project(source, slot):
        def pair(m, _):
            rows = pl.ds(pl.multiple_of(m * 2 * LANES, 2 * LANES), 2 * LANES)
            out = lax.dot_general(
                cot_all[source], w[rows, :], (((1,), (1,)), ((), ())), preferred_element_type=f32
            ).astype(bf16)
            ga_send[slot, 2 * m] = out[:, :LANES]
            ga_send[slot, 2 * m + 1] = out[:, LANES:]
            return _

        lax.fori_loop(0, cpd // 2, pair, 0)

    mine = pl.ds(d * cpd, cpd)
    project(d, 0)
    ga[mine] = ga_send[0]
    arrived(cot_all.at[partner], ids["partner"])
    project(partner, 1)
    send(ga_send.at[1], ga.at[mine], ids["ga"] + 1, s, partner)
    relay()
    for j in range(1, N // 2):
        origin = lax.rem(d + N - 2 * j, N)
        project(origin, 2 * j)
        send(ga_send.at[2 * j], ga.at[mine], ids["ga"] + 2 * j, s, origin)
    for j in range(1, N // 2):
        origin = lax.rem(partner + N - 2 * j, N)
        for h in range(HALVES):
            arrived(cot_all.at[origin, pl.ds(h * hrows, hrows)], ids["relay"] + j * HALVES + h)
        project(origin, 2 * j + 1)
        send(ga_send.at[2 * j + 1], ga.at[mine], ids["ga"] + 2 * j + 1, s, origin)

    for j in range(1, N):
        arrived(act_all.at[lax.rem(d + N - j, N)], ids["act"] + j)
    NT = min(C, 512)

    def weight_tile(i, _):
        m, n = i // (C // NT), lax.rem(i, C // NT)
        cols = pl.ds(pl.multiple_of(n * NT, NT), NT)
        acc = jnp.zeros((LANES, NT), f32)
        for q in range(N):
            acc = acc + lax.dot_general(
                act_all[q, m], cot_all[q, :, cols], (((0,), (0,)), ((), ())),
                preferred_element_type=f32,
            )
        wpart[pl.ds(pl.multiple_of(m * LANES, LANES), LANES), cols] = acc.astype(bf16)
        return _

    lax.fori_loop(0, cpd * (C // NT), weight_tile, 0)

    def block_of(j):
        i = lax.rem(s + j, S)
        owner = d * S + i
        rows = pl.ds(pl.multiple_of(i * block, block), block)
        return owner, rows, pltpu.make_async_remote_copy(
            src_ref=wpart.at[rows], dst_ref=rbuf.at[s], send_sem=send_sem.at[ids["rs"] + j],
            recv_sem=recv_sem.at[ids["rs"] + s],
            device_id={"sp": owner // N, "dp": lax.rem(owner, N)},
            device_id_type=pl.DeviceIdType.MESH,
        )

    def send_blocks(first, last):
        for j in range(first, last):
            owner, rows, c = block_of(j)

            @pl.when(owner != me)
            def _():
                c.start()

            @pl.when(owner == me)
            def _():
                rbuf[s] = wpart[rows, :]

    send_blocks(0, S // 2)

    for j in range(1, N // 2):
        arrived(ga.at[pl.ds(lax.rem(d + 2 * j, N) * cpd, cpd)], ids["ga"] + 2 * j)
        arrived(ga.at[pl.ds(lax.rem(partner + 2 * j, N) * cpd, cpd)], ids["ga"] + 2 * j + 1)
    arrived(ga.at[pl.ds(partner * cpd, cpd)], ids["ga"] + 1)

    def grad_chunk(cb, sums):
        one, two = sums
        centred = cen[cb]
        gain = kall[cb].astype(f32)[K : K + 1]
        normed = centred * gain
        sg = jax.nn.sigmoid(normed)
        grad = ga[cb].astype(f32) * sg * (1.0 + normed * (1.0 - sg))
        kg[cb, pl.ds(K, 1), :] = jnp.sum(grad * centred, axis=0, keepdims=True)
        grad = grad * gain
        gc[cb] = grad
        return one + grad, two + grad * centred

    zero = jnp.zeros((T, LANES), f32)
    one, two = lax.fori_loop(0, chunks, grad_chunk, (zero, zero))
    first = jnp.sum(one, axis=1, keepdims=True) / C
    second = jnp.sum(two, axis=1, keepdims=True) / C

    def conv_grad(cb, _):
        gext[cb, pl.ds(0, T), :] = (gc[cb] - first - cen[cb] * second) * inv
        return _

    lax.fori_loop(0, chunks, conv_grad, 0)
    send(gext.at[:, pl.ds(0, HB), :], gext.at[:, pl.ds(T, HB), :], ids["back"], preceding, d)

    def taps_chunk(cb, _):
        for k in range(K):
            acc = jnp.zeros((8, LANES), f32)
            for rb in range(T // RB):
                prod = gext[cb, pl.ds(rb * RB, RB), :] * ext[cb, pl.ds(HB - k + rb * RB, RB), :]
                acc = acc + jnp.sum(prod.reshape(RB // 8, 8, LANES), axis=0)
            kg[cb, pl.ds(k, 1), :] = jnp.sum(acc, axis=0, keepdims=True)
        return _

    lax.fori_loop(0, chunks, taps_chunk, 0)
    for j in range(1, S):
        to = lax.rem(s + j, S)
        send(kg.at[pl.ds(to * cps, cps)], krecv.at[j], ids["kg"] + j, to, d)
    send_blocks(S // 2, S)

    arrived(gext.at[:, pl.ds(T, HB), :], ids["back"])

    @pl.when(s == S - 1)
    def _():
        gext[:, pl.ds(T, HB), :] = jnp.zeros((chunks, HB, LANES), f32)

    def gated_chunk(cb, _):
        cols = pl.ds(pl.multiple_of(cb * LANES, LANES), LANES)
        tf = kall[cb].astype(f32)
        for rb in range(T // RB):
            rows = pl.ds(rb * RB, RB)
            acc = jnp.zeros((RB, LANES), f32)
            for k in range(K):
                acc = acc + tf[k : k + 1] * gext[cb, pl.ds(k + rb * RB, RB), :]
            acc = acc.astype(bf16).astype(f32)
            sig = jax.nn.sigmoid(gate[rows, cols].astype(f32))
            gv[rows, cols] = (acc * sig).astype(bf16)
            gg[rows, cols] = (acc * val[rows, cols].astype(f32) * sig * (1.0 - sig)).astype(bf16)
        return _

    lax.fori_loop(0, chunks, gated_chunk, 0)

    acc = kg[pl.ds(s * cps, cps)]
    for j in range(1, S):
        arrived(krecv.at[j], ids["kg"] + j)
        acc = acc + krecv[j]
    ksum[...] = acc
    for j in range(1, N):
        send(ksum, k2recv.at[j], ids["k2"] + j, s, lax.rem(d + j, N))
    for j in range(1, N):
        arrived(k2recv.at[j], ids["k2"] + j)
        acc = acc + k2recv[j]
    for c in range(cps):
        cols = slice(c * LANES, (c + 1) * LANES)
        kout[:, cols] = (acc[c] * factor)[:K]
        gout[:, cols] = (acc[c] * factor)[K : K + 1]

    home = me // S
    for q in range(S):
        @pl.when(jnp.logical_or(q != s, home != d))
        def _():
            arrived(rbuf.at[q], ids["rs"] + q)

    def sum_tile(n, _):
        cols = pl.ds(pl.multiple_of(n * LANES, LANES), LANES)
        acc = rbuf[0, :, cols].astype(f32)
        for q in range(1, S):
            acc = acc + rbuf[q, :, cols].astype(f32)
        gw[:, cols] = acc * factor
        return _

    lax.fori_loop(0, chunks, sum_tile, 0)
    for j in range(S):
        owner, rows, c = block_of(j)

        @pl.when(owner != me)
        def _():
            c.wait_send()

    for c in waits:
        c.wait_send()


def pair_kernel(
    S, N, Y, T, C, K, HB, ids,
    cot_in, val_in, gate_in, w_in, kernel_in, gain_in,
    gv, gg, gw, kout,
    kernel, gain, taps, cot, val, gate, w, w_p, cot_m, cot_p, fsend, frecv, bsend, brecv, ext, cen, gc, gext, kall,
    act, act_m, act_p, ga_s, ga, wacc, wpart, yrecv, ysum, zmid, zrecv, fin, fbuf,
    means, invs, sum1, sum2, kacc, kg, kgb, krecv, ksum, k2recv, send_sem, recv_sem, load_sem, ready,
):
    s = lax.axis_index("sp")
    d = lax.axis_index("dp")
    X, Z, H = N // 2, S // Y, C // 2
    x, c = d // 2, lax.rem(d, 2)
    y, z = lax.rem(s, Y), s // Y
    other = 1 - c
    partner = d + 1 - 2 * c
    chunks = C // LANES
    cps = chunks // S
    cpd = chunks // N
    block = C // (S * N)
    M = chunks // X
    RB = min(T, 128)
    TB = T // BLOCKS
    factor = float(S * N * T) ** (-0.5)
    waits = []

    def copy(src, dst, i, to_s, to_d, j=None):
        return pltpu.make_async_remote_copy(
            src_ref=src, dst_ref=dst, send_sem=send_sem.at[i],
            recv_sem=recv_sem.at[i if j is None else j],
            device_id={"sp": to_s, "dp": to_d}, device_id_type=pl.DeviceIdType.MESH,
        )

    def send(src, dst, i, to_s, to_d, j=None):
        r = copy(src, dst, i, to_s, to_d, j)
        r.start()
        waits.append(r)

    def arrived(dst, i):
        copy(dst, dst, i, s, partner).wait_recv()

    loads = [
        pltpu.make_async_copy(a, b, load_sem.at[i])
        for i, (a, b) in enumerate((
            (gate_in, gate), (val_in, val), (cot_in, cot), (w_in, w), (kernel_in, kernel), (gain_in, gain),
        ))
    ]
    for l in loads:
        l.start()

    barrier = pltpu.get_barrier_semaphore()

    def signal(sem, to_s, to_d):
        pl.semaphore_signal(
            sem, inc=1, device_id={"sp": to_s, "dp": to_d}, device_id_type=pl.DeviceIdType.MESH
        )

    def along_z(action):
        @pl.when(z > 0)
        def _():
            action(0, s - Y)

        @pl.when(z < Z - 1)
        def _():
            action(1, s + Y)

    signal(barrier, s, partner)
    for j in range(1, X):
        signal(barrier, s, lax.rem(d + 2 * j, N))
    for j in range(1, Y):
        signal(barrier, z * Y + lax.rem(y + j, Y), d)
    along_z(lambda side, to_s: signal(barrier, to_s, d))
    loads[2].wait()
    with jax.named_scope("barrierwait"):
        pl.semaphore_wait(barrier, X + Y - 1 + jnp.where(z > 0, 1, 0) + jnp.where(z < Z - 1, 1, 0))

    def pass_on(r):
        along_z(lambda side, to_s: signal(ready.at[2 * r + 1 - side], to_s, d))

    def passed(r):
        along_z(lambda side, to_s: pl.semaphore_wait(ready.at[2 * r + side], 1))

    pass_on(0)
    strips = ((0, H - H // BLOCKS), (H - H // BLOCKS, H // BLOCKS))
    parts = ((0, H // 2), (H // 2, H // BLOCKS), (H - H // BLOCKS, H // BLOCKS))
    P = len(parts)

    def strip(side, p):
        return pl.ds(pl.multiple_of(side * H + strips[p][0], LANES), strips[p][1])

    def part(p):
        return pl.ds(parts[p][0], parts[p][1])

    def send_cot(p):
        for j in range(1, X):
            for side in range(2):
                send(
                    cot.at[:, strip(side, p)], cot_m.at[j - 1, :, strip(side, p)],
                    ids["cot"] + (j * 2 + p) * 2 + side, s, lax.rem(d + 2 * j, N),
                )

    send_cot(0)
    loads[0].wait()
    loads[1].wait()

    def gate_chunk(cb, _):
        cols = pl.ds(pl.multiple_of(cb * LANES, LANES), LANES)
        sig = jax.nn.sigmoid(gate[:, cols].astype(f32))
        gated = (val[:, cols].astype(f32) * sig).astype(bf16)
        ext[cb, pl.ds(HB, T), :] = gated.astype(f32)
        fsend[cb] = gated[T - HB :]
        return _

    with jax.named_scope("gate"):
        lax.fori_loop(0, chunks, gate_chunk, 0)
    loads[4].wait()
    loads[5].wait()
    KP = taps.shape[1]
    for q in range(cps):
        cols = slice(q * LANES, (q + 1) * LANES)
        taps[q] = jnp.concatenate(
            [kernel[:, cols].astype(f32), gain[cols].astype(f32).reshape(1, LANES)]
            + [jnp.zeros((KP - K - 1, LANES), f32)] * (KP > K + 1),
            axis=0,
        ).astype(bf16)
    half = pl.ds(pl.multiple_of(c * H, LANES), H)
    ohalf = pl.ds(pl.multiple_of(other * H, LANES), H)
    loads[3].wait()
    send(w, w_p, ids["w"], s, partner)
    send(cot.at[:, ohalf], cot_p.at[0], ids["cotp"], s, partner)
    kall[pl.ds(s * cps, cps)] = taps[...]
    with jax.named_scope("ready"):
        for r in range(Z - 2):
            if r > 0:
                pass_on(r)
            passed(r)
        for j in range(1, Y):
            signal(ready.at[2 * (Z - 2)], z * Y + lax.rem(y + j, Y), d)
        pl.semaphore_wait(ready.at[2 * (Z - 2)], Y - 1)
    for j in range(1, S):
        send(taps, kall.at[pl.ds(s * cps, cps)], ids["taps"] + j, lax.rem(s + j, S), d)
    front = copy(fsend, frecv, ids["front"], lax.rem(s + 1, S), d)

    @pl.when(s < S - 1)
    def _():
        front.start()


    def project(rows_of, weights, out, base):
        def pair(m, _):
            rows = pl.ds(pl.multiple_of(m * 2 * LANES, 2 * LANES), 2 * LANES)
            prod = lax.dot_general(
                rows_of[...], weights[rows, :], (((1,), (1,)), ((), ())), preferred_element_type=f32
            ).astype(bf16)
            out[base + 2 * m] = prod[:, :LANES]
            out[base + 2 * m + 1] = prod[:, LANES:]
            return _

        lax.fori_loop(0, cpd // 2, pair, 0)

    with jax.named_scope("proj_own"):
        project(cot, w, ga, d * cpd)
    with jax.named_scope("tapswait"):
        for j in range(1, S):
            arrived(kall.at[pl.ds(lax.rem(s + S - j, S) * cps, cps)], ids["taps"] + j)

        @pl.when(s > 0)
        def _():
            arrived(frecv, ids["front"])

    @pl.when(s == 0)
    def _():
        ext[:, pl.ds(0, HB), :] = jnp.zeros((chunks, HB, LANES), f32)

    @pl.when(s > 0)
    def _():
        ext[:, pl.ds(0, HB), :] = frecv[...].astype(f32)

    def convolve(cb, rb):
        tf = kall[cb].astype(f32)
        acc = jnp.zeros((RB, LANES), f32)
        for k in range(K):
            acc = acc + tf[k : k + 1] * ext[cb, pl.ds(HB - k + rb * RB, RB), :]
        cen[cb, pl.ds(rb * RB, RB), :] = acc
        return acc

    def conv_chunk(cb, _):
        for rb in range(T // RB):
            rows = pl.ds(rb * RB, RB)
            dev = convolve(cb, rb) - means[rows, :]
            sum1[rows, :] = sum1[rows, :] + dev
            sum2[rows, :] = sum2[rows, :] + dev * dev
        return _

    with jax.named_scope("conv"):
        for rb in range(T // RB):
            rows = pl.ds(rb * RB, RB)
            acc = convolve(0, rb)
            start = jnp.broadcast_to(jnp.sum(acc, axis=1, keepdims=True) / LANES, (RB, LANES))
            means[rows, :] = start
            sum1[rows, :] = acc - start
            sum2[rows, :] = (acc - start) * (acc - start)
        lax.fori_loop(1, chunks, conv_chunk, 0)
    with jax.named_scope("moments"):
        shift = jnp.sum(sum1[...], axis=1, keepdims=True) / C
        variance = jnp.sum(sum2[...], axis=1, keepdims=True) / C - shift * shift
        means[...] = means[...] + shift
        invs[...] = jnp.broadcast_to(lax.rsqrt(variance + epsilon), (T, LANES))

    def act_chunk(cb, _):
        centred = (cen[cb] - means[...]) * invs[...]
        cen[cb] = centred
        normed = centred * kall[cb].astype(f32)[K : K + 1]
        act[lax.rem(cb, X), cb // X] = (normed * jax.nn.sigmoid(normed)).T.astype(bf16)
        return _

    with jax.named_scope("act"):
        lax.fori_loop(0, chunks, act_chunk, 0)
    send(act.at[x], act_p.at[0], ids["actp"], s, partner)

    near = Z // 2
    low = z < near
    inner_z = jnp.where(low, near - 1, near)
    inner = z == inner_z

    def plane(k):
        if k < near:
            return jnp.where(low, Z - 1 - k, k)
        return jnp.where(low, 0, near) + lax.rem(z + 1 + k, near)

    def planes(k, own):
        if k < Z - 1:
            return [(plane(k) * Y, Y, 0)]
        return [(plane(k) * Y + lax.rem(y + j, Y), 1, j) for j in (range(1) if own else range(1, Y))]

    def send_act(k, own=False):
        for first, size, n in planes(k, own):
            piece = pl.ds(first, size)
            for j in range(1, X):
                send(
                    act.at[lax.rem(x + j, X), piece], act_m.at[j - 1, piece],
                    ids["act"] + (j * Z + k) * Y + n, s, lax.rem(d + 2 * j, N),
                )

    def relay_mirror(p):
        with jax.named_scope("cotwait%d" % p):
            for j in range(1, X):
                for side in range(2):
                    arrived(cot_m.at[j - 1, :, strip(side, p)], ids["cot"] + (j * 2 + p) * 2 + side)
                send(
                    cot_m.at[j - 1, :, strip(other, p)], cot_p.at[j, :, strip(0, p)],
                    ids["cotp"] + j * 2 + p, s, partner,
                )

    def project_mirror():
        for j in range(1, X):
            with jax.named_scope("proj_m"):
                project(cot_m.at[j - 1], w, ga_s.at[j - 1], c * cpd)
                project(cot_m.at[j - 1], w_p, ga_s.at[j - 1], other * cpd)
            for b in range(BLOCKS):
                rows = pl.ds(b * TB, TB)
                send(
                    ga_s.at[j - 1, :, rows], ga.at[pl.ds(x * 2 * cpd, 2 * cpd), rows],
                    ids["ga"] + j * BLOCKS + b, s, lax.rem(d + 2 * (X - j), N),
                )

    dims = (((1,), (0,)), ((), ()))

    def dot(a, b):
        return lax.dot_general(a, b, dims, preferred_element_type=f32)

    LT = H // 2

    def local_plane(k):
        def tile(i, _):
            m, n = plane(k) * Y + i // 2, lax.rem(i, 2)
            cols = pl.ds(pl.multiple_of(n * LT, LT), LT)
            own = pl.ds(pl.multiple_of(c * H + n * LT, LT), LT)
            wacc[m, :, cols] = dot(act[x, m], cot[:, own]) + dot(act_p[0, m], cot_p[0, :, cols])
            return _

        with jax.named_scope("wlocal%d" % k):
            if k == 0:
                arrived(cot_p.at[0], ids["cotp"])
                arrived(act_p.at[0], ids["actp"])
            lax.fori_loop(0, Y * 2, tile, 0)

    NT = H // BLOCKS

    def remote_part(m, n):
        cols = pl.ds(pl.multiple_of(n * NT, NT), NT)
        own = pl.ds(pl.multiple_of(c * H + n * NT, NT), NT)
        acc = wacc[m, :, cols]
        for j in range(1, X):
            acc = acc + dot(act_m[j - 1, m], cot_m[j - 1, :, own]) + dot(act_p[j, m], cot_p[j, :, cols])
        return cols, acc

    def relay_act(k, own=False):
        with jax.named_scope("actwait%d" % k):
            for first, size, n in planes(k, own):
                piece = pl.ds(first, size)
                for j in range(1, X):
                    i = (j * Z + k) * Y + n
                    arrived(act_m.at[j - 1, piece], ids["act"] + i)
                    send(act_m.at[j - 1, piece], act_p.at[j, piece], ids["actp"] + i, s, partner)

    def relayed(k, own=False):
        with jax.named_scope("relaywait%d" % k):
            for first, size, n in planes(k, own):
                for j in range(1, X):
                    arrived(act_p.at[j, pl.ds(first, size)], ids["actp"] + (j * Z + k) * Y + n)

    def own_part(k, off, size):
        def own_tile(n, _):
            m = plane(k) * Y + y
            cols, acc = remote_part(m, n)
            wacc[m, :, cols] = acc
            return _

        lax.fori_loop(off // NT, (off + size) // NT, own_tile, 0)

    def weight_part(k, p):
        off, size = parts[p]
        if p == 0:
            relayed(k)
        if k == 0 and p != 1:
            q = 0 if p == 0 else 1
            for j in range(1, X):
                arrived(cot_p.at[j, :, strip(0, q)], ids["cotp"] + j * 2 + q)
        with jax.named_scope("wremote%d%d" % (k, p)):
            for j in range(1, Y):
                to_y = lax.rem(y + j, Y)
                i = (j - 1) * Z + k

                def send_tile(n, _):
                    cols, acc = remote_part(plane(k) * Y + to_y, n)
                    wpart[i, :, cols] = acc.astype(bf16)
                    return _

                lax.fori_loop(off // NT, (off + size) // NT, send_tile, 0)
                send(
                    wpart.at[i, :, part(p)], yrecv.at[i, :, part(p)],
                    ids["y"] + i * P + p, z * Y + to_y, d,
                )

            if k < Z - 1:
                own_part(k, off, size)

    def reduce_y(k, p):
        for q in (p,) if k < Z - 1 else range(P):
            with jax.named_scope("ywait%d%d" % (k, q)):
                for j in range(1, Y):
                    i = (j - 1) * Z + k
                    arrived(yrecv.at[i, :, part(q)], ids["y"] + i * P + q)
        to_z = plane(k)
        m = to_z * Y + y

        def tile(n, _):
            cols = pl.ds(pl.multiple_of(n * LANES, LANES), LANES)
            acc = wacc[m, :, cols]
            for j in range(1, Y):
                acc = acc + yrecv[(j - 1) * Z + k, :, cols].astype(f32)
            if k < Z - 1:
                ysum[k, :, cols] = acc.astype(bf16)
            if k != Z - 2:
                wacc[m, :, cols] = acc
            return _

        off, size = parts[p] if k < Z - 1 else (0, H)
        lax.fori_loop(off // LANES, (off + size) // LANES, tile, 0)
        if k < near:
            r = copy(
                ysum.at[k, :, part(p)], zmid.at[k, :, part(p)], ids["zmid"] + k * P + p,
                inner_z * Y + y, d,
            )

            @pl.when(jnp.logical_not(inner))
            def _():
                r.start()

            outer.append(r)
        elif k < Z - 1:
            send(
                ysum.at[k, :, part(p)], zrecv.at[0, :, part(p)], ids["znear"] + p,
                to_z * Y + y, d,
            )

    def reduce_z(k, p):
        to_z = plane(k)
        m = to_z * Y + y
        off, size = parts[p]

        def tile(n, _):
            cols = pl.ds(pl.multiple_of(n * LANES, LANES), LANES)
            ysum[k, :, cols] = (wacc[m, :, cols] + zmid[k, :, cols].astype(f32)).astype(bf16)
            return _

        @pl.when(inner)
        def _():
            with jax.named_scope("zmid%d%d" % (k, p)):
                arrived(zmid.at[k, :, part(p)], ids["zmid"] + k * P + p)
            lax.fori_loop(off // LANES, (off + size) // LANES, tile, 0)
            copy(
                ysum.at[k, :, part(p)], zrecv.at[1, :, part(p)], ids["zmid"] + k * P + p,
                to_z * Y + y, d, ids["zfar"] + p,
            ).start()

    outer = []

    def fold(v):
        return jnp.sum(v.reshape(v.shape[0] // 8, 8, LANES), axis=0)

    def gradient(b):
        rows = pl.ds(b * TB, TB)
        with jax.named_scope("gawait%d" % b):
            for j in range(1, X):
                origin = lax.rem(x + j, X)
                arrived(ga.at[pl.ds(origin * 2 * cpd, 2 * cpd), rows], ids["ga"] + j * BLOCKS + b)

        def grad_chunk(cb, sums):
            one, two = sums
            centred = cen[cb, rows, :]
            gain = kall[cb].astype(f32)[K : K + 1]
            normed = centred * gain
            sg = jax.nn.sigmoid(normed)
            grad = ga[cb, rows, :].astype(f32) * sg * (1.0 + normed * (1.0 - sg))
            scaled = grad * centred
            kacc[cb, K] = fold(scaled) if b == 0 else kacc[cb, K] + fold(scaled)
            gc[cb, rows, :] = grad * gain
            return one + grad * gain, two + scaled * gain

        zero = jnp.zeros((TB, LANES), f32)
        with jax.named_scope("gradchunk%d" % b):
            one, two = lax.fori_loop(0, chunks, grad_chunk, (zero, zero))
        first = jnp.sum(one, axis=1, keepdims=True) / C
        second = jnp.sum(two, axis=1, keepdims=True) / C
        scale = invs[rows, :]

        def conv_grad(cb, _):
            grad = (gc[cb, rows, :] - first - cen[cb, rows, :] * second) * scale
            gext[cb, rows, :] = grad
            if b == 0:
                bsend[cb] = grad[:HB].astype(bf16)
            return _

        with jax.named_scope("convgrad%d" % b):
            lax.fori_loop(0, chunks, conv_grad, 0)

    def kg_copy(off):
        to = lax.rem(s + off, S)
        return copy(kgb.at[pl.ds(to * cps, cps)], krecv.at[off], ids["kg"] + off, to, d)

    def taps_grad(b):
        def taps_chunk(cb, _):
            grad = gext[cb, pl.ds(b * TB, TB), :]
            for k in range(K):
                acc = fold(grad * ext[cb, pl.ds(HB - k + b * TB, TB), :])
                if b > 0:
                    acc = acc + kacc[cb, k]
                if b < BLOCKS - 1:
                    kacc[cb, k] = acc
                else:
                    kg[cb, pl.ds(k, 1), :] = jnp.sum(acc, axis=0, keepdims=True)
            if b == BLOCKS - 1:
                kg[cb, pl.ds(K, 1), :] = jnp.sum(kacc[cb, K], axis=0, keepdims=True)
                kgb[cb] = kg[cb].astype(bf16)
            return _

        def taps_owner(n, _):
            off = 1 + lax.rem(n + S // 2 - 1, S - 1)
            to = lax.rem(s + off, S)
            lax.fori_loop(to * cps, to * cps + cps, taps_chunk, 0)
            kg_copy(off).start()
            return _

        with jax.named_scope("taps%d" % b):
            if b < BLOCKS - 1:
                lax.fori_loop(0, chunks, taps_chunk, 0)
            else:
                lax.fori_loop(0, S - 1, taps_owner, 0)
                lax.fori_loop(s * cps, s * cps + cps, taps_chunk, 0)

    def gated_grad(b):
        rows = pl.ds(b * TB, TB)

        def gated_chunk(cb, _):
            cols = pl.ds(pl.multiple_of(cb * LANES, LANES), LANES)
            tf = kall[cb].astype(f32)
            acc = jnp.zeros((TB, LANES), f32)
            for k in range(K):
                acc = acc + tf[k : k + 1] * gext[cb, pl.ds(k + b * TB, TB), :]
            acc = acc.astype(bf16).astype(f32)
            sig = jax.nn.sigmoid(gate[rows, cols].astype(f32))
            gv[rows, cols] = (acc * sig).astype(bf16)
            gg[rows, cols] = (acc * val[rows, cols].astype(f32) * sig * (1.0 - sig)).astype(bf16)
            return _

        with jax.named_scope("gated%d" % b):
            lax.fori_loop(0, chunks, gated_chunk, 0)

    back = copy(bsend, brecv, ids["back"], lax.rem(s + S - 1, S), d)
    send_act(0)
    send_act(1)
    send_cot(1)
    send_act(2)
    send_act(3)
    arrived(w_p, ids["w"])
    with jax.named_scope("proj_p"):
        project(cot, w_p, ga, partner * cpd)
    local_plane(0)
    local_plane(1)
    local_plane(2)
    relay_mirror(0)
    relay_act(0)
    weight_part(0, 0)
    weight_part(0, 1)
    relay_act(1)
    local_plane(3)
    weight_part(1, 0)
    weight_part(1, 1)
    relay_mirror(1)
    reduce_y(0, 0)
    project_mirror()
    send_act(3, own=True)
    reduce_y(0, 1)
    weight_part(0, 2)
    weight_part(1, 2)
    relay_act(2)
    reduce_y(1, 0)
    reduce_z(0, 0)
    relay_act(3)
    reduce_y(1, 1)
    for p in range(P):
        weight_part(2, p)
    reduce_z(0, 1)
    reduce_y(0, 2)
    reduce_y(1, 2)
    for p in range(P):
        weight_part(3, p)
    reduce_z(1, 0)
    gradient(0)

    @pl.when(s > 0)
    def _():
        back.start()

    taps_grad(0)
    reduce_z(1, 1)
    gradient(1)
    taps_grad(1)
    reduce_z(0, 2)
    reduce_z(1, 2)
    gradient(2)
    taps_grad(2)
    reduce_y(2, 0)
    reduce_y(2, 1)
    gradient(3)
    taps_grad(3)
    waits.extend(kg_copy(j) for j in range(1, S))
    reduce_y(2, 2)
    relay_act(3, own=True)
    gated_grad(0)
    gated_grad(1)
    relayed(3, own=True)
    own_part(3, 0, H)
    reduce_y(3, 0)
    gated_grad(2)
    with jax.named_scope("drain"):
        for r in waits + outer:
            r.wait_send()
        waits.clear()
        outer.clear()
    with jax.named_scope("kgwait"):
        for j in range(1, S):
            arrived(krecv.at[j], ids["kg"] + j)
    acc = kg[pl.ds(s * cps, cps)]
    for j in range(1, S):
        acc = acc + krecv[j].astype(f32)
    ksum[...] = acc
    for j in range(1, N):
        send(ksum, k2recv.at[j], ids["k2"] + j, s, lax.rem(d + j, N))
    with jax.named_scope("zwait"):
        for p in range(P):
            arrived(zrecv.at[0, :, part(p)], ids["znear"] + p)
            arrived(zrecv.at[1, :, part(p)], ids["zfar"] + p)

    def final_tile(n, _):
        cols = pl.ds(pl.multiple_of(n * LANES, LANES), LANES)
        acc = wacc[s, :, cols]
        for q in range(2):
            acc = acc + zrecv[q, :, cols].astype(f32)
        acc = acc * factor
        fin[0, :, cols] = acc[:block]
        fin[1, :, cols] = acc[block:]
        return _

    with jax.named_scope("final"):
        lax.fori_loop(0, H // LANES, final_tile, 0)
    send(fin.at[other], fbuf, ids["fin"], s, partner)
    gw[:, half] = fin[c]
    with jax.named_scope("backwait"):
        @pl.when(s < S - 1)
        def _():
            arrived(brecv, ids["back"])

    @pl.when(s == S - 1)
    def _():
        gext[:, pl.ds(T, HB), :] = jnp.zeros((chunks, HB, LANES), f32)

    @pl.when(s < S - 1)
    def _():
        gext[:, pl.ds(T, HB), :] = brecv[...].astype(f32)

    gated_grad(3)
    with jax.named_scope("k2wait"):
        for j in range(1, N):
            arrived(k2recv.at[j], ids["k2"] + j)
            acc = acc + k2recv[j]
    for q in range(cps):
        cols = slice(q * LANES, (q + 1) * LANES)
        kout[:, cols] = acc[q] * factor

    with jax.named_scope("finwait"):
        arrived(fbuf, ids["fin"])
    with jax.named_scope("fincopy"):
        gw[:, ohalf] = fbuf[...]
    with jax.named_scope("endwaits"):
        for r in waits:
            r.wait_send()

        @pl.when(s < S - 1)
        def _():
            front.wait_send()

        @pl.when(s > 0)
        def _():
            back.wait_send()


def number(*sizes):
    ids, count = {}, 0
    for name, size in sizes:
        ids[name] = count
        count += size
    return ids, count


def hand_over(K, gv_in, gg_in, gw_in, k_in, gv, gg, gw, kout, gout, sem):
    pieces = ((gv_in, gv), (gg_in, gg), (gw_in, gw))
    stores = [pltpu.make_async_copy(a, b, sem.at[i]) for i, (a, b) in enumerate(pieces)]
    for st in stores:
        st.start()
    kout[...] = k_in[:K]
    gout[...] = k_in[K : K + 1]
    for st in stores:
        st.wait()


def pair_call(S, N, Y, T, C, K, HB, KP, cot, val, gate, w, kernel, gain):
    X, Z, H = N // 2, S // Y, C // 2
    chunks, cps, cpd, block = C // LANES, C // LANES // S, C // LANES // N, C // (S * N)
    M, CR = chunks // X, C // N
    ids, count = number(
        ("taps", S), ("front", 1), ("back", 1), ("w", 1), ("cot", X * 4), ("cotp", X * 2),
        ("act", X * Z * Y), ("actp", X * Z * Y), ("ga", X * BLOCKS), ("y", (Y - 1) * Z * 3), ("zmid", Z // 2 * 3), ("znear", 3), ("zfar", 3),
        ("fin", 1),
        ("kg", S), ("k2", N),
    )
    vm = pl.BlockSpec(memory_space=pltpu.VMEM)
    hbm = pl.BlockSpec(memory_space=pl.ANY)
    partial = pl.pallas_call(
        functools.partial(pair_kernel, S, N, Y, T, C, K, HB, ids),
        out_shape=(
            jax.ShapeDtypeStruct((T, C), bf16),
            jax.ShapeDtypeStruct((T, C), bf16),
            jax.ShapeDtypeStruct((block, C), f32),
            jax.ShapeDtypeStruct((KP, C // S), f32),
        ),
        in_specs=[hbm] * 6,
        out_specs=(vm,) * 4,
        scratch_shapes=[
            pltpu.VMEM((K, C // S), bf16),
            pltpu.VMEM((C // S,), bf16),
            pltpu.VMEM((cps, KP, LANES), bf16),
            pltpu.VMEM((T, C), bf16),
            pltpu.VMEM((T, C), bf16),
            pltpu.VMEM((T, C), bf16),
            pltpu.VMEM((CR, C), bf16),
            pltpu.VMEM((CR, C), bf16),
            pltpu.VMEM((X - 1, T, C), bf16),
            pltpu.VMEM((X, T, H), bf16),
            pltpu.VMEM((chunks, HB, LANES), bf16),
            pltpu.VMEM((chunks, HB, LANES), bf16),
            pltpu.VMEM((chunks, HB, LANES), bf16),
            pltpu.VMEM((chunks, HB, LANES), bf16),
            pltpu.VMEM((chunks, T + HB, LANES), f32),
            pltpu.VMEM((chunks, T, LANES), f32),
            pltpu.VMEM((chunks, T, LANES), f32),
            pltpu.VMEM((chunks, T + HB, LANES), f32),
            pltpu.VMEM((chunks, KP, LANES), bf16),
            pltpu.VMEM((X, M, LANES, T), bf16),
            pltpu.VMEM((X - 1, M, LANES, T), bf16),
            pltpu.VMEM((X, M, LANES, T), bf16),
            pltpu.VMEM((X - 1, 2 * cpd, T, LANES), bf16),
            pltpu.VMEM((chunks, T, LANES), bf16),
            pltpu.VMEM((M, LANES, H), f32),
            pltpu.VMEM(((Y - 1) * Z, LANES, H), bf16),
            pltpu.VMEM(((Y - 1) * Z, LANES, H), bf16),
            pltpu.VMEM((Z - 1, LANES, H), bf16),
            pltpu.VMEM((Z // 2, LANES, H), bf16),
            pltpu.VMEM((2, LANES, H), bf16),
            pltpu.VMEM((2, block, H), f32),
            pltpu.VMEM((block, H), f32),
            pltpu.VMEM((T, LANES), f32),
            pltpu.VMEM((T, LANES), f32),
            pltpu.VMEM((T, LANES), f32),
            pltpu.VMEM((T, LANES), f32),
            pltpu.VMEM((chunks, K + 1, 8, LANES), f32),
            pltpu.VMEM((chunks, KP, LANES), f32),
            pltpu.VMEM((chunks, KP, LANES), bf16),
            pltpu.VMEM((S, cps, KP, LANES), bf16),
            pltpu.VMEM((cps, KP, LANES), f32),
            pltpu.VMEM((N, cps, KP, LANES), f32),
            pltpu.SemaphoreType.DMA((count,)),
            pltpu.SemaphoreType.DMA((count,)),
            pltpu.SemaphoreType.DMA((6,)),
            pltpu.SemaphoreType.REGULAR((2 * (Z - 2) + 1,)),
        ],
        compiler_params=pltpu.CompilerParams(
            collective_id=0, has_side_effects=True, vmem_limit_bytes=48 * 1024 * 1024
        ),
        name="block_backward",
    )(*(pltpu.with_memory_space_constraint(a, pltpu.HBM) for a in (cot, val, gate, w, kernel, gain)))
    return pl.pallas_call(
        functools.partial(hand_over, K),
        out_shape=(
            jax.ShapeDtypeStruct((T, C), bf16),
            jax.ShapeDtypeStruct((T, C), bf16),
            jax.ShapeDtypeStruct((block, C), f32),
            jax.ShapeDtypeStruct((K, C // S), f32),
            jax.ShapeDtypeStruct((1, C // S), f32),
        ),
        in_specs=[vm] * 4,
        out_specs=(hbm, hbm, hbm, vm, vm),
        scratch_shapes=[
            pltpu.SemaphoreType.DMA((3,)),
        ],
        compiler_params=pltpu.CompilerParams(vmem_limit_bytes=16 * T * LANES),
        name="hand_over",
    )(*partial)


def general_call(S, N, T, C, K, HB, KP, cot, val, gate, w, packed):
    chunks, cps, cpd, block = C // LANES, C // LANES // S, C // LANES // N, C // (S * N)
    ids, count = number(
        ("taps", S), ("front", 1), ("back", 1), ("partner", 1), ("mirror", N // 2 * HALVES),
        ("relay", N // 2 * HALVES), ("act", N), ("ga", N), ("rs", S), ("kg", S), ("k2", N),
    )
    vm = pl.BlockSpec(memory_space=pltpu.VMEM)
    return pl.pallas_call(
        functools.partial(general_kernel, S, N, T, C, K, HB, ids),
        out_shape=(
            jax.ShapeDtypeStruct((T, C), bf16),
            jax.ShapeDtypeStruct((T, C), bf16),
            jax.ShapeDtypeStruct((block, C), f32),
            jax.ShapeDtypeStruct((K, C // S), f32),
            jax.ShapeDtypeStruct((1, C // S), f32),
        ),
        in_specs=[vm] * 5,
        out_specs=(vm,) * 5,
        scratch_shapes=[
            pltpu.VMEM((N, T, C), bf16),
            pltpu.VMEM((chunks, T + HB, LANES), f32),
            pltpu.VMEM((chunks, T, LANES), f32),
            pltpu.VMEM((chunks, T, LANES), f32),
            pltpu.VMEM((chunks, T + HB, LANES), f32),
            pltpu.VMEM((chunks, KP, LANES), bf16),
            pltpu.VMEM((chunks, T, LANES), bf16),
            pltpu.VMEM((N, cpd, T, LANES), bf16),
            pltpu.VMEM((N, cpd, T, LANES), bf16),
            pltpu.VMEM((chunks, T, LANES), bf16),
            pltpu.VMEM((cpd * LANES, C), bf16),
            pltpu.VMEM((S, block, C), bf16),
            pltpu.VMEM((chunks, KP, LANES), f32),
            pltpu.VMEM((S, cps, KP, LANES), f32),
            pltpu.VMEM((cps, KP, LANES), f32),
            pltpu.VMEM((N, cps, KP, LANES), f32),
            pltpu.SemaphoreType.DMA((count,)),
            pltpu.SemaphoreType.DMA((count,)),
        ],
        compiler_params=pltpu.CompilerParams(
            collective_id=0, has_side_effects=True, vmem_limit_bytes=60 * 1024 * 1024
        ),
        name="block_backward",
    )(cot, val, gate, w, packed)


def shards(out_cotangent, value_pre, gate_pre, out_weight, conv_kernel, norm_gain):
    S, N = lax.axis_size("sp"), lax.axis_size("dp")
    _, T, C = out_cotangent.shape
    K = conv_kernel.shape[0]
    chunks, cps = C // LANES, C // LANES // S
    HB = -(-(K - 1) // 16) * 16
    KP = -(-(K + 1) // 16) * 16
    args = (out_cotangent[0], value_pre[0], gate_pre[0], out_weight)
    X = N // 2
    if N == 2 * X > 2 and S == 2 * 2 * X and chunks == S * X:
        outs = pair_call(S, N, X, T, C, K, HB, KP, *args, conv_kernel, norm_gain)
    else:
        packed = jnp.concatenate(
            [conv_kernel, norm_gain[None], jnp.zeros((KP - K - 1, C // S), bf16)], axis=0
        )
        packed = jnp.transpose(packed.reshape(KP, cps, LANES), (1, 0, 2))
        outs = general_call(S, N, T, C, K, HB, KP, *args, packed)
    grad_value, grad_gate, grad_weight, grad_taps, grad_gain = outs
    return grad_value[None], grad_gate[None], grad_weight, grad_taps, grad_gain[0]


def solution(mesh):
    placed = (
        P("dp", "sp", None),
        P("dp", "sp", None),
        P("dp", "sp", None),
        P("dp", None),
        P(None, "sp"),
        P("sp"),
    )
    return jax.shard_map(
        shards,
        mesh=mesh,
        in_specs=placed,
        out_specs=(
            P("dp", "sp", None),
            P("dp", "sp", None),
            P(("sp", "dp"), None),
            P(None, "sp"),
            P("sp"),
        ),
        check_vma=False,
    )
```

```python
import functools

import jax
import jax.numpy as jnp
from jax import lax
from jax.experimental import pallas as pl
from jax.experimental.pallas import tpu as pltpu
from jax.sharding import PartitionSpec as P

epsilon = 1e-05
LANES = 128
HALVES = 2
BLOCKS = 4
f32 = jnp.float32
bf16 = jnp.bfloat16


def general_kernel(
    S, N, T, C, K, HB, ids,
    cot, val, gate, w, taps,
    gv, gg, gw, kout, gout,
    cot_all, ext, cen, gc, gext, kall, act, act_all, ga_send, ga, wpart, rbuf,
    kg, krecv, ksum, k2recv, send_sem, recv_sem,
):
    s = lax.axis_index("sp")
    d = lax.axis_index("dp")
    chunks = C // LANES
    cps = chunks // S
    cpd = chunks // N
    block = C // (S * N)
    RB = min(T, 128)
    total = S * N
    me = s * N + d
    partner = d + 1 - 2 * lax.rem(d, 2)
    factor = float(S * N * T) ** (-0.5)
    hrows = T // HALVES
    waits = []

    def copy(src, dst, i, to_s, to_d):
        return pltpu.make_async_remote_copy(
            src_ref=src, dst_ref=dst, send_sem=send_sem.at[i], recv_sem=recv_sem.at[i],
            device_id={"sp": to_s, "dp": to_d}, device_id_type=pl.DeviceIdType.MESH,
        )

    def send(src, dst, i, to_s, to_d):
        c = copy(src, dst, i, to_s, to_d)
        c.start()
        waits.append(c)

    def arrived(dst, i):
        copy(dst, dst, i, s, partner).wait_recv()

    barrier = pltpu.get_barrier_semaphore()

    def greet(j, _):
        other = lax.rem(me + j, total)
        pl.semaphore_signal(
            barrier, inc=1, device_id={"sp": other // N, "dp": lax.rem(other, N)},
            device_id_type=pl.DeviceIdType.MESH,
        )
        return _

    lax.fori_loop(1, total, greet, 0)
    def gate_chunk(cb, _):
        cols = pl.ds(pl.multiple_of(cb * LANES, LANES), LANES)
        sig = jax.nn.sigmoid(gate[:, cols].astype(f32))
        ext[cb, pl.ds(HB, T), :] = (val[:, cols].astype(f32) * sig).astype(bf16).astype(f32)
        return _

    lax.fori_loop(0, chunks, gate_chunk, 0)
    pl.semaphore_wait(barrier, total - 1)

    for j in range(1, S):
        send(taps, kall.at[pl.ds(s * cps, cps)], ids["taps"] + j, lax.rem(s + j, S), d)
    following = lax.rem(s + 1, S)
    preceding = lax.rem(s + S - 1, S)
    send(ext.at[:, pl.ds(T, HB), :], ext.at[:, pl.ds(0, HB), :], ids["front"], following, d)
    for j in range(1, N // 2):
        for h in range(HALVES):
            rows = pl.ds(h * hrows, hrows)
            send(cot.at[rows], cot_all.at[d, rows], ids["mirror"] + j * HALVES + h, s, lax.rem(d + 2 * j, N))
    send(cot, cot_all.at[d], ids["partner"], s, partner)
    kall[pl.ds(s * cps, cps)] = taps[...]
    cot_all[d] = cot[...]
    for j in range(1, S):
        arrived(kall.at[pl.ds(lax.rem(s + S - j, S) * cps, cps)], ids["taps"] + j)
    arrived(ext.at[:, pl.ds(0, HB), :], ids["front"])

    @pl.when(s == 0)
    def _():
        ext[:, pl.ds(0, HB), :] = jnp.zeros((chunks, HB, LANES), f32)

    def conv_chunk(cb, sums):
        tf = kall[cb].astype(f32)
        parts = []
        for rb in range(T // RB):
            acc = jnp.zeros((RB, LANES), f32)
            for k in range(K):
                acc = acc + tf[k : k + 1] * ext[cb, pl.ds(HB - k + rb * RB, RB), :]
            cen[cb, pl.ds(rb * RB, RB), :] = acc
            parts.append(jnp.sum(acc, axis=1, keepdims=True))
        return sums + jnp.concatenate(parts, axis=0)

    column = jnp.zeros((T, 1), f32)
    mean = lax.fori_loop(0, chunks, conv_chunk, column) / C

    def square_chunk(cb, sums):
        dev = cen[cb] - mean
        return sums + dev * dev

    squares = lax.fori_loop(0, chunks, square_chunk, jnp.zeros((T, LANES), f32))
    inv = lax.rsqrt(jnp.sum(squares, axis=1, keepdims=True) / C + epsilon)

    def relay():
        for j in range(1, N // 2):
            origin = lax.rem(d + N - 2 * j, N)
            for h in range(HALVES):
                piece = cot_all.at[origin, pl.ds(h * hrows, hrows)]
                arrived(piece, ids["mirror"] + j * HALVES + h)
                send(piece, piece, ids["relay"] + j * HALVES + h, s, partner)

    def act_chunk(cb, _):
        centred = (cen[cb] - mean) * inv
        cen[cb] = centred
        normed = centred * kall[cb].astype(f32)[K : K + 1]
        act[cb] = (normed * jax.nn.sigmoid(normed)).astype(bf16)
        return _

    lax.fori_loop(0, chunks, act_chunk, 0)
    for j in range(1, N):
        to = lax.rem(d + j, N)
        send(act.at[pl.ds(to * cpd, cpd)], act_all.at[d], ids["act"] + j, s, to)
    act_all[d] = act[pl.ds(d * cpd, cpd)]

    def project(source, slot):
        def pair(m, _):
            rows = pl.ds(pl.multiple_of(m * 2 * LANES, 2 * LANES), 2 * LANES)
            out = lax.dot_general(
                cot_all[source], w[rows, :], (((1,), (1,)), ((), ())), preferred_element_type=f32
            ).astype(bf16)
            ga_send[slot, 2 * m] = out[:, :LANES]
            ga_send[slot, 2 * m + 1] = out[:, LANES:]
            return _

        lax.fori_loop(0, cpd // 2, pair, 0)

    mine = pl.ds(d * cpd, cpd)
    project(d, 0)
    ga[mine] = ga_send[0]
    arrived(cot_all.at[partner], ids["partner"])
    project(partner, 1)
    send(ga_send.at[1], ga.at[mine], ids["ga"] + 1, s, partner)
    relay()
    for j in range(1, N // 2):
        origin = lax.rem(d + N - 2 * j, N)
        project(origin, 2 * j)
        send(ga_send.at[2 * j], ga.at[mine], ids["ga"] + 2 * j, s, origin)
    for j in range(1, N // 2):
        origin = lax.rem(partner + N - 2 * j, N)
        for h in range(HALVES):
            arrived(cot_all.at[origin, pl.ds(h * hrows, hrows)], ids["relay"] + j * HALVES + h)
        project(origin, 2 * j + 1)
        send(ga_send.at[2 * j + 1], ga.at[mine], ids["ga"] + 2 * j + 1, s, origin)

    for j in range(1, N):
        arrived(act_all.at[lax.rem(d + N - j, N)], ids["act"] + j)
    NT = min(C, 512)

    def weight_tile(i, _):
        m, n = i // (C // NT), lax.rem(i, C // NT)
        cols = pl.ds(pl.multiple_of(n * NT, NT), NT)
        acc = jnp.zeros((LANES, NT), f32)
        for q in range(N):
            acc = acc + lax.dot_general(
                act_all[q, m], cot_all[q, :, cols], (((0,), (0,)), ((), ())),
                preferred_element_type=f32,
            )
        wpart[pl.ds(pl.multiple_of(m * LANES, LANES), LANES), cols] = acc.astype(bf16)
        return _

    lax.fori_loop(0, cpd * (C // NT), weight_tile, 0)

    def block_of(j):
        i = lax.rem(s + j, S)
        owner = d * S + i
        rows = pl.ds(pl.multiple_of(i * block, block), block)
        return owner, rows, pltpu.make_async_remote_copy(
            src_ref=wpart.at[rows], dst_ref=rbuf.at[s], send_sem=send_sem.at[ids["rs"] + j],
            recv_sem=recv_sem.at[ids["rs"] + s],
            device_id={"sp": owner // N, "dp": lax.rem(owner, N)},
            device_id_type=pl.DeviceIdType.MESH,
        )

    def send_blocks(first, last):
        for j in range(first, last):
            owner, rows, c = block_of(j)

            @pl.when(owner != me)
            def _():
                c.start()

            @pl.when(owner == me)
            def _():
                rbuf[s] = wpart[rows, :]

    send_blocks(0, S // 2)

    for j in range(1, N // 2):
        arrived(ga.at[pl.ds(lax.rem(d + 2 * j, N) * cpd, cpd)], ids["ga"] + 2 * j)
        arrived(ga.at[pl.ds(lax.rem(partner + 2 * j, N) * cpd, cpd)], ids["ga"] + 2 * j + 1)
    arrived(ga.at[pl.ds(partner * cpd, cpd)], ids["ga"] + 1)

    def grad_chunk(cb, sums):
        one, two = sums
        centred = cen[cb]
        gain = kall[cb].astype(f32)[K : K + 1]
        normed = centred * gain
        sg = jax.nn.sigmoid(normed)
        grad = ga[cb].astype(f32) * sg * (1.0 + normed * (1.0 - sg))
        kg[cb, pl.ds(K, 1), :] = jnp.sum(grad * centred, axis=0, keepdims=True)
        grad = grad * gain
        gc[cb] = grad
        return one + grad, two + grad * centred

    zero = jnp.zeros((T, LANES), f32)
    one, two = lax.fori_loop(0, chunks, grad_chunk, (zero, zero))
    first = jnp.sum(one, axis=1, keepdims=True) / C
    second = jnp.sum(two, axis=1, keepdims=True) / C

    def conv_grad(cb, _):
        gext[cb, pl.ds(0, T), :] = (gc[cb] - first - cen[cb] * second) * inv
        return _

    lax.fori_loop(0, chunks, conv_grad, 0)
    send(gext.at[:, pl.ds(0, HB), :], gext.at[:, pl.ds(T, HB), :], ids["back"], preceding, d)

    def taps_chunk(cb, _):
        for k in range(K):
            acc = jnp.zeros((8, LANES), f32)
            for rb in range(T // RB):
                prod = gext[cb, pl.ds(rb * RB, RB), :] * ext[cb, pl.ds(HB - k + rb * RB, RB), :]
                acc = acc + jnp.sum(prod.reshape(RB // 8, 8, LANES), axis=0)
            kg[cb, pl.ds(k, 1), :] = jnp.sum(acc, axis=0, keepdims=True)
        return _

    lax.fori_loop(0, chunks, taps_chunk, 0)
    for j in range(1, S):
        to = lax.rem(s + j, S)
        send(kg.at[pl.ds(to * cps, cps)], krecv.at[j], ids["kg"] + j, to, d)
    send_blocks(S // 2, S)

    arrived(gext.at[:, pl.ds(T, HB), :], ids["back"])

    @pl.when(s == S - 1)
    def _():
        gext[:, pl.ds(T, HB), :] = jnp.zeros((chunks, HB, LANES), f32)

    def gated_chunk(cb, _):
        cols = pl.ds(pl.multiple_of(cb * LANES, LANES), LANES)
        tf = kall[cb].astype(f32)
        for rb in range(T // RB):
            rows = pl.ds(rb * RB, RB)
            acc = jnp.zeros((RB, LANES), f32)
            for k in range(K):
                acc = acc + tf[k : k + 1] * gext[cb, pl.ds(k + rb * RB, RB), :]
            acc = acc.astype(bf16).astype(f32)
            sig = jax.nn.sigmoid(gate[rows, cols].astype(f32))
            gv[rows, cols] = (acc * sig).astype(bf16)
            gg[rows, cols] = (acc * val[rows, cols].astype(f32) * sig * (1.0 - sig)).astype(bf16)
        return _

    lax.fori_loop(0, chunks, gated_chunk, 0)

    acc = kg[pl.ds(s * cps, cps)]
    for j in range(1, S):
        arrived(krecv.at[j], ids["kg"] + j)
        acc = acc + krecv[j]
    ksum[...] = acc
    for j in range(1, N):
        send(ksum, k2recv.at[j], ids["k2"] + j, s, lax.rem(d + j, N))
    for j in range(1, N):
        arrived(k2recv.at[j], ids["k2"] + j)
        acc = acc + k2recv[j]
    for c in range(cps):
        cols = slice(c * LANES, (c + 1) * LANES)
        kout[:, cols] = (acc[c] * factor)[:K]
        gout[:, cols] = (acc[c] * factor)[K : K + 1]

    home = me // S
    for q in range(S):
        @pl.when(jnp.logical_or(q != s, home != d))
        def _():
            arrived(rbuf.at[q], ids["rs"] + q)

    def sum_tile(n, _):
        cols = pl.ds(pl.multiple_of(n * LANES, LANES), LANES)
        acc = rbuf[0, :, cols].astype(f32)
        for q in range(1, S):
            acc = acc + rbuf[q, :, cols].astype(f32)
        gw[:, cols] = acc * factor
        return _

    lax.fori_loop(0, chunks, sum_tile, 0)
    for j in range(S):
        owner, rows, c = block_of(j)

        @pl.when(owner != me)
        def _():
            c.wait_send()

    for c in waits:
        c.wait_send()


def pair_kernel(
    S, N, Y, T, C, K, HB, ids,
    cot_in, val_in, gate_in, w_in, kernel_in, gain_in,
    gv, gg, gw, kout, gout,
    kernel, gain, taps, cot, val, gate, w, w_p, cot_m, cot_p, fsend, frecv, bsend, brecv, ext, cen, gc, gext, kall,
    act, act_m, act_p, ga_s, ga, wacc, wpart, yrecv, ysum, zmid, zrecv, fin, fbuf,
    means, invs, sum1, sum2, kacc, kg, kgb, krecv, ksum, k2recv, send_sem, recv_sem, load_sem, ready,
):
    s = lax.axis_index("sp")
    d = lax.axis_index("dp")
    X, Z, H = N // 2, S // Y, C // 2
    x, c = d // 2, lax.rem(d, 2)
    y, z = lax.rem(s, Y), s // Y
    other = 1 - c
    partner = d + 1 - 2 * c
    chunks = C // LANES
    cps = chunks // S
    cpd = chunks // N
    block = C // (S * N)
    M = chunks // X
    RB = min(T, 128)
    TB = T // BLOCKS
    factor = float(S * N * T) ** (-0.5)
    waits = []

    def copy(src, dst, i, to_s, to_d, j=None):
        return pltpu.make_async_remote_copy(
            src_ref=src, dst_ref=dst, send_sem=send_sem.at[i],
            recv_sem=recv_sem.at[i if j is None else j],
            device_id={"sp": to_s, "dp": to_d}, device_id_type=pl.DeviceIdType.MESH,
        )

    def send(src, dst, i, to_s, to_d, j=None):
        r = copy(src, dst, i, to_s, to_d, j)
        r.start()
        waits.append(r)

    def arrived(dst, i):
        copy(dst, dst, i, s, partner).wait_recv()

    loads = [
        pltpu.make_async_copy(a, b, load_sem.at[i])
        for i, (a, b) in enumerate((
            (gate_in, gate), (val_in, val), (cot_in, cot), (w_in, w), (kernel_in, kernel), (gain_in, gain),
        ))
    ]
    for l in loads:
        l.start()

    barrier = pltpu.get_barrier_semaphore()

    def signal(sem, to_s, to_d):
        pl.semaphore_signal(
            sem, inc=1, device_id={"sp": to_s, "dp": to_d}, device_id_type=pl.DeviceIdType.MESH
        )

    def along_z(action):
        @pl.when(z > 0)
        def _():
            action(0, s - Y)

        @pl.when(z < Z - 1)
        def _():
            action(1, s + Y)

    signal(barrier, s, partner)
    for j in range(1, X):
        signal(barrier, s, lax.rem(d + 2 * j, N))
    for j in range(1, Y):
        signal(barrier, z * Y + lax.rem(y + j, Y), d)
    along_z(lambda side, to_s: signal(barrier, to_s, d))
    loads[2].wait()
    with jax.named_scope("barrierwait"):
        pl.semaphore_wait(barrier, X + Y - 1 + jnp.where(z > 0, 1, 0) + jnp.where(z < Z - 1, 1, 0))

    def pass_on(r):
        along_z(lambda side, to_s: signal(ready.at[2 * r + 1 - side], to_s, d))

    def passed(r):
        along_z(lambda side, to_s: pl.semaphore_wait(ready.at[2 * r + side], 1))

    pass_on(0)
    strips = ((0, H - H // BLOCKS), (H - H // BLOCKS, H // BLOCKS))
    parts = ((0, H // 2), (H // 2, H // BLOCKS), (H - H // BLOCKS, H // BLOCKS))
    P = len(parts)

    def strip(side, p):
        return pl.ds(pl.multiple_of(side * H + strips[p][0], LANES), strips[p][1])

    def part(p):
        return pl.ds(parts[p][0], parts[p][1])

    def send_cot(p):
        for j in range(1, X):
            for side in range(2):
                send(
                    cot.at[:, strip(side, p)], cot_m.at[j - 1, :, strip(side, p)],
                    ids["cot"] + ((j - 1) * 2 + p) * 2 + side, s, lax.rem(d + 2 * j, N),
                )

    send_cot(0)
    loads[0].wait()
    loads[1].wait()

    def gate_chunk(cb, _):
        cols = pl.ds(pl.multiple_of(cb * LANES, LANES), LANES)
        sig = jax.nn.sigmoid(gate[:, cols].astype(f32))
        gated = (val[:, cols].astype(f32) * sig).astype(bf16)
        ext[cb, pl.ds(HB, T), :] = gated.astype(f32)
        fsend[cb] = gated[T - HB :]
        return _

    with jax.named_scope("gate"):
        lax.fori_loop(0, chunks, gate_chunk, 0)
    loads[4].wait()
    loads[5].wait()
    KP = taps.shape[1]
    for q in range(cps):
        cols = slice(q * LANES, (q + 1) * LANES)
        taps[q] = jnp.concatenate(
            [kernel[:, cols].astype(f32), gain[cols].astype(f32).reshape(1, LANES)]
            + [jnp.zeros((KP - K - 1, LANES), f32)] * (KP > K + 1),
            axis=0,
        ).astype(bf16)
    half = pl.ds(pl.multiple_of(c * H, LANES), H)
    ohalf = pl.ds(pl.multiple_of(other * H, LANES), H)
    loads[3].wait()
    send(w, w_p, ids["w"], s, partner)
    send(cot.at[:, ohalf], cot_p.at[0], ids["cotp"], s, partner)
    kall[pl.ds(s * cps, cps)] = taps[...]
    with jax.named_scope("ready"):
        for r in range(Z - 2):
            if r > 0:
                pass_on(r)
            passed(r)
        for j in range(1, Y):
            signal(ready.at[2 * (Z - 2)], z * Y + lax.rem(y + j, Y), d)
        pl.semaphore_wait(ready.at[2 * (Z - 2)], Y - 1)
    for j in range(1, S):
        copy(taps, kall.at[pl.ds(s * cps, cps)], ids["taps"], lax.rem(s + j, S), d).start()
    all_taps = kall.at[pl.ds(0, chunks - cps)]
    waits.append(copy(all_taps, all_taps, ids["taps"], s, partner))
    front = copy(fsend, frecv, ids["front"], lax.rem(s + 1, S), d)

    @pl.when(s < S - 1)
    def _():
        front.start()


    def project(rows_of, weights, out, base):
        def pair(m, _):
            rows = pl.ds(pl.multiple_of(m * 2 * LANES, 2 * LANES), 2 * LANES)
            prod = lax.dot_general(
                rows_of[...], weights[rows, :], (((1,), (1,)), ((), ())), preferred_element_type=f32
            ).astype(bf16)
            out[base + 2 * m] = prod[:, :LANES]
            out[base + 2 * m + 1] = prod[:, LANES:]
            return _

        lax.fori_loop(0, cpd // 2, pair, 0)

    with jax.named_scope("proj_own"):
        project(cot, w, ga, d * cpd)
    with jax.named_scope("tapswait"):
        arrived(all_taps, ids["taps"])

        @pl.when(s > 0)
        def _():
            arrived(frecv, ids["front"])

    @pl.when(s == 0)
    def _():
        ext[:, pl.ds(0, HB), :] = jnp.zeros((chunks, HB, LANES), f32)

    @pl.when(s > 0)
    def _():
        ext[:, pl.ds(0, HB), :] = frecv[...].astype(f32)

    def convolve(cb, rb):
        tf = kall[cb].astype(f32)
        acc = jnp.zeros((RB, LANES), f32)
        for k in range(K):
            acc = acc + tf[k : k + 1] * ext[cb, pl.ds(HB - k + rb * RB, RB), :]
        cen[cb, pl.ds(rb * RB, RB), :] = acc
        return acc

    def conv_chunk(cb, _):
        for rb in range(T // RB):
            rows = pl.ds(rb * RB, RB)
            dev = convolve(cb, rb) - means[rows, :]
            sum1[rows, :] = sum1[rows, :] + dev
            sum2[rows, :] = sum2[rows, :] + dev * dev
        return _

    with jax.named_scope("conv"):
        for rb in range(T // RB):
            rows = pl.ds(rb * RB, RB)
            acc = convolve(0, rb)
            start = jnp.broadcast_to(jnp.sum(acc, axis=1, keepdims=True) / LANES, (RB, LANES))
            means[rows, :] = start
            sum1[rows, :] = acc - start
            sum2[rows, :] = (acc - start) * (acc - start)
        lax.fori_loop(1, chunks, conv_chunk, 0)
    with jax.named_scope("moments"):
        shift = jnp.sum(sum1[...], axis=1, keepdims=True) / C
        variance = jnp.sum(sum2[...], axis=1, keepdims=True) / C - shift * shift
        means[...] = means[...] + shift
        invs[...] = jnp.broadcast_to(lax.rsqrt(variance + epsilon), (T, LANES))

    def act_chunk(cb, _):
        centred = (cen[cb] - means[...]) * invs[...]
        cen[cb] = centred
        normed = centred * kall[cb].astype(f32)[K : K + 1]
        act[lax.rem(cb, X), cb // X] = (normed * jax.nn.sigmoid(normed)).T.astype(bf16)
        return _

    with jax.named_scope("act"):
        lax.fori_loop(0, chunks, act_chunk, 0)
    send(act.at[x], act_p.at[0], ids["actp"], s, partner)

    near = Z // 2
    low = z < near
    inner_z = jnp.where(low, near - 1, near)
    inner = z == inner_z

    def plane(k):
        if k < near:
            return jnp.where(low, Z - 1 - k, k)
        return jnp.where(low, 0, near) + lax.rem(z + 1 + k, near)

    def planes(k, own):
        if k < Z - 1:
            return [(plane(k) * Y, Y, 0)]
        return [(plane(k) * Y + lax.rem(y + j, Y), 1, j) for j in (range(1) if own else range(1, Y))]

    def send_act(k, own=False):
        for first, size, n in planes(k, own):
            piece = pl.ds(first, size)
            for j in range(1, X):
                send(
                    act.at[lax.rem(x + j, X), piece], act_m.at[j - 1, piece],
                    ids["act"] + (j - 1) * (Z - 1 + Y) + k + n, s, lax.rem(d + 2 * j, N),
                )

    def relay_mirror(p):
        with jax.named_scope("cotwait%d" % p):
            for j in range(1, X):
                for side in range(2):
                    arrived(cot_m.at[j - 1, :, strip(side, p)], ids["cot"] + ((j - 1) * 2 + p) * 2 + side)
                send(
                    cot_m.at[j - 1, :, strip(other, p)], cot_p.at[j, :, strip(0, p)],
                    ids["cotm"] + (j - 1) * 2 + p, s, partner,
                )

    def project_mirror():
        for j in range(1, X):
            with jax.named_scope("proj_m"):
                project(cot_m.at[j - 1], w, ga_s.at[j - 1], c * cpd)
                project(cot_m.at[j - 1], w_p, ga_s.at[j - 1], other * cpd)
            for b in range(BLOCKS):
                rows = pl.ds(b * TB, TB)
                send(
                    ga_s.at[j - 1, :, rows], ga.at[pl.ds(x * 2 * cpd, 2 * cpd), rows],
                    ids["ga"] + (j - 1) * BLOCKS + b, s, lax.rem(d + 2 * (X - j), N),
                )

    dims = (((1,), (0,)), ((), ()))

    def dot(a, b):
        return lax.dot_general(a, b, dims, preferred_element_type=f32)

    LT = H // 2

    def local_plane(k):
        def tile(i, _):
            m, n = plane(k) * Y + i // 2, lax.rem(i, 2)
            cols = pl.ds(pl.multiple_of(n * LT, LT), LT)
            own = pl.ds(pl.multiple_of(c * H + n * LT, LT), LT)
            wacc[m, :, cols] = dot(act[x, m], cot[:, own]) + dot(act_p[0, m], cot_p[0, :, cols])
            return _

        with jax.named_scope("wlocal%d" % k):
            if k == 0:
                arrived(cot_p.at[0], ids["cotp"])
                arrived(act_p.at[0], ids["actp"])
            lax.fori_loop(0, Y * 2, tile, 0)

    NT = H // BLOCKS

    def remote_part(m, n):
        cols = pl.ds(pl.multiple_of(n * NT, NT), NT)
        own = pl.ds(pl.multiple_of(c * H + n * NT, NT), NT)
        acc = wacc[m, :, cols]
        for j in range(1, X):
            acc = acc + dot(act_m[j - 1, m], cot_m[j - 1, :, own]) + dot(act_p[j, m], cot_p[j, :, cols])
        return cols, acc

    def relay_act(k, own=False):
        with jax.named_scope("actwait%d" % k):
            for first, size, n in planes(k, own):
                piece = pl.ds(first, size)
                for j in range(1, X):
                    i = (j - 1) * (Z - 1 + Y) + k + n
                    arrived(act_m.at[j - 1, piece], ids["act"] + i)
                    send(act_m.at[j - 1, piece], act_p.at[j, piece], ids["actm"] + i, s, partner)

    def relayed(k, own=False):
        with jax.named_scope("relaywait%d" % k):
            for first, size, n in planes(k, own):
                for j in range(1, X):
                    arrived(act_p.at[j, pl.ds(first, size)], ids["actm"] + (j - 1) * (Z - 1 + Y) + k + n)

    def own_part(k, off, size):
        def own_tile(n, _):
            m = plane(k) * Y + y
            cols, acc = remote_part(m, n)
            wacc[m, :, cols] = acc
            return _

        lax.fori_loop(off // NT, (off + size) // NT, own_tile, 0)

    def weight_part(k, p):
        off, size = parts[p]
        if p == 0:
            relayed(k)
        if k == 0 and p != 1:
            q = 0 if p == 0 else 1
            for j in range(1, X):
                arrived(cot_p.at[j, :, strip(0, q)], ids["cotm"] + (j - 1) * 2 + q)
        with jax.named_scope("wremote%d%d" % (k, p)):
            for j in range(1, Y):
                to_y = lax.rem(y + j, Y)
                i = (j - 1) * Z + k

                def send_tile(n, _):
                    cols, acc = remote_part(plane(k) * Y + to_y, n)
                    wpart[i, :, cols] = acc.astype(bf16)
                    return _

                lax.fori_loop(off // NT, (off + size) // NT, send_tile, 0)
                send(
                    wpart.at[i, :, part(p)], yrecv.at[i, :, part(p)],
                    ids["y"] + i * P + p, z * Y + to_y, d,
                )

            if k < Z - 1:
                own_part(k, off, size)

    def reduce_y(k, p):
        for q in (p,) if k < Z - 1 else range(P):
            with jax.named_scope("ywait%d%d" % (k, q)):
                for j in range(1, Y):
                    i = (j - 1) * Z + k
                    arrived(yrecv.at[i, :, part(q)], ids["y"] + i * P + q)
        to_z = plane(k)
        m = to_z * Y + y

        def tile(n, _):
            cols = pl.ds(pl.multiple_of(n * LANES, LANES), LANES)
            acc = wacc[m, :, cols]
            for j in range(1, Y):
                acc = acc + yrecv[(j - 1) * Z + k, :, cols].astype(f32)
            if k < Z - 1:
                ysum[k, :, cols] = acc.astype(bf16)
            if k != Z - 2:
                wacc[m, :, cols] = acc
            return _

        off, size = parts[p] if k < Z - 1 else (0, H)
        lax.fori_loop(off // LANES, (off + size) // LANES, tile, 0)
        if k < near:
            r = copy(
                ysum.at[k, :, part(p)], zmid.at[k, :, part(p)], ids["zmid"] + k * P + p,
                inner_z * Y + y, d,
            )

            @pl.when(jnp.logical_not(inner))
            def _():
                r.start()

            outer.append(r)
        elif k < Z - 1:
            send(
                ysum.at[k, :, part(p)], zrecv.at[0, :, part(p)], ids["znear"] + p,
                to_z * Y + y, d,
            )

    def reduce_z(k, p):
        to_z = plane(k)
        m = to_z * Y + y
        off, size = parts[p]

        def tile(n, _):
            cols = pl.ds(pl.multiple_of(n * LANES, LANES), LANES)
            ysum[k, :, cols] = (wacc[m, :, cols] + zmid[k, :, cols].astype(f32)).astype(bf16)
            return _

        @pl.when(inner)
        def _():
            with jax.named_scope("zmid%d%d" % (k, p)):
                arrived(zmid.at[k, :, part(p)], ids["zmid"] + k * P + p)
            lax.fori_loop(off // LANES, (off + size) // LANES, tile, 0)
            copy(
                ysum.at[k, :, part(p)], zrecv.at[1, :, part(p)], ids["zmid"] + k * P + p,
                to_z * Y + y, d, ids["zfar"] + p,
            ).start()

    outer = []

    def fold(v):
        return jnp.sum(v.reshape(v.shape[0] // 8, 8, LANES), axis=0)

    def gradient(b):
        rows = pl.ds(b * TB, TB)
        with jax.named_scope("gawait%d" % b):
            for j in range(1, X):
                origin = lax.rem(x + j, X)
                arrived(ga.at[pl.ds(origin * 2 * cpd, 2 * cpd), rows], ids["ga"] + (X - j - 1) * BLOCKS + b)

        def grad_chunk(cb, sums):
            one, two = sums
            centred = cen[cb, rows, :]
            gain = kall[cb].astype(f32)[K : K + 1]
            normed = centred * gain
            sg = jax.nn.sigmoid(normed)
            grad = ga[cb, rows, :].astype(f32) * sg * (1.0 + normed * (1.0 - sg))
            scaled = grad * centred
            kacc[cb, K] = fold(scaled) if b == 0 else kacc[cb, K] + fold(scaled)
            gc[cb, rows, :] = grad * gain
            return one + grad * gain, two + scaled * gain

        zero = jnp.zeros((TB, LANES), f32)
        with jax.named_scope("gradchunk%d" % b):
            one, two = lax.fori_loop(0, chunks, grad_chunk, (zero, zero))
        first = jnp.sum(one, axis=1, keepdims=True) / C
        second = jnp.sum(two, axis=1, keepdims=True) / C
        scale = invs[rows, :]

        def conv_grad(cb, _):
            grad = (gc[cb, rows, :] - first - cen[cb, rows, :] * second) * scale
            gext[cb, rows, :] = grad
            if b == 0:
                bsend[cb] = grad[:HB].astype(bf16)
            return _

        with jax.named_scope("convgrad%d" % b):
            lax.fori_loop(0, chunks, conv_grad, 0)

    def kg_copy(off):
        to = lax.rem(s + off, S)
        return copy(kgb.at[pl.ds(to * cps, cps)], krecv.at[off], ids["kg"], to, d)

    def taps_grad(b):
        def taps_chunk(cb, _):
            grad = gext[cb, pl.ds(b * TB, TB), :]
            for k in range(K):
                acc = fold(grad * ext[cb, pl.ds(HB - k + b * TB, TB), :])
                if b > 0:
                    acc = acc + kacc[cb, k]
                if b < BLOCKS - 1:
                    kacc[cb, k] = acc
                else:
                    kg[cb, pl.ds(k, 1), :] = jnp.sum(acc, axis=0, keepdims=True)
            if b == BLOCKS - 1:
                kg[cb, pl.ds(K, 1), :] = jnp.sum(kacc[cb, K], axis=0, keepdims=True)
                kgb[cb] = kg[cb].astype(bf16)
            return _

        def taps_owner(n, _):
            off = 1 + lax.rem(n + S // 2 - 1, S - 1)
            to = lax.rem(s + off, S)
            lax.fori_loop(to * cps, to * cps + cps, taps_chunk, 0)
            kg_copy(off).start()
            return _

        with jax.named_scope("taps%d" % b):
            if b < BLOCKS - 1:
                lax.fori_loop(0, chunks, taps_chunk, 0)
            else:
                lax.fori_loop(0, S - 1, taps_owner, 0)
                lax.fori_loop(s * cps, s * cps + cps, taps_chunk, 0)

    def gated_grad(b):
        rows = pl.ds(b * TB, TB)

        def gated_chunk(cb, _):
            cols = pl.ds(pl.multiple_of(cb * LANES, LANES), LANES)
            tf = kall[cb].astype(f32)
            acc = jnp.zeros((TB, LANES), f32)
            for k in range(K):
                acc = acc + tf[k : k + 1] * gext[cb, pl.ds(k + b * TB, TB), :]
            acc = acc.astype(bf16).astype(f32)
            sig = jax.nn.sigmoid(gate[rows, cols].astype(f32))
            gv[rows, cols] = (acc * sig).astype(bf16)
            gg[rows, cols] = (acc * val[rows, cols].astype(f32) * sig * (1.0 - sig)).astype(bf16)
            return _

        with jax.named_scope("gated%d" % b):
            lax.fori_loop(0, chunks, gated_chunk, 0)

    back = copy(bsend, brecv, ids["back"], lax.rem(s + S - 1, S), d)
    send_act(0)
    send_act(1)
    send_cot(1)
    send_act(2)
    send_act(3)
    arrived(w_p, ids["w"])
    with jax.named_scope("proj_p"):
        project(cot, w_p, ga, partner * cpd)
    local_plane(0)
    local_plane(1)
    local_plane(2)
    relay_mirror(0)
    relay_act(0)
    weight_part(0, 0)
    weight_part(0, 1)
    relay_act(1)
    local_plane(3)
    weight_part(1, 0)
    weight_part(1, 1)
    relay_mirror(1)
    reduce_y(0, 0)
    project_mirror()
    send_act(3, own=True)
    reduce_y(0, 1)
    weight_part(0, 2)
    weight_part(1, 2)
    relay_act(2)
    reduce_y(1, 0)
    reduce_z(0, 0)
    relay_act(3)
    reduce_y(1, 1)
    for p in range(P):
        weight_part(2, p)
    reduce_z(0, 1)
    reduce_y(0, 2)
    reduce_y(1, 2)
    for p in range(P):
        weight_part(3, p)
    reduce_z(1, 0)
    gradient(0)

    @pl.when(s > 0)
    def _():
        back.start()

    taps_grad(0)
    reduce_z(1, 1)
    gradient(1)
    taps_grad(1)
    reduce_z(0, 2)
    reduce_z(1, 2)
    gradient(2)
    taps_grad(2)
    reduce_y(2, 0)
    reduce_y(2, 1)
    gradient(3)
    taps_grad(3)
    all_sums = krecv.at[pl.ds(1, S - 1)]
    waits.append(copy(all_sums, all_sums, ids["kg"], s, partner))
    reduce_y(2, 2)
    relay_act(3, own=True)
    gated_grad(0)
    gated_grad(1)
    relayed(3, own=True)
    own_part(3, 0, H)
    reduce_y(3, 0)
    gated_grad(2)
    with jax.named_scope("drain"):
        for r in waits + outer:
            r.wait_send()
        waits.clear()
        outer.clear()
    with jax.named_scope("kgwait"):
        arrived(all_sums, ids["kg"])
    acc = kg[pl.ds(s * cps, cps)]
    for j in range(1, S):
        acc = acc + krecv[j].astype(f32)
    ksum[...] = acc
    for j in range(1, N):
        copy(ksum, k2recv.at[j], ids["k2"], s, lax.rem(d + j, N)).start()
    all_parts = k2recv.at[pl.ds(1, N - 1)]
    waits.append(copy(all_parts, all_parts, ids["k2"], s, partner))
    with jax.named_scope("zwait"):
        for p in range(P):
            arrived(zrecv.at[0, :, part(p)], ids["znear"] + p)
            arrived(zrecv.at[1, :, part(p)], ids["zfar"] + p)

    def final_tile(n, _):
        cols = pl.ds(pl.multiple_of(n * LANES, LANES), LANES)
        acc = wacc[s, :, cols]
        for q in range(2):
            acc = acc + zrecv[q, :, cols].astype(f32)
        acc = acc * factor
        fin[0, :, cols] = acc[:block]
        fin[1, :, cols] = acc[block:]
        return _

    with jax.named_scope("final"):
        lax.fori_loop(0, H // LANES, final_tile, 0)
    send(fin.at[other], fbuf, ids["fin"], s, partner)
    gw[:, half] = fin[c]
    with jax.named_scope("backwait"):
        @pl.when(s < S - 1)
        def _():
            arrived(brecv, ids["back"])

    @pl.when(s == S - 1)
    def _():
        gext[:, pl.ds(T, HB), :] = jnp.zeros((chunks, HB, LANES), f32)

    @pl.when(s < S - 1)
    def _():
        gext[:, pl.ds(T, HB), :] = brecv[...].astype(f32)

    gated_grad(3)
    with jax.named_scope("k2wait"):
        arrived(all_parts, ids["k2"])
        for j in range(1, N):
            acc = acc + k2recv[j]
    for q in range(cps):
        cols = slice(q * LANES, (q + 1) * LANES)
        kout[:, cols] = (acc[q] * factor)[:K]
        gout[:, cols] = (acc[q] * factor)[K : K + 1]

    with jax.named_scope("finwait"):
        arrived(fbuf, ids["fin"])
    with jax.named_scope("fincopy"):
        gw[:, ohalf] = fbuf[...]
    with jax.named_scope("endwaits"):
        for r in waits:
            r.wait_send()

        @pl.when(s < S - 1)
        def _():
            front.wait_send()

        @pl.when(s > 0)
        def _():
            back.wait_send()


def number(*sizes):
    ids, count = {}, 0
    for name, size in sizes:
        ids[name] = count
        count += size
    return ids, count


def hand_over(*refs):
    half = len(refs) // 2
    stores = [pltpu.make_async_copy(refs[i], refs[half + i], refs[-1].at[i]) for i in range(half)]
    for st in stores:
        st.start()
    for st in stores:
        st.wait()


def pair_call(S, N, Y, T, C, K, HB, KP, cot, val, gate, w, kernel, gain):
    X, Z, H = N // 2, S // Y, C // 2
    chunks, cps, cpd, block = C // LANES, C // LANES // S, C // LANES // N, C // (S * N)
    M, CR = chunks // X, C // N
    ids, count = number(
        ("taps", 1), ("front", 1), ("back", 1), ("w", 1), ("cot", (X - 1) * 4), ("cotp", 1),
        ("cotm", (X - 1) * 2), ("act", (X - 1) * (Z - 1 + Y)), ("actp", 1),
        ("actm", (X - 1) * (Z - 1 + Y)), ("ga", (X - 1) * BLOCKS), ("y", (Y - 1) * Z * 3),
        ("zmid", Z // 2 * 3), ("znear", 3), ("zfar", 3), ("fin", 1), ("kg", 1), ("k2", 1),
    )
    vm = pl.BlockSpec(memory_space=pltpu.VMEM)
    hbm = pl.BlockSpec(memory_space=pl.ANY)
    partial = pl.pallas_call(
        functools.partial(pair_kernel, S, N, Y, T, C, K, HB, ids),
        out_shape=(
            jax.ShapeDtypeStruct((T, C), bf16),
            jax.ShapeDtypeStruct((T, C), bf16),
            jax.ShapeDtypeStruct((block, C), f32),
            jax.ShapeDtypeStruct((K, C // S), f32),
            jax.ShapeDtypeStruct((1, C // S), f32),
        ),
        in_specs=[hbm] * 6,
        out_specs=(vm,) * 5,
        scratch_shapes=[
            pltpu.VMEM((K, C // S), bf16),
            pltpu.VMEM((C // S,), bf16),
            pltpu.VMEM((cps, KP, LANES), bf16),
            pltpu.VMEM((T, C), bf16),
            pltpu.VMEM((T, C), bf16),
            pltpu.VMEM((T, C), bf16),
            pltpu.VMEM((CR, C), bf16),
            pltpu.VMEM((CR, C), bf16),
            pltpu.VMEM((X - 1, T, C), bf16),
            pltpu.VMEM((X, T, H), bf16),
            pltpu.VMEM((chunks, HB, LANES), bf16),
            pltpu.VMEM((chunks, HB, LANES), bf16),
            pltpu.VMEM((chunks, HB, LANES), bf16),
            pltpu.VMEM((chunks, HB, LANES), bf16),
            pltpu.VMEM((chunks, T + HB, LANES), f32),
            pltpu.VMEM((chunks, T, LANES), f32),
            pltpu.VMEM((chunks, T, LANES), f32),
            pltpu.VMEM((chunks, T + HB, LANES), f32),
            pltpu.VMEM((chunks, KP, LANES), bf16),
            pltpu.VMEM((X, M, LANES, T), bf16),
            pltpu.VMEM((X - 1, M, LANES, T), bf16),
            pltpu.VMEM((X, M, LANES, T), bf16),
            pltpu.VMEM((X - 1, 2 * cpd, T, LANES), bf16),
            pltpu.VMEM((chunks, T, LANES), bf16),
            pltpu.VMEM((M, LANES, H), f32),
            pltpu.VMEM(((Y - 1) * Z, LANES, H), bf16),
            pltpu.VMEM(((Y - 1) * Z, LANES, H), bf16),
            pltpu.VMEM((Z - 1, LANES, H), bf16),
            pltpu.VMEM((Z // 2, LANES, H), bf16),
            pltpu.VMEM((2, LANES, H), bf16),
            pltpu.VMEM((2, block, H), f32),
            pltpu.VMEM((block, H), f32),
            pltpu.VMEM((T, LANES), f32),
            pltpu.VMEM((T, LANES), f32),
            pltpu.VMEM((T, LANES), f32),
            pltpu.VMEM((T, LANES), f32),
            pltpu.VMEM((chunks, K + 1, 8, LANES), f32),
            pltpu.VMEM((chunks, KP, LANES), f32),
            pltpu.VMEM((chunks, KP, LANES), bf16),
            pltpu.VMEM((S, cps, KP, LANES), bf16),
            pltpu.VMEM((cps, KP, LANES), f32),
            pltpu.VMEM((N, cps, KP, LANES), f32),
            pltpu.SemaphoreType.DMA((count,)),
            pltpu.SemaphoreType.DMA((count,)),
            pltpu.SemaphoreType.DMA((6,)),
            pltpu.SemaphoreType.REGULAR((2 * (Z - 2) + 1,)),
        ],
        compiler_params=pltpu.CompilerParams(
            collective_id=0, has_side_effects=True, vmem_limit_bytes=48 * 1024 * 1024
        ),
        name="block_backward",
    )(*(pltpu.with_memory_space_constraint(a, pltpu.HBM) for a in (cot, val, gate, w, kernel, gain)))
    return pl.pallas_call(
        hand_over,
        out_shape=(
            jax.ShapeDtypeStruct((T, C), bf16),
            jax.ShapeDtypeStruct((T, C), bf16),
            jax.ShapeDtypeStruct((block, C), f32),
            jax.ShapeDtypeStruct((K, C // S), f32),
            jax.ShapeDtypeStruct((1, C // S), f32),
        ),
        in_specs=[vm] * 5,
        out_specs=(hbm,) * 5,
        scratch_shapes=[
            pltpu.SemaphoreType.DMA((5,)),
        ],
        compiler_params=pltpu.CompilerParams(vmem_limit_bytes=16 * T * LANES),
        name="hand_over",
    )(*partial)


def general_call(S, N, T, C, K, HB, KP, cot, val, gate, w, packed):
    chunks, cps, cpd, block = C // LANES, C // LANES // S, C // LANES // N, C // (S * N)
    ids, count = number(
        ("taps", S), ("front", 1), ("back", 1), ("partner", 1), ("mirror", N // 2 * HALVES),
        ("relay", N // 2 * HALVES), ("act", N), ("ga", N), ("rs", S), ("kg", S), ("k2", N),
    )
    vm = pl.BlockSpec(memory_space=pltpu.VMEM)
    return pl.pallas_call(
        functools.partial(general_kernel, S, N, T, C, K, HB, ids),
        out_shape=(
            jax.ShapeDtypeStruct((T, C), bf16),
            jax.ShapeDtypeStruct((T, C), bf16),
            jax.ShapeDtypeStruct((block, C), f32),
            jax.ShapeDtypeStruct((K, C // S), f32),
            jax.ShapeDtypeStruct((1, C // S), f32),
        ),
        in_specs=[vm] * 5,
        out_specs=(vm,) * 5,
        scratch_shapes=[
            pltpu.VMEM((N, T, C), bf16),
            pltpu.VMEM((chunks, T + HB, LANES), f32),
            pltpu.VMEM((chunks, T, LANES), f32),
            pltpu.VMEM((chunks, T, LANES), f32),
            pltpu.VMEM((chunks, T + HB, LANES), f32),
            pltpu.VMEM((chunks, KP, LANES), bf16),
            pltpu.VMEM((chunks, T, LANES), bf16),
            pltpu.VMEM((N, cpd, T, LANES), bf16),
            pltpu.VMEM((N, cpd, T, LANES), bf16),
            pltpu.VMEM((chunks, T, LANES), bf16),
            pltpu.VMEM((cpd * LANES, C), bf16),
            pltpu.VMEM((S, block, C), bf16),
            pltpu.VMEM((chunks, KP, LANES), f32),
            pltpu.VMEM((S, cps, KP, LANES), f32),
            pltpu.VMEM((cps, KP, LANES), f32),
            pltpu.VMEM((N, cps, KP, LANES), f32),
            pltpu.SemaphoreType.DMA((count,)),
            pltpu.SemaphoreType.DMA((count,)),
        ],
        compiler_params=pltpu.CompilerParams(
            collective_id=0, has_side_effects=True, vmem_limit_bytes=60 * 1024 * 1024
        ),
        name="block_backward",
    )(cot, val, gate, w, packed)


def shards(out_cotangent, value_pre, gate_pre, out_weight, conv_kernel, norm_gain):
    S, N = lax.axis_size("sp"), lax.axis_size("dp")
    _, T, C = out_cotangent.shape
    K = conv_kernel.shape[0]
    chunks, cps = C // LANES, C // LANES // S
    HB = -(-(K - 1) // 16) * 16
    KP = -(-(K + 1) // 16) * 16
    args = (out_cotangent[0], value_pre[0], gate_pre[0], out_weight)
    X = N // 2
    if N == 2 * X > 2 and S == 2 * 2 * X and chunks == S * X:
        outs = pair_call(S, N, X, T, C, K, HB, KP, *args, conv_kernel, norm_gain)
    else:
        packed = jnp.concatenate(
            [conv_kernel, norm_gain[None], jnp.zeros((KP - K - 1, C // S), bf16)], axis=0
        )
        packed = jnp.transpose(packed.reshape(KP, cps, LANES), (1, 0, 2))
        outs = general_call(S, N, T, C, K, HB, KP, *args, packed)
    grad_value, grad_gate, grad_weight, grad_taps, grad_gain = outs
    return grad_value[None], grad_gate[None], grad_weight, grad_taps, grad_gain[0]


def solution(mesh):
    placed = (
        P("dp", "sp", None),
        P("dp", "sp", None),
        P("dp", "sp", None),
        P("dp", None),
        P(None, "sp"),
        P("sp"),
    )
    return jax.shard_map(
        shards,
        mesh=mesh,
        in_specs=placed,
        out_specs=(
            P("dp", "sp", None),
            P("dp", "sp", None),
            P(("sp", "dp"), None),
            P(None, "sp"),
            P("sp"),
        ),
        check_vma=False,
    )
```

```python
import functools

import jax
import jax.numpy as jnp
from jax import lax
from jax.experimental import pallas as pl
from jax.experimental.pallas import tpu as pltpu
from jax.sharding import PartitionSpec as P

epsilon = 1e-05
LANES = 128
HALVES = 2
BLOCKS = 4
f32 = jnp.float32
bf16 = jnp.bfloat16


def general_kernel(
    S, N, T, C, K, HB, ids,
    cot, val, gate, w, taps,
    gv, gg, gw, kout, gout,
    cot_all, ext, cen, gc, gext, kall, act, act_all, ga_send, ga, wpart, rbuf,
    kg, krecv, ksum, k2recv, send_sem, recv_sem,
):
    s = lax.axis_index("sp")
    d = lax.axis_index("dp")
    chunks = C // LANES
    cps = chunks // S
    cpd = chunks // N
    block = C // (S * N)
    RB = min(T, 128)
    total = S * N
    me = s * N + d
    partner = d + 1 - 2 * lax.rem(d, 2)
    factor = float(S * N * T) ** (-0.5)
    hrows = T // HALVES
    waits = []

    def copy(src, dst, i, to_s, to_d):
        return pltpu.make_async_remote_copy(
            src_ref=src, dst_ref=dst, send_sem=send_sem.at[i], recv_sem=recv_sem.at[i],
            device_id={"sp": to_s, "dp": to_d}, device_id_type=pl.DeviceIdType.MESH,
        )

    def send(src, dst, i, to_s, to_d):
        c = copy(src, dst, i, to_s, to_d)
        c.start()
        waits.append(c)

    def arrived(dst, i):
        copy(dst, dst, i, s, partner).wait_recv()

    barrier = pltpu.get_barrier_semaphore()

    def greet(j, _):
        other = lax.rem(me + j, total)
        pl.semaphore_signal(
            barrier, inc=1, device_id={"sp": other // N, "dp": lax.rem(other, N)},
            device_id_type=pl.DeviceIdType.MESH,
        )
        return _

    lax.fori_loop(1, total, greet, 0)
    def gate_chunk(cb, _):
        cols = pl.ds(pl.multiple_of(cb * LANES, LANES), LANES)
        sig = jax.nn.sigmoid(gate[:, cols].astype(f32))
        ext[cb, pl.ds(HB, T), :] = (val[:, cols].astype(f32) * sig).astype(bf16).astype(f32)
        return _

    lax.fori_loop(0, chunks, gate_chunk, 0)
    pl.semaphore_wait(barrier, total - 1)

    for j in range(1, S):
        send(taps, kall.at[pl.ds(s * cps, cps)], ids["taps"] + j, lax.rem(s + j, S), d)
    following = lax.rem(s + 1, S)
    preceding = lax.rem(s + S - 1, S)
    send(ext.at[:, pl.ds(T, HB), :], ext.at[:, pl.ds(0, HB), :], ids["front"], following, d)
    for j in range(1, N // 2):
        for h in range(HALVES):
            rows = pl.ds(h * hrows, hrows)
            send(cot.at[rows], cot_all.at[d, rows], ids["mirror"] + j * HALVES + h, s, lax.rem(d + 2 * j, N))
    send(cot, cot_all.at[d], ids["partner"], s, partner)
    kall[pl.ds(s * cps, cps)] = taps[...]
    cot_all[d] = cot[...]
    for j in range(1, S):
        arrived(kall.at[pl.ds(lax.rem(s + S - j, S) * cps, cps)], ids["taps"] + j)
    arrived(ext.at[:, pl.ds(0, HB), :], ids["front"])

    @pl.when(s == 0)
    def _():
        ext[:, pl.ds(0, HB), :] = jnp.zeros((chunks, HB, LANES), f32)

    def conv_chunk(cb, sums):
        tf = kall[cb].astype(f32)
        parts = []
        for rb in range(T // RB):
            acc = jnp.zeros((RB, LANES), f32)
            for k in range(K):
                acc = acc + tf[k : k + 1] * ext[cb, pl.ds(HB - k + rb * RB, RB), :]
            cen[cb, pl.ds(rb * RB, RB), :] = acc
            parts.append(jnp.sum(acc, axis=1, keepdims=True))
        return sums + jnp.concatenate(parts, axis=0)

    column = jnp.zeros((T, 1), f32)
    mean = lax.fori_loop(0, chunks, conv_chunk, column) / C

    def square_chunk(cb, sums):
        dev = cen[cb] - mean
        return sums + dev * dev

    squares = lax.fori_loop(0, chunks, square_chunk, jnp.zeros((T, LANES), f32))
    inv = lax.rsqrt(jnp.sum(squares, axis=1, keepdims=True) / C + epsilon)

    def relay():
        for j in range(1, N // 2):
            origin = lax.rem(d + N - 2 * j, N)
            for h in range(HALVES):
                piece = cot_all.at[origin, pl.ds(h * hrows, hrows)]
                arrived(piece, ids["mirror"] + j * HALVES + h)
                send(piece, piece, ids["relay"] + j * HALVES + h, s, partner)

    def act_chunk(cb, _):
        centred = (cen[cb] - mean) * inv
        cen[cb] = centred
        normed = centred * kall[cb].astype(f32)[K : K + 1]
        act[cb] = (normed * jax.nn.sigmoid(normed)).astype(bf16)
        return _

    lax.fori_loop(0, chunks, act_chunk, 0)
    for j in range(1, N):
        to = lax.rem(d + j, N)
        send(act.at[pl.ds(to * cpd, cpd)], act_all.at[d], ids["act"] + j, s, to)
    act_all[d] = act[pl.ds(d * cpd, cpd)]

    def project(source, slot):
        def pair(m, _):
            rows = pl.ds(pl.multiple_of(m * 2 * LANES, 2 * LANES), 2 * LANES)
            out = lax.dot_general(
                cot_all[source], w[rows, :], (((1,), (1,)), ((), ())), preferred_element_type=f32
            ).astype(bf16)
            ga_send[slot, 2 * m] = out[:, :LANES]
            ga_send[slot, 2 * m + 1] = out[:, LANES:]
            return _

        lax.fori_loop(0, cpd // 2, pair, 0)

    mine = pl.ds(d * cpd, cpd)
    project(d, 0)
    ga[mine] = ga_send[0]
    arrived(cot_all.at[partner], ids["partner"])
    project(partner, 1)
    send(ga_send.at[1], ga.at[mine], ids["ga"] + 1, s, partner)
    relay()
    for j in range(1, N // 2):
        origin = lax.rem(d + N - 2 * j, N)
        project(origin, 2 * j)
        send(ga_send.at[2 * j], ga.at[mine], ids["ga"] + 2 * j, s, origin)
    for j in range(1, N // 2):
        origin = lax.rem(partner + N - 2 * j, N)
        for h in range(HALVES):
            arrived(cot_all.at[origin, pl.ds(h * hrows, hrows)], ids["relay"] + j * HALVES + h)
        project(origin, 2 * j + 1)
        send(ga_send.at[2 * j + 1], ga.at[mine], ids["ga"] + 2 * j + 1, s, origin)

    for j in range(1, N):
        arrived(act_all.at[lax.rem(d + N - j, N)], ids["act"] + j)
    NT = min(C, 512)

    def weight_tile(i, _):
        m, n = i // (C // NT), lax.rem(i, C // NT)
        cols = pl.ds(pl.multiple_of(n * NT, NT), NT)
        acc = jnp.zeros((LANES, NT), f32)
        for q in range(N):
            acc = acc + lax.dot_general(
                act_all[q, m], cot_all[q, :, cols], (((0,), (0,)), ((), ())),
                preferred_element_type=f32,
            )
        wpart[pl.ds(pl.multiple_of(m * LANES, LANES), LANES), cols] = acc.astype(bf16)
        return _

    lax.fori_loop(0, cpd * (C // NT), weight_tile, 0)

    def block_of(j):
        i = lax.rem(s + j, S)
        owner = d * S + i
        rows = pl.ds(pl.multiple_of(i * block, block), block)
        return owner, rows, pltpu.make_async_remote_copy(
            src_ref=wpart.at[rows], dst_ref=rbuf.at[s], send_sem=send_sem.at[ids["rs"] + j],
            recv_sem=recv_sem.at[ids["rs"] + s],
            device_id={"sp": owner // N, "dp": lax.rem(owner, N)},
            device_id_type=pl.DeviceIdType.MESH,
        )

    def send_blocks(first, last):
        for j in range(first, last):
            owner, rows, c = block_of(j)

            @pl.when(owner != me)
            def _():
                c.start()

            @pl.when(owner == me)
            def _():
                rbuf[s] = wpart[rows, :]

    send_blocks(0, S // 2)

    for j in range(1, N // 2):
        arrived(ga.at[pl.ds(lax.rem(d + 2 * j, N) * cpd, cpd)], ids["ga"] + 2 * j)
        arrived(ga.at[pl.ds(lax.rem(partner + 2 * j, N) * cpd, cpd)], ids["ga"] + 2 * j + 1)
    arrived(ga.at[pl.ds(partner * cpd, cpd)], ids["ga"] + 1)

    def grad_chunk(cb, sums):
        one, two = sums
        centred = cen[cb]
        gain = kall[cb].astype(f32)[K : K + 1]
        normed = centred * gain
        sg = jax.nn.sigmoid(normed)
        grad = ga[cb].astype(f32) * sg * (1.0 + normed * (1.0 - sg))
        kg[cb, pl.ds(K, 1), :] = jnp.sum(grad * centred, axis=0, keepdims=True)
        grad = grad * gain
        gc[cb] = grad
        return one + grad, two + grad * centred

    zero = jnp.zeros((T, LANES), f32)
    one, two = lax.fori_loop(0, chunks, grad_chunk, (zero, zero))
    first = jnp.sum(one, axis=1, keepdims=True) / C
    second = jnp.sum(two, axis=1, keepdims=True) / C

    def conv_grad(cb, _):
        gext[cb, pl.ds(0, T), :] = (gc[cb] - first - cen[cb] * second) * inv
        return _

    lax.fori_loop(0, chunks, conv_grad, 0)
    send(gext.at[:, pl.ds(0, HB), :], gext.at[:, pl.ds(T, HB), :], ids["back"], preceding, d)

    def taps_chunk(cb, _):
        for k in range(K):
            acc = jnp.zeros((8, LANES), f32)
            for rb in range(T // RB):
                prod = gext[cb, pl.ds(rb * RB, RB), :] * ext[cb, pl.ds(HB - k + rb * RB, RB), :]
                acc = acc + jnp.sum(prod.reshape(RB // 8, 8, LANES), axis=0)
            kg[cb, pl.ds(k, 1), :] = jnp.sum(acc, axis=0, keepdims=True)
        return _

    lax.fori_loop(0, chunks, taps_chunk, 0)
    for j in range(1, S):
        to = lax.rem(s + j, S)
        send(kg.at[pl.ds(to * cps, cps)], krecv.at[j], ids["kg"] + j, to, d)
    send_blocks(S // 2, S)

    arrived(gext.at[:, pl.ds(T, HB), :], ids["back"])

    @pl.when(s == S - 1)
    def _():
        gext[:, pl.ds(T, HB), :] = jnp.zeros((chunks, HB, LANES), f32)

    def gated_chunk(cb, _):
        cols = pl.ds(pl.multiple_of(cb * LANES, LANES), LANES)
        tf = kall[cb].astype(f32)
        for rb in range(T // RB):
            rows = pl.ds(rb * RB, RB)
            acc = jnp.zeros((RB, LANES), f32)
            for k in range(K):
                acc = acc + tf[k : k + 1] * gext[cb, pl.ds(k + rb * RB, RB), :]
            acc = acc.astype(bf16).astype(f32)
            sig = jax.nn.sigmoid(gate[rows, cols].astype(f32))
            gv[rows, cols] = (acc * sig).astype(bf16)
            gg[rows, cols] = (acc * val[rows, cols].astype(f32) * sig * (1.0 - sig)).astype(bf16)
        return _

    lax.fori_loop(0, chunks, gated_chunk, 0)

    acc = kg[pl.ds(s * cps, cps)]
    for j in range(1, S):
        arrived(krecv.at[j], ids["kg"] + j)
        acc = acc + krecv[j]
    ksum[...] = acc
    for j in range(1, N):
        send(ksum, k2recv.at[j], ids["k2"] + j, s, lax.rem(d + j, N))
    for j in range(1, N):
        arrived(k2recv.at[j], ids["k2"] + j)
        acc = acc + k2recv[j]
    for c in range(cps):
        cols = slice(c * LANES, (c + 1) * LANES)
        kout[:, cols] = (acc[c] * factor)[:K]
        gout[:, cols] = (acc[c] * factor)[K : K + 1]

    home = me // S
    for q in range(S):
        @pl.when(jnp.logical_or(q != s, home != d))
        def _():
            arrived(rbuf.at[q], ids["rs"] + q)

    def sum_tile(n, _):
        cols = pl.ds(pl.multiple_of(n * LANES, LANES), LANES)
        acc = rbuf[0, :, cols].astype(f32)
        for q in range(1, S):
            acc = acc + rbuf[q, :, cols].astype(f32)
        gw[:, cols] = acc * factor
        return _

    lax.fori_loop(0, chunks, sum_tile, 0)
    for j in range(S):
        owner, rows, c = block_of(j)

        @pl.when(owner != me)
        def _():
            c.wait_send()

    for c in waits:
        c.wait_send()


def pair_kernel(
    S, N, Y, T, C, K, HB, ids,
    cot_in, val_in, gate_in, w_in, kernel_in, gain_in,
    gv, gg, gw, kout, gout,
    kernel, gain, taps, cot, val, gate, w, w_p, cot_m, cot_p, fsend, frecv, bsend, brecv, ext, cen, gc, gext, kall,
    act, act_m, act_p, ga_s, ga, wacc, wpart, yrecv, ysum, zmid, zrecv, fin, fbuf,
    sigs, slopes, means, invs, sum1, sum2, kacc, kg, kgb, krecv, ksum, k2recv, send_sem, recv_sem, load_sem, ready,
):
    s = lax.axis_index("sp")
    d = lax.axis_index("dp")
    X, Z, H = N // 2, S // Y, C // 2
    x, c = d // 2, lax.rem(d, 2)
    y, z = lax.rem(s, Y), s // Y
    other = 1 - c
    partner = d + 1 - 2 * c
    chunks = C // LANES
    cps = chunks // S
    cpd = chunks // N
    block = C // (S * N)
    M = chunks // X
    RB = min(T, 128)
    TB = T // BLOCKS
    factor = float(S * N * T) ** (-0.5)
    waits = []

    kinds = sorted(ids.values())

    def copy(src, dst, i, to_s, to_d, j=None):
        kind = max(n for n, first in enumerate(kinds) if first <= i)
        return pltpu.make_async_remote_copy(
            src_ref=src, dst_ref=dst, send_sem=send_sem.at[kind],
            recv_sem=recv_sem.at[i if j is None else j],
            device_id={"sp": to_s, "dp": to_d}, device_id_type=pl.DeviceIdType.MESH,
        )

    def send(src, dst, i, to_s, to_d, j=None):
        r = copy(src, dst, i, to_s, to_d, j)
        r.start()
        if i in (ids["w"], ids["cotp"], ids["actp"], ids["fin"]):
            waits.append(r)

    def arrived(dst, i):
        copy(dst, dst, i, s, partner).wait_recv()

    loads = [
        pltpu.make_async_copy(a, b, load_sem.at[i])
        for i, (a, b) in enumerate((
            (gate_in, gate), (val_in, val), (cot_in, cot), (w_in, w), (kernel_in, kernel), (gain_in, gain),
        ))
    ]
    for l in loads:
        l.start()

    barrier = pltpu.get_barrier_semaphore()

    def signal(sem, to_s, to_d):
        pl.semaphore_signal(
            sem, inc=1, device_id={"sp": to_s, "dp": to_d}, device_id_type=pl.DeviceIdType.MESH
        )

    def along_z(action):
        @pl.when(z > 0)
        def _():
            action(0, s - Y)

        @pl.when(z < Z - 1)
        def _():
            action(1, s + Y)

    signal(barrier, s, partner)
    for j in range(1, X):
        signal(barrier, s, lax.rem(d + 2 * j, N))
    for j in range(1, Y):
        signal(barrier, z * Y + lax.rem(y + j, Y), d)
    along_z(lambda side, to_s: signal(barrier, to_s, d))
    loads[2].wait()
    with jax.named_scope("barrierwait"):
        pl.semaphore_wait(barrier, X + Y - 1 + jnp.where(z > 0, 1, 0) + jnp.where(z < Z - 1, 1, 0))

    def pass_on(r):
        along_z(lambda side, to_s: signal(ready.at[2 * r + 1 - side], to_s, d))

    def passed(r):
        along_z(lambda side, to_s: pl.semaphore_wait(ready.at[2 * r + side], 1))

    pass_on(0)
    strips = ((0, H - H // BLOCKS), (H - H // BLOCKS, H // BLOCKS))
    parts = ((0, H // 2), (H // 2, H // BLOCKS), (H - H // BLOCKS, H // BLOCKS))
    P = len(parts)

    def strip(side, p):
        return pl.ds(pl.multiple_of(side * H + strips[p][0], LANES), strips[p][1])

    def part(p):
        return pl.ds(parts[p][0], parts[p][1])

    def send_cot(p):
        for j in range(1, X):
            for side in range(2):
                send(
                    cot.at[:, strip(side, p)], cot_m.at[j - 1, :, strip(side, p)],
                    ids["cot"] + ((j - 1) * 2 + p) * 2 + side, s, lax.rem(d + 2 * j, N),
                )

    send_cot(0)
    loads[0].wait()
    loads[1].wait()

    def gate_chunk(cb, _):
        cols = pl.ds(pl.multiple_of(cb * LANES, LANES), LANES)
        sig = jax.nn.sigmoid(gate[:, cols].astype(f32))
        gated = (val[:, cols].astype(f32) * sig).astype(bf16)
        ext[cb, pl.ds(HB, T), :] = gated.astype(f32)
        fsend[cb] = gated[T - HB :]
        return _

    with jax.named_scope("gate"):
        lax.fori_loop(0, chunks, gate_chunk, 0)
    loads[4].wait()
    loads[5].wait()
    KP = taps.shape[1]
    for q in range(cps):
        cols = slice(q * LANES, (q + 1) * LANES)
        taps[q] = jnp.concatenate(
            [kernel[:, cols].astype(f32), gain[cols].astype(f32).reshape(1, LANES)]
            + [jnp.zeros((KP - K - 1, LANES), f32)] * (KP > K + 1),
            axis=0,
        ).astype(bf16)
    half = pl.ds(pl.multiple_of(c * H, LANES), H)
    ohalf = pl.ds(pl.multiple_of(other * H, LANES), H)
    loads[3].wait()
    send(w, w_p, ids["w"], s, partner)
    send(cot.at[:, ohalf], cot_p.at[0], ids["cotp"], s, partner)
    kall[pl.ds(s * cps, cps)] = taps[...]
    with jax.named_scope("ready"):
        for r in range(Z - 2):
            if r > 0:
                pass_on(r)
            passed(r)
        for j in range(1, Y):
            signal(ready.at[2 * (Z - 2)], z * Y + lax.rem(y + j, Y), d)
        pl.semaphore_wait(ready.at[2 * (Z - 2)], Y - 1)
    for j in range(1, S):
        copy(taps, kall.at[pl.ds(s * cps, cps)], ids["taps"], lax.rem(s + j, S), d).start()
    all_taps = kall.at[pl.ds(0, chunks - cps)]
    waits.append(copy(all_taps, all_taps, ids["taps"], s, partner))
    front = copy(fsend, frecv, ids["front"], lax.rem(s + 1, S), d)

    @pl.when(s < S - 1)
    def _():
        front.start()


    def project(rows_of, weights, out, base):
        def pair(m, _):
            rows = pl.ds(pl.multiple_of(m * 2 * LANES, 2 * LANES), 2 * LANES)
            prod = lax.dot_general(
                rows_of[...], weights[rows, :], (((1,), (1,)), ((), ())), preferred_element_type=f32
            ).astype(bf16)
            out[base + 2 * m] = prod[:, :LANES]
            out[base + 2 * m + 1] = prod[:, LANES:]
            return _

        lax.fori_loop(0, cpd // 2, pair, 0)

    def slope_chunk(cb, _):
        cols = pl.ds(pl.multiple_of(cb * LANES, LANES), LANES)
        sig = jax.nn.sigmoid(gate[:, cols].astype(f32))
        sigs[cb] = sig
        slopes[cb] = val[:, cols].astype(f32) * sig * (1.0 - sig)
        return _

    with jax.named_scope("slopes"):
        lax.fori_loop(0, chunks, slope_chunk, 0)
    with jax.named_scope("proj_own"):
        project(cot, w, ga, d * cpd)
    with jax.named_scope("tapswait"):
        arrived(all_taps, ids["taps"])

        @pl.when(s > 0)
        def _():
            arrived(frecv, ids["front"])

    @pl.when(s == 0)
    def _():
        ext[:, pl.ds(0, HB), :] = jnp.zeros((chunks, HB, LANES), f32)

    @pl.when(s > 0)
    def _():
        ext[:, pl.ds(0, HB), :] = frecv[...].astype(f32)

    def convolve(cb, rb):
        tf = kall[cb].astype(f32)
        acc = jnp.zeros((RB, LANES), f32)
        for k in range(K):
            acc = acc + tf[k : k + 1] * ext[cb, pl.ds(HB - k + rb * RB, RB), :]
        cen[cb, pl.ds(rb * RB, RB), :] = acc
        return acc

    def conv_chunk(cb, _):
        for rb in range(T // RB):
            rows = pl.ds(rb * RB, RB)
            dev = convolve(cb, rb) - means[rows, :]
            sum1[rows, :] = sum1[rows, :] + dev
            sum2[rows, :] = sum2[rows, :] + dev * dev
        return _

    with jax.named_scope("conv"):
        for rb in range(T // RB):
            rows = pl.ds(rb * RB, RB)
            acc = convolve(0, rb)
            start = jnp.broadcast_to(jnp.sum(acc, axis=1, keepdims=True) / LANES, (RB, LANES))
            means[rows, :] = start
            sum1[rows, :] = acc - start
            sum2[rows, :] = (acc - start) * (acc - start)
        lax.fori_loop(1, chunks, conv_chunk, 0)
    with jax.named_scope("moments"):
        shift = jnp.sum(sum1[...], axis=1, keepdims=True) / C
        variance = jnp.sum(sum2[...], axis=1, keepdims=True) / C - shift * shift
        means[...] = means[...] + shift
        invs[...] = jnp.broadcast_to(lax.rsqrt(variance + epsilon), (T, LANES))

    def act_chunk(cb, _):
        centred = (cen[cb] - means[...]) * invs[...]
        cen[cb] = centred
        normed = centred * kall[cb].astype(f32)[K : K + 1]
        act[lax.rem(cb, X), cb // X] = (normed * jax.nn.sigmoid(normed)).T.astype(bf16)
        return _

    with jax.named_scope("act"):
        lax.fori_loop(0, chunks, act_chunk, 0)
    send(act.at[x], act_p.at[0], ids["actp"], s, partner)

    near = Z // 2
    low = z < near
    inner_z = jnp.where(low, near - 1, near)
    inner = z == inner_z

    def plane(k):
        if k < near:
            return jnp.where(low, Z - 1 - k, k)
        return jnp.where(low, 0, near) + lax.rem(z + 1 + k, near)

    def planes(k, own):
        first = k if k == 0 else k + Y - 1
        if 0 < k < Z - 1:
            return [(plane(k) * Y, Y, first)]
        chosen = range(1) if own else range(1, Y)
        return [(plane(k) * Y + lax.rem(y + j, Y), 1, first + j) for j in chosen]

    def send_act(k, own=False):
        for first, size, n in planes(k, own):
            piece = pl.ds(first, size)
            for j in range(1, X):
                send(
                    act.at[lax.rem(x + j, X), piece], act_m.at[j - 1, piece],
                    ids["act"] + (j - 1) * (Z - 2 + 2 * Y) + n, s, lax.rem(d + 2 * j, N),
                )

    def relay_mirror(p):
        with jax.named_scope("cotwait%d" % p):
            for j in range(1, X):
                for side in range(2):
                    arrived(cot_m.at[j - 1, :, strip(side, p)], ids["cot"] + ((j - 1) * 2 + p) * 2 + side)
                send(
                    cot_m.at[j - 1, :, strip(other, p)], cot_p.at[j, :, strip(0, p)],
                    ids["cotm"] + (j - 1) * 2 + p, s, partner,
                )

    def project_mirror():
        for j in range(1, X):
            with jax.named_scope("proj_m"):
                project(cot_m.at[j - 1], w, ga_s.at[j - 1], c * cpd)
                project(cot_m.at[j - 1], w_p, ga_s.at[j - 1], other * cpd)
            for b in range(BLOCKS):
                rows = pl.ds(b * TB, TB)
                send(
                    ga_s.at[j - 1, :, rows], ga.at[pl.ds(x * 2 * cpd, 2 * cpd), rows],
                    ids["ga"] + (j - 1) * BLOCKS + b, s, lax.rem(d + 2 * (X - j), N),
                )

    dims = (((1,), (0,)), ((), ()))

    def dot(a, b):
        return lax.dot_general(a, b, dims, preferred_element_type=f32)

    LT = H // 2

    def local_plane(k):
        def tile(i, _):
            m, n = plane(k) * Y + i // 2, lax.rem(i, 2)
            cols = pl.ds(pl.multiple_of(n * LT, LT), LT)
            own = pl.ds(pl.multiple_of(c * H + n * LT, LT), LT)
            wacc[m, :, cols] = dot(act[x, m], cot[:, own]) + dot(act_p[0, m], cot_p[0, :, cols])
            return _

        with jax.named_scope("wlocal%d" % k):
            if k == 0:
                arrived(cot_p.at[0], ids["cotp"])
                arrived(act_p.at[0], ids["actp"])
            lax.fori_loop(0, Y * 2, tile, 0)

    NT = H // BLOCKS

    def remote_part(m, n):
        cols = pl.ds(pl.multiple_of(n * NT, NT), NT)
        own = pl.ds(pl.multiple_of(c * H + n * NT, NT), NT)
        acc = wacc[m, :, cols]
        for j in range(1, X):
            acc = acc + dot(act_m[j - 1, m], cot_m[j - 1, :, own]) + dot(act_p[j, m], cot_p[j, :, cols])
        return cols, acc

    def relay_act(k, own=False):
        with jax.named_scope("actwait%d" % k):
            for first, size, n in planes(k, own):
                piece = pl.ds(first, size)
                for j in range(1, X):
                    i = (j - 1) * (Z - 2 + 2 * Y) + n
                    arrived(act_m.at[j - 1, piece], ids["act"] + i)
                    send(act_m.at[j - 1, piece], act_p.at[j, piece], ids["actm"] + i, s, partner)

    def relayed(k, own=False):
        with jax.named_scope("relaywait%d" % k):
            for first, size, n in planes(k, own):
                for j in range(1, X):
                    arrived(act_p.at[j, pl.ds(first, size)], ids["actm"] + (j - 1) * (Z - 2 + 2 * Y) + n)

    def own_part(k, off, size):
        def own_tile(n, _):
            m = plane(k) * Y + y
            cols, acc = remote_part(m, n)
            wacc[m, :, cols] = acc
            return _

        lax.fori_loop(off // NT, (off + size) // NT, own_tile, 0)

    def weight_part(k, p):
        off, size = parts[p]
        if p == 0:
            relayed(k)
        if k == 0 and p != 1:
            q = 0 if p == 0 else 1
            for j in range(1, X):
                arrived(cot_p.at[j, :, strip(0, q)], ids["cotm"] + (j - 1) * 2 + q)
        with jax.named_scope("wremote%d%d" % (k, p)):
            for j in range(1, Y):
                to_y = lax.rem(y + j, Y)
                i = (j - 1) * Z + k

                def send_tile(n, _):
                    cols, acc = remote_part(plane(k) * Y + to_y, n)
                    wpart[i, :, cols] = acc.astype(bf16)
                    return _

                lax.fori_loop(off // NT, (off + size) // NT, send_tile, 0)
                send(
                    wpart.at[i, :, part(p)], yrecv.at[i, :, part(p)],
                    ids["y"] + i * P + p, z * Y + to_y, d,
                )

            if 0 < k < Z - 1:
                own_part(k, off, size)

    def reduce_y(k, p):
        for q in (p,) if k < Z - 1 else range(P):
            with jax.named_scope("ywait%d%d" % (k, q)):
                for j in range(1, Y):
                    i = (j - 1) * Z + k
                    arrived(yrecv.at[i, :, part(q)], ids["y"] + i * P + q)
        to_z = plane(k)
        m = to_z * Y + y

        def tile(n, _):
            cols = pl.ds(pl.multiple_of(n * LANES, LANES), LANES)
            acc = wacc[m, :, cols]
            for j in range(1, Y):
                acc = acc + yrecv[(j - 1) * Z + k, :, cols].astype(f32)
            if k < Z - 1:
                ysum[k, :, cols] = acc.astype(bf16)
            if k != Z - 2:
                wacc[m, :, cols] = acc
            return _

        off, size = parts[p] if k < Z - 1 else (0, H)
        lax.fori_loop(off // LANES, (off + size) // LANES, tile, 0)
        if k < near:
            r = copy(
                ysum.at[k, :, part(p)], zmid.at[k, :, part(p)], ids["zmid"] + k * P + p,
                inner_z * Y + y, d,
            )

            @pl.when(jnp.logical_not(inner))
            def _():
                r.start()

        elif k < Z - 1:
            send(
                ysum.at[k, :, part(p)], zrecv.at[0, :, part(p)], ids["znear"] + p,
                to_z * Y + y, d,
            )

    def reduce_z(k, p):
        to_z = plane(k)
        m = to_z * Y + y
        off, size = parts[p]

        def tile(n, _):
            cols = pl.ds(pl.multiple_of(n * LANES, LANES), LANES)
            ysum[k, :, cols] = (wacc[m, :, cols] + zmid[k, :, cols].astype(f32)).astype(bf16)
            return _

        @pl.when(inner)
        def _():
            with jax.named_scope("zmid%d%d" % (k, p)):
                arrived(zmid.at[k, :, part(p)], ids["zmid"] + k * P + p)
            lax.fori_loop(off // LANES, (off + size) // LANES, tile, 0)
            copy(
                ysum.at[k, :, part(p)], zrecv.at[1, :, part(p)], ids["zmid"] + k * P + p,
                to_z * Y + y, d, ids["zfar"] + p,
            ).start()

    def fold(v):
        return jnp.sum(v.reshape(v.shape[0] // 8, 8, LANES), axis=0)

    def gradient(b):
        rows = pl.ds(b * TB, TB)
        with jax.named_scope("gawait%d" % b):
            for j in range(1, X):
                origin = lax.rem(x + j, X)
                arrived(ga.at[pl.ds(origin * 2 * cpd, 2 * cpd), rows], ids["ga"] + (X - j - 1) * BLOCKS + b)

        def grad_chunk(cb, sums):
            one, two = sums
            centred = cen[cb, rows, :]
            gain = kall[cb].astype(f32)[K : K + 1]
            normed = centred * gain
            sg = jax.nn.sigmoid(normed)
            grad = ga[cb, rows, :].astype(f32) * sg * (1.0 + normed * (1.0 - sg))
            scaled = grad * centred
            kacc[cb, K] = fold(scaled) if b == 0 else kacc[cb, K] + fold(scaled)
            gc[cb, rows, :] = grad * gain
            return one + grad * gain, two + scaled * gain

        zero = jnp.zeros((TB, LANES), f32)
        with jax.named_scope("gradchunk%d" % b):
            one, two = lax.fori_loop(0, chunks, grad_chunk, (zero, zero))
        first = jnp.sum(one, axis=1, keepdims=True) / C
        second = jnp.sum(two, axis=1, keepdims=True) / C
        scale = invs[rows, :]

        def conv_grad(cb, _):
            grad = (gc[cb, rows, :] - first - cen[cb, rows, :] * second) * scale
            gext[cb, rows, :] = grad
            if b == 0:
                bsend[cb] = grad[:HB].astype(bf16)
            return _

        with jax.named_scope("convgrad%d" % b):
            lax.fori_loop(0, chunks, conv_grad, 0)

    def kg_copy(off):
        to = lax.rem(s + off, S)
        return copy(kgb.at[pl.ds(to * cps, cps)], krecv.at[off], ids["kg"], to, d)

    def taps_grad(b):
        def taps_chunk(cb, _):
            grad = gext[cb, pl.ds(b * TB, TB), :]
            for k in range(K):
                acc = fold(grad * ext[cb, pl.ds(HB - k + b * TB, TB), :])
                if b > 0:
                    acc = acc + kacc[cb, k]
                if b < BLOCKS - 1:
                    kacc[cb, k] = acc
                else:
                    kg[cb, pl.ds(k, 1), :] = jnp.sum(acc, axis=0, keepdims=True)
            if b == BLOCKS - 1:
                kg[cb, pl.ds(K, 1), :] = jnp.sum(kacc[cb, K], axis=0, keepdims=True)
                kgb[cb] = kg[cb].astype(bf16)
            return _

        def taps_owner(n, _):
            off = jnp.where(low, S - 1 - n, 1 + n)
            to = lax.rem(s + off, S)
            lax.fori_loop(to * cps, to * cps + cps, taps_chunk, 0)
            kg_copy(off).start()
            return _

        with jax.named_scope("taps%d" % b):
            if b < BLOCKS - 1:
                lax.fori_loop(0, chunks, taps_chunk, 0)
            else:
                lax.fori_loop(0, S - 1, taps_owner, 0)
                lax.fori_loop(s * cps, s * cps + cps, taps_chunk, 0)

    def gated_grad(b):
        rows = pl.ds(b * TB, TB)

        def gated_chunk(cb, _):
            cols = pl.ds(pl.multiple_of(cb * LANES, LANES), LANES)
            tf = kall[cb].astype(f32)
            acc = jnp.zeros((TB, LANES), f32)
            for k in range(K):
                acc = acc + tf[k : k + 1] * gext[cb, pl.ds(k + b * TB, TB), :]
            acc = acc.astype(bf16).astype(f32)
            gv[rows, cols] = (acc * sigs[cb, rows, :]).astype(bf16)
            gg[rows, cols] = (acc * slopes[cb, rows, :]).astype(bf16)
            return _

        with jax.named_scope("gated%d" % b):
            lax.fori_loop(0, chunks, gated_chunk, 0)

    back = copy(bsend, brecv, ids["back"], lax.rem(s + S - 1, S), d)
    send_act(0)
    send_act(0, own=True)
    send_act(1)
    send_cot(1)
    send_act(2)
    send_act(3)
    arrived(w_p, ids["w"])
    with jax.named_scope("proj_p"):
        project(cot, w_p, ga, partner * cpd)
    local_plane(0)
    local_plane(1)
    relay_mirror(0)
    relay_act(0)
    local_plane(2)
    weight_part(0, 0)
    weight_part(0, 1)
    relay_act(0, own=True)
    local_plane(3)
    relay_act(1)
    relayed(0, own=True)
    own_part(0, 0, H - H // BLOCKS)
    weight_part(1, 0)
    weight_part(1, 1)
    relay_mirror(1)
    reduce_y(0, 0)
    project_mirror()
    send_act(3, own=True)
    reduce_y(0, 1)
    weight_part(0, 2)
    own_part(0, H - H // BLOCKS, H // BLOCKS)
    weight_part(1, 2)
    relay_act(2)
    reduce_y(1, 0)
    reduce_z(0, 0)
    relay_act(3)
    reduce_y(1, 1)
    for p in range(P):
        weight_part(2, p)
    reduce_z(0, 1)
    reduce_y(0, 2)
    reduce_y(1, 2)
    for p in range(P):
        weight_part(3, p)
    reduce_z(1, 0)
    gradient(0)

    @pl.when(s > 0)
    def _():
        back.start()

    taps_grad(0)
    reduce_z(1, 1)
    gradient(1)
    taps_grad(1)
    reduce_z(0, 2)
    reduce_z(1, 2)
    gradient(2)
    taps_grad(2)
    reduce_y(2, 0)
    reduce_y(2, 1)
    gradient(3)
    taps_grad(3)
    all_sums = krecv.at[pl.ds(1, S - 1)]
    waits.append(copy(all_sums, all_sums, ids["kg"], s, partner))
    reduce_y(2, 2)
    relay_act(3, own=True)
    gated_grad(0)
    gated_grad(1)
    relayed(3, own=True)
    own_part(3, 0, H)
    reduce_y(3, 0)
    gated_grad(2)
    with jax.named_scope("drain"):
        for name, whole in (
            ("cot", cot_m), ("cotm", cot_p.at[pl.ds(1, X - 1)]), ("act", act_m),
            ("actm", act_p.at[pl.ds(1, X - 1)]), ("ga", ga_s), ("y", wpart), ("zmid", zmid),
            ("znear", zrecv.at[0]),
        ):
            waits.append(copy(whole, whole, ids[name], s, partner))
        for r in waits:
            r.wait_send()
        waits.clear()
    with jax.named_scope("kgwait"):
        arrived(all_sums, ids["kg"])
    acc = kg[pl.ds(s * cps, cps)]
    for j in range(1, S):
        acc = acc + krecv[j].astype(f32)
    ksum[...] = acc.astype(bf16)
    acc = ksum[...].astype(f32)
    for j in range(1, N):
        copy(ksum, k2recv.at[j], ids["k2"], s, lax.rem(d + j, N)).start()
    all_parts = k2recv.at[pl.ds(1, N - 1)]
    waits.append(copy(all_parts, all_parts, ids["k2"], s, partner))
    with jax.named_scope("zwait"):
        for p in range(P):
            arrived(zrecv.at[0, :, part(p)], ids["znear"] + p)
            arrived(zrecv.at[1, :, part(p)], ids["zfar"] + p)

    def final_tile(n, _):
        cols = pl.ds(pl.multiple_of(n * LANES, LANES), LANES)
        acc = wacc[s, :, cols]
        for q in range(2):
            acc = acc + zrecv[q, :, cols].astype(f32)
        acc = acc * factor
        fin[0, :, cols] = acc[:block]
        fin[1, :, cols] = acc[block:]
        return _

    with jax.named_scope("final"):
        lax.fori_loop(0, H // LANES, final_tile, 0)
    send(fin.at[other], fbuf, ids["fin"], s, partner)
    gw[:, half] = fin[c]
    with jax.named_scope("backwait"):
        @pl.when(s < S - 1)
        def _():
            arrived(brecv, ids["back"])

    @pl.when(s == S - 1)
    def _():
        gext[:, pl.ds(T, HB), :] = jnp.zeros((chunks, HB, LANES), f32)

    @pl.when(s < S - 1)
    def _():
        gext[:, pl.ds(T, HB), :] = brecv[...].astype(f32)

    gated_grad(3)
    with jax.named_scope("k2wait"):
        arrived(all_parts, ids["k2"])
        for j in range(1, N):
            acc = acc + k2recv[j].astype(f32)
    for q in range(cps):
        cols = slice(q * LANES, (q + 1) * LANES)
        kout[:, cols] = (acc[q] * factor)[:K]
        gout[:, cols] = (acc[q] * factor)[K : K + 1]

    with jax.named_scope("finwait"):
        arrived(fbuf, ids["fin"])
    with jax.named_scope("fincopy"):
        gw[:, ohalf] = fbuf[...]
    with jax.named_scope("endwaits"):
        for r in waits:
            r.wait_send()

        @pl.when(s < S - 1)
        def _():
            front.wait_send()

        @pl.when(s > 0)
        def _():
            back.wait_send()


def number(*sizes):
    ids, count = {}, 0
    for name, size in sizes:
        ids[name] = count
        count += size
    return ids, count


def hand_over(*refs):
    half = len(refs) // 2
    stores = [pltpu.make_async_copy(refs[i], refs[half + i], refs[-1].at[i]) for i in range(half)]
    for st in stores:
        st.start()
    for st in stores:
        st.wait()


def pair_call(S, N, Y, T, C, K, HB, KP, cot, val, gate, w, kernel, gain):
    X, Z, H = N // 2, S // Y, C // 2
    chunks, cps, cpd, block = C // LANES, C // LANES // S, C // LANES // N, C // (S * N)
    M, CR = chunks // X, C // N
    ids, count = number(
        ("taps", 1), ("front", 1), ("back", 1), ("w", 1), ("cot", (X - 1) * 4), ("cotp", 1),
        ("cotm", (X - 1) * 2), ("act", (X - 1) * (Z - 2 + 2 * Y)), ("actp", 1),
        ("actm", (X - 1) * (Z - 2 + 2 * Y)), ("ga", (X - 1) * BLOCKS), ("y", (Y - 1) * Z * 3),
        ("zmid", Z // 2 * 3), ("znear", 3), ("zfar", 3), ("fin", 1), ("kg", 1), ("k2", 1),
    )
    vm = pl.BlockSpec(memory_space=pltpu.VMEM)
    hbm = pl.BlockSpec(memory_space=pl.ANY)
    partial = pl.pallas_call(
        functools.partial(pair_kernel, S, N, Y, T, C, K, HB, ids),
        out_shape=(
            jax.ShapeDtypeStruct((T, C), bf16),
            jax.ShapeDtypeStruct((T, C), bf16),
            jax.ShapeDtypeStruct((block, C), f32),
            jax.ShapeDtypeStruct((K, C // S), f32),
            jax.ShapeDtypeStruct((1, C // S), f32),
        ),
        in_specs=[hbm] * 6,
        out_specs=(vm,) * 5,
        scratch_shapes=[
            pltpu.VMEM((K, C // S), bf16),
            pltpu.VMEM((C // S,), bf16),
            pltpu.VMEM((cps, KP, LANES), bf16),
            pltpu.VMEM((T, C), bf16),
            pltpu.VMEM((T, C), bf16),
            pltpu.VMEM((T, C), bf16),
            pltpu.VMEM((CR, C), bf16),
            pltpu.VMEM((CR, C), bf16),
            pltpu.VMEM((X - 1, T, C), bf16),
            pltpu.VMEM((X, T, H), bf16),
            pltpu.VMEM((chunks, HB, LANES), bf16),
            pltpu.VMEM((chunks, HB, LANES), bf16),
            pltpu.VMEM((chunks, HB, LANES), bf16),
            pltpu.VMEM((chunks, HB, LANES), bf16),
            pltpu.VMEM((chunks, T + HB, LANES), f32),
            pltpu.VMEM((chunks, T, LANES), f32),
            pltpu.VMEM((chunks, T, LANES), f32),
            pltpu.VMEM((chunks, T + HB, LANES), f32),
            pltpu.VMEM((chunks, KP, LANES), bf16),
            pltpu.VMEM((X, M, LANES, T), bf16),
            pltpu.VMEM((X - 1, M, LANES, T), bf16),
            pltpu.VMEM((X, M, LANES, T), bf16),
            pltpu.VMEM((X - 1, 2 * cpd, T, LANES), bf16),
            pltpu.VMEM((chunks, T, LANES), bf16),
            pltpu.VMEM((M, LANES, H), f32),
            pltpu.VMEM(((Y - 1) * Z, LANES, H), bf16),
            pltpu.VMEM(((Y - 1) * Z, LANES, H), bf16),
            pltpu.VMEM((Z - 1, LANES, H), bf16),
            pltpu.VMEM((Z // 2, LANES, H), bf16),
            pltpu.VMEM((2, LANES, H), bf16),
            pltpu.VMEM((2, block, H), f32),
            pltpu.VMEM((block, H), f32),
            pltpu.VMEM((chunks, T, LANES), f32),
            pltpu.VMEM((chunks, T, LANES), f32),
            pltpu.VMEM((T, LANES), f32),
            pltpu.VMEM((T, LANES), f32),
            pltpu.VMEM((T, LANES), f32),
            pltpu.VMEM((T, LANES), f32),
            pltpu.VMEM((chunks, K + 1, 8, LANES), f32),
            pltpu.VMEM((chunks, KP, LANES), f32),
            pltpu.VMEM((chunks, KP, LANES), bf16),
            pltpu.VMEM((S, cps, KP, LANES), bf16),
            pltpu.VMEM((cps, KP, LANES), bf16),
            pltpu.VMEM((N, cps, KP, LANES), bf16),
            pltpu.SemaphoreType.DMA((len(ids),)),
            pltpu.SemaphoreType.DMA((count,)),
            pltpu.SemaphoreType.DMA((6,)),
            pltpu.SemaphoreType.REGULAR((2 * (Z - 2) + 1,)),
        ],
        compiler_params=pltpu.CompilerParams(
            collective_id=0, has_side_effects=True, vmem_limit_bytes=48 * 1024 * 1024
        ),
        name="block_backward",
    )(*(pltpu.with_memory_space_constraint(a, pltpu.HBM) for a in (cot, val, gate, w, kernel, gain)))
    return pl.pallas_call(
        hand_over,
        out_shape=(
            jax.ShapeDtypeStruct((T, C), bf16),
            jax.ShapeDtypeStruct((T, C), bf16),
            jax.ShapeDtypeStruct((block, C), f32),
            jax.ShapeDtypeStruct((K, C // S), f32),
            jax.ShapeDtypeStruct((1, C // S), f32),
        ),
        in_specs=[vm] * 5,
        out_specs=(hbm,) * 5,
        scratch_shapes=[
            pltpu.SemaphoreType.DMA((5,)),
        ],
        compiler_params=pltpu.CompilerParams(vmem_limit_bytes=16 * T * LANES),
        name="hand_over",
    )(*partial)


def general_call(S, N, T, C, K, HB, KP, cot, val, gate, w, packed):
    chunks, cps, cpd, block = C // LANES, C // LANES // S, C // LANES // N, C // (S * N)
    ids, count = number(
        ("taps", S), ("front", 1), ("back", 1), ("partner", 1), ("mirror", N // 2 * HALVES),
        ("relay", N // 2 * HALVES), ("act", N), ("ga", N), ("rs", S), ("kg", S), ("k2", N),
    )
    vm = pl.BlockSpec(memory_space=pltpu.VMEM)
    return pl.pallas_call(
        functools.partial(general_kernel, S, N, T, C, K, HB, ids),
        out_shape=(
            jax.ShapeDtypeStruct((T, C), bf16),
            jax.ShapeDtypeStruct((T, C), bf16),
            jax.ShapeDtypeStruct((block, C), f32),
            jax.ShapeDtypeStruct((K, C // S), f32),
            jax.ShapeDtypeStruct((1, C // S), f32),
        ),
        in_specs=[vm] * 5,
        out_specs=(vm,) * 5,
        scratch_shapes=[
            pltpu.VMEM((N, T, C), bf16),
            pltpu.VMEM((chunks, T + HB, LANES), f32),
            pltpu.VMEM((chunks, T, LANES), f32),
            pltpu.VMEM((chunks, T, LANES), f32),
            pltpu.VMEM((chunks, T + HB, LANES), f32),
            pltpu.VMEM((chunks, KP, LANES), bf16),
            pltpu.VMEM((chunks, T, LANES), bf16),
            pltpu.VMEM((N, cpd, T, LANES), bf16),
            pltpu.VMEM((N, cpd, T, LANES), bf16),
            pltpu.VMEM((chunks, T, LANES), bf16),
            pltpu.VMEM((cpd * LANES, C), bf16),
            pltpu.VMEM((S, block, C), bf16),
            pltpu.VMEM((chunks, KP, LANES), f32),
            pltpu.VMEM((S, cps, KP, LANES), f32),
            pltpu.VMEM((cps, KP, LANES), f32),
            pltpu.VMEM((N, cps, KP, LANES), f32),
            pltpu.SemaphoreType.DMA((count,)),
            pltpu.SemaphoreType.DMA((count,)),
        ],
        compiler_params=pltpu.CompilerParams(
            collective_id=0, has_side_effects=True, vmem_limit_bytes=60 * 1024 * 1024
        ),
        name="block_backward",
    )(cot, val, gate, w, packed)


def shards(out_cotangent, value_pre, gate_pre, out_weight, conv_kernel, norm_gain):
    S, N = lax.axis_size("sp"), lax.axis_size("dp")
    _, T, C = out_cotangent.shape
    K = conv_kernel.shape[0]
    chunks, cps = C // LANES, C // LANES // S
    HB = -(-(K - 1) // 16) * 16
    KP = -(-(K + 1) // 16) * 16
    args = (out_cotangent[0], value_pre[0], gate_pre[0], out_weight)
    X = N // 2
    if N == 2 * X > 2 and S == 2 * 2 * X and chunks == S * X:
        outs = pair_call(S, N, X, T, C, K, HB, KP, *args, conv_kernel, norm_gain)
    else:
        packed = jnp.concatenate(
            [conv_kernel, norm_gain[None], jnp.zeros((KP - K - 1, C // S), bf16)], axis=0
        )
        packed = jnp.transpose(packed.reshape(KP, cps, LANES), (1, 0, 2))
        outs = general_call(S, N, T, C, K, HB, KP, *args, packed)
    grad_value, grad_gate, grad_weight, grad_taps, grad_gain = outs
    return grad_value[None], grad_gate[None], grad_weight, grad_taps, grad_gain[0]


def solution(mesh):
    placed = (
        P("dp", "sp", None),
        P("dp", "sp", None),
        P("dp", "sp", None),
        P("dp", None),
        P(None, "sp"),
        P("sp"),
    )
    return jax.shard_map(
        shards,
        mesh=mesh,
        in_specs=placed,
        out_specs=(
            P("dp", "sp", None),
            P("dp", "sp", None),
            P(("sp", "dp"), None),
            P(None, "sp"),
            P("sp"),
        ),
        check_vma=False,
    )
```
